128 devices in a mesh: sp: 32 (over z, y, core), tp: 4 (over x).
Axes of the slice: x: 4, y: 4, z: 4, core: 2. Of those that a mesh axis runs over, the one named last changes fastest.
Arguments:
- layer_source: bfloat16 [32768, 2048], P(('sp', 'tp')), may hold values from -6 to 6
- broad_probe_tensor: bfloat16 [32768, 512], P('sp', 'tp'), may hold values from -6 to 6
- broad_retention_preact: bfloat16 [32768, 512], P('sp', 'tp'), may hold values from -6 to 6
- broad_floor_margin: float32 [512], P('tp'), may hold values from 9.1552734e-06 to 0.12
- slim_probe_tensor: bfloat16 [32768, 256], P('sp', 'tp'), may hold values from -6 to 6
- slim_retention_preact: bfloat16 [32768, 256], P('sp', 'tp'), may hold values from -6 to 6
- slim_floor_margin: float32 [256], P('tp'), may hold values from 9.1552734e-06 to 0.12
- branch_content_tensor: bfloat16 [2, 32768, 512], P(None, 'sp', 'tp'), may hold values from -6 to 6
- emitted_switch_preact: bfloat16 [2, 32768, 512], P(None, 'sp', 'tp'), may hold values from -6 to 6
- extra_log_fades: float32 [2, 32768, 4], P(None, 'sp', 'tp'), may hold values from -1.4 to 0
- channel_norm_scale: float32 [128], replicated, may hold values from 0.1 to 1.9
- emission_projection: bfloat16 [2, 512, 2048], replicated, may hold values from -0.1875 to 0.1875
- mlp_norm_scale: float32 [2048], replicated, may hold values from 0.1 to 1.9
- switch_projection: bfloat16 [2048, 5632], P('sp', 'tp'), may hold values from -0.125 to 0.125
- expand_projection: bfloat16 [2048, 5632], P('sp', 'tp'), may hold values from -0.125 to 0.125
- shrink_projection: bfloat16 [5632, 2048], P('tp', 'sp'), may hold values from -0.078125 to 0.078125
Outputs:
- layer_out: bfloat16 [32768, 2048], P(('sp', 'tp'))
The draws below stay inside these ranges and needn't reach their ends.
All inputs are finite; a program needn't handle non-finite values.
Results may differ from the reference program's by a relative error of at most 0.0095.
Values may be sent and summed in bfloat16 or wider, within the bound.
A program may use at most 192 MiB of HBM per device.

```python
import jax
import jax.numpy as jnp
from jax import lax

D = 2048
FF = 5632
BRANCH_CHANNELS = 4
KW = 128
KN = 64
DV = 128
BLOCK = 64
TOK_DEV = 1024
TOKENS = 32768


def forget_draw(key, key_width):
    block_rows = TOK_DEV // 2
    block_count = TOKENS // block_rows
    noise = jax.random.normal(key, (TOKENS, BRANCH_CHANNELS * key_width), jnp.float32)
    offsets = jax.random.uniform(jax.random.fold_in(key, 7), (block_count, 1, BRANCH_CHANNELS, 1), jnp.float32, -1.5, 1.5)
    shaped = noise.reshape(block_count, block_rows, BRANCH_CHANNELS, key_width) + offsets
    return jnp.clip(shaped.reshape(TOKENS, BRANCH_CHANNELS * key_width), -6.0, 6.0).astype(jnp.bfloat16)


def gap_draw(key, key_width):
    order = jax.random.permutation(jax.random.fold_in(key, 3), BRANCH_CHANNELS)
    slow_count = BRANCH_CHANNELS // 2
    slow_heads = (order < slow_count)[:, None]
    spread = jax.random.uniform(jax.random.fold_in(key, 5), (BRANCH_CHANNELS, key_width), jnp.float32)
    slow_gap = jnp.exp(jnp.log(0.3 / TOKENS) + spread * jnp.log(5.0))
    fast_gap = jnp.exp(jnp.log(0.04) + spread * jnp.log(3.0))
    return jnp.where(slow_heads, slow_gap, fast_gap).reshape(BRANCH_CHANNELS * key_width)


def draw_broad_retention_preact(key, part):
    return forget_draw(key, KW)


def draw_slim_retention_preact(key, part):
    return forget_draw(key, KN)


def draw_broad_floor_margin(key, part):
    return gap_draw(key, KW)


def draw_slim_floor_margin(key, part):
    return gap_draw(key, KN)


def draw_extra_log_fades(key, part):
    picks = jax.random.randint(key, (2, 2, BRANCH_CHANNELS), 0, TOKENS)
    amounts = jax.random.uniform(jax.random.fold_in(key, 11), (2, 2, BRANCH_CHANNELS), jnp.float32, jnp.log(0.5), jnp.log(0.8))
    matched = jnp.arange(TOKENS)[None, None, :, None] == picks[:, :, None, :]
    return jnp.sum(jnp.where(matched, amounts[:, :, None, :], 0.0), axis=1)


def level_of(own_key, dims, cuts, least, high):
    loudness = 1.0
    for position, shards_of in cuts:
        steps = jax.random.uniform(jax.random.fold_in(jax.random.fold_in(own_key, 6), position), (shards_of,), jnp.float32, least / len(cuts), high / len(cuts))
        loudness = loudness * jnp.repeat(jnp.exp(steps), dims[position] // shards_of).reshape((-1,) + (1,) * (len(dims) - 1 - position))
    return loudness


def gaussian(key, shape, scale, most, pieces=(), kind=jnp.bfloat16):
    values = scale * jax.random.normal(key, shape, jnp.float32)
    if pieces:
        values = values * level_of(key, shape, pieces, -0.22, 0.18)
    return jnp.clip(values, -most, most).astype(kind)


def setup_inputs(seed: int = 0) -> dict:
    seeds = jax.random.split(jax.random.key(seed), 17)
    return {
        "layer_source": gaussian(seeds[0], (TOKENS, D), 1.0, 6.0, ((0, 128),)),
        "broad_probe_tensor": gaussian(seeds[1], (TOKENS, BRANCH_CHANNELS * KW), 1.0, 6.0, ((0, 32), (1, 4))),
        "broad_retention_preact": draw_broad_retention_preact(jax.random.fold_in(seeds[16], 71), 0),
        "broad_floor_margin": draw_broad_floor_margin(jax.random.fold_in(seeds[16], 71), 0),
        "slim_probe_tensor": gaussian(seeds[4], (TOKENS, BRANCH_CHANNELS * KN), 1.0, 6.0, ((0, 32), (1, 4))),
        "slim_retention_preact": draw_slim_retention_preact(jax.random.fold_in(seeds[16], 71), 0),
        "slim_floor_margin": draw_slim_floor_margin(jax.random.fold_in(seeds[16], 71), 0),
        "branch_content_tensor": gaussian(seeds[7], (2, TOKENS, BRANCH_CHANNELS * DV), 1.0, 6.0, ((1, 32), (2, 4))),
        "emitted_switch_preact": gaussian(seeds[8], (2, TOKENS, BRANCH_CHANNELS * DV), 1.0, 6.0, ((1, 32), (2, 4))),
        "extra_log_fades": draw_extra_log_fades(jax.random.fold_in(seeds[16], 71), 0),
        "channel_norm_scale": jnp.clip(1.0 + 0.18 * jax.random.normal(seeds[10], (DV,), jnp.float32), 0.1, 1.9),
        "emission_projection": gaussian(seeds[11], (2, BRANCH_CHANNELS * DV, D), (2 * BRANCH_CHANNELS * DV) ** -0.5, 0.1875),
        "mlp_norm_scale": jnp.clip(1.0 + 0.18 * jax.random.normal(seeds[12], (D,), jnp.float32), 0.1, 1.9),
        "switch_projection": gaussian(seeds[13], (D, FF), D ** -0.5, 0.125, ((0, 32), (1, 4))),
        "expand_projection": gaussian(seeds[14], (D, FF), D ** -0.5, 0.125, ((0, 32), (1, 4))),
        "shrink_projection": gaussian(seeds[15], (FF, D), FF ** -0.5, 0.078125, ((0, 4), (1, 32))),
    }


EPSILON = 1e-06
EXACT_PRECISION = lax.Precision.HIGHEST

def switched_token_entries(probe_array, retention_sigmoid, floor_margin, spike_rows, rows_of_values, count_heads):
    length = probe_array.shape[0]
    key_width = probe_array.shape[1] // count_heads
    shaped = retention_sigmoid.astype(jnp.float32).reshape(length, count_heads, key_width)
    address_entries = floor_margin.reshape(count_heads, key_width) * jax.nn.sigmoid(-shaped)
    log_fade_amount = jnp.log1p(-address_entries) + spike_rows[:, :, None]
    probe_entries = jax.nn.silu(probe_array.astype(jnp.float32)).reshape(length, count_heads, key_width) * key_width ** (-0.5)
    content_arrays = rows_of_values.astype(jnp.float32).reshape(length, count_heads, -1)
    return (probe_entries, address_entries, log_fade_amount, content_arrays)

def block_recurrence(probe_entries, address_entries, log_fade_amount, content_arrays, block_len):
    length, count_heads, key_width = probe_entries.shape
    value_width = content_arrays.shape[2]
    block_count = length // block_len

    def to_blocks(tensor):
        return jnp.moveaxis(tensor.reshape(block_count, block_len, count_heads, tensor.shape[2]), 2, 1)
    causal_mask = jnp.tril(jnp.ones((block_len, block_len), dtype=bool))[None, :, :, None]

    def advance(carried, inputs):
        state_stack, running = carried
        block_queries, key_block, block_values, decay_block = inputs
        prefix_decay = jnp.cumsum(decay_block, axis=1)
        state_contribution = jnp.einsum('yga,yau->ygu', block_queries * jnp.exp(prefix_decay), state_stack, precision=EXACT_PRECISION)
        relative = prefix_decay[:, :, None, :] - prefix_decay[:, None, :, :]
        decays = jnp.exp(jnp.where(causal_mask, relative, -jnp.inf))
        scores = jnp.einsum('htk,hsk,htsk->hts', block_queries, key_block, decays, precision=EXACT_PRECISION)
        inside = jnp.einsum('hts,hsv->htv', scores, block_values, precision=EXACT_PRECISION)
        total_blocks = prefix_decay[:, -1, :]
        weighted_scores = key_block * jnp.exp(total_blocks[:, None, :] - prefix_decay)
        state_stack = jnp.exp(total_blocks)[:, :, None] * state_stack + jnp.einsum('xpf,xpq->xfq', weighted_scores, block_values, precision=EXACT_PRECISION)
        reached_state = block_queries * jnp.exp(running[:, None, :] + prefix_decay)
        return ((state_stack, running + total_blocks), (state_contribution + inside, reached_state))
    initial = (jnp.zeros((count_heads, key_width, value_width), jnp.float32), jnp.zeros((count_heads, key_width), jnp.float32))
    last_carry, (output_rows, reached_state) = lax.scan(advance, initial, (to_blocks(probe_entries), to_blocks(address_entries), to_blocks(content_arrays), to_blocks(log_fade_amount)))

    def from_blocks(tensor):
        return jnp.moveaxis(tensor, 1, 2).reshape(length, count_heads, tensor.shape[3])
    return (from_blocks(output_rows), from_blocks(reached_state), last_carry)

def head_norm(output_rows, channel_norm_scale, gate_rows):
    inverse = lax.rsqrt(lax.optimization_barrier(jnp.mean(output_rows * output_rows, axis=2, keepdims=True)) + EPSILON)
    normed = (output_rows * inverse * channel_norm_scale).reshape(output_rows.shape[0], -1)
    return (normed * jax.nn.silu(gate_rows.astype(jnp.float32))).astype(jnp.bfloat16)

def reference(layer_source, broad_probe_tensor, broad_retention_preact, broad_floor_margin, slim_probe_tensor, slim_retention_preact, slim_floor_margin, branch_content_tensor, emitted_switch_preact, extra_log_fades, channel_norm_scale, emission_projection, mlp_norm_scale, switch_projection, expand_projection, shrink_projection):
    groups = ((broad_probe_tensor, broad_retention_preact, broad_floor_margin), (slim_probe_tensor, slim_retention_preact, slim_floor_margin))
    branch = jnp.zeros(layer_source.shape, jnp.float32)
    for element_ordinal in range(2):
        probe_array, retention_sigmoid, floor_margin = groups[element_ordinal]
        probe_entries, address_entries, log_fade_amount, content_arrays = switched_token_entries(probe_array, retention_sigmoid, floor_margin, extra_log_fades[element_ordinal], branch_content_tensor[element_ordinal], BRANCH_CHANNELS)
        output_rows, reached_state, last_carry = block_recurrence(probe_entries, address_entries, log_fade_amount, content_arrays, BLOCK)
        mixed = head_norm(output_rows, channel_norm_scale, emitted_switch_preact[element_ordinal])
        branch = branch + jnp.dot(mixed, emission_projection[element_ordinal], preferred_element_type=jnp.float32)
    updated = layer_source.astype(jnp.float32) + branch
    inverse = lax.rsqrt(lax.optimization_barrier(jnp.mean(updated * updated, axis=1, keepdims=True)) + EPSILON)
    normed = (updated * inverse * mlp_norm_scale).astype(jnp.bfloat16)
    gate_part = jnp.dot(normed, switch_projection, preferred_element_type=jnp.float32)
    up_part = jnp.dot(normed, expand_projection, preferred_element_type=jnp.float32)
    hidden = (jax.nn.silu(gate_part) * up_part).astype(jnp.bfloat16)
    ffn_sum = jnp.dot(hidden, shrink_projection, preferred_element_type=jnp.float32)
    return (updated + 0.5 * ffn_sum).astype(jnp.bfloat16)
```

```python
import jax
import jax.numpy as jnp
from jax import lax
from jax.experimental import pallas as pl
from jax.experimental.pallas import tpu as pltpu
from jax.sharding import Mesh
from jax.sharding import PartitionSpec as P

BRANCH_CHANNELS = 4
BLOCK = 64
SP = ("sp_0", "sp_1", "sp_2")
SP_TP = ("sp_0", "sp_1", "sp_2", "tp")


EPSILON = 1e-06
EXACT_PRECISION = lax.Precision.HIGHEST


def filled_with(value, identity):
    return jax.tree.map(
        lambda part, zero: jnp.zeros_like(part) + jnp.asarray(zero, part.dtype), value, identity
    )


def collected_together(value, axis):
    leaves = jax.tree.leaves(value)
    turns = sorted(range(len(leaves)), key=lambda k: -leaves[k].size)
    width = (1, *leaves[turns[0]].shape)[-1]
    lines = [
        jnp.pad(leaves[k].reshape(-1), (0, -leaves[k].size % width)).reshape(-1, width)
        for k in turns
    ]
    both, at, found = (lax.all_gather(jnp.concatenate(lines), axis), 0, {})
    for k, line in zip(turns, lines):
        share = both[:, at : at + len(line)].reshape(len(both), -1)
        found[k] = share[:, : leaves[k].size].reshape(-1, *leaves[k].shape)
        at += len(line)
    numbers = iter(range(len(leaves)))
    return jax.tree.map(lambda _: found[next(numbers)], value)


def entering(value, axes, combine, identity):
    before = start = filled_with(value, identity)
    total = value
    for axis in reversed(axes):
        count, mine = (lax.axis_size(axis), lax.axis_index(axis))
        pieces = collected_together(total, axis)
        inside, total = (start, start)
        for k in range(count):
            passed = k < mine
            total = combine(total, jax.tree.map(lambda part: part[k], pieces))
            inside = jax.tree.map(lambda new, old: jnp.where(passed, new, old), total, inside)
        before = combine(inside, before)
    return before


def in_order(parts, dim):
    parts = jnp.moveaxis(parts, 0, dim)
    shape = parts.shape
    return parts.reshape(*shape[:dim], shape[dim] * shape[dim + 1], *shape[dim + 2 :])


def sent_to_all(value, axis):
    count = lax.axis_size(axis)
    return lax.all_to_all(
        jnp.broadcast_to(value[None], (count, *value.shape)), axis, 0, 0, tiled=True
    )


def collect(value, axis, dim):
    return in_order(sent_to_all(value, axis), dim)


def centred_block(query, key, value, prefix, mask, state):
    half = BLOCK // 2
    middle, total = (prefix[half - 1 : half, :], prefix[BLOCK - 1 : BLOCK, :])
    query_in = query * jnp.exp(prefix - middle)
    key_in = key * jnp.exp(middle - prefix)
    scores = lax.dot_general(
        query_in.astype(jnp.bfloat16),
        key_in.astype(jnp.bfloat16),
        (((1,), (1,)), ((), ())),
        preferred_element_type=jnp.float32,
    )
    scores = jnp.where(mask, scores, 0.0).astype(jnp.bfloat16)
    inside = jnp.dot(scores, value, preferred_element_type=jnp.float32)
    reach = query_in * jnp.exp(middle)
    earlier = lax.dot_general(
        reach.astype(jnp.bfloat16),
        state.astype(jnp.bfloat16),
        (((1,), (1,)), ((), ())),
        preferred_element_type=jnp.float32,
    )
    leaving = (key_in * jnp.exp(total - middle)).astype(jnp.bfloat16)
    state = state * jnp.exp(total) + lax.dot_general(
        value, leaving, (((0,), (0,)), ((), ())), preferred_element_type=jnp.float32
    )
    return (inside + earlier, reach, total, state)


def recurrence_kernel(
    wide_query,
    wide_forget,
    wide_gap,
    narrow_query,
    narrow_forget,
    narrow_gap,
    values,
    fades,
    wide_out,
    wide_reach,
    wide_state,
    wide_log,
    narrow_out,
    narrow_reach,
    narrow_state,
    narrow_log,
):
    rows = lax.broadcasted_iota(jnp.int32, (BLOCK, BLOCK), 0)
    columns = lax.broadcasted_iota(jnp.int32, (BLOCK, BLOCK), 1)
    mask = rows >= columns
    ones = jnp.where(mask, 1.0, 0.0)
    groups = (
        (wide_query, wide_forget, wide_gap, wide_out, wide_reach),
        (narrow_query, narrow_forget, narrow_gap, narrow_out, narrow_reach),
    )

    def advance(block, carried):
        at = pl.ds(pl.multiple_of(block * BLOCK, BLOCK), BLOCK)
        left = []
        for g in range(2):
            query_ref, forget_ref, gap_ref, out_ref, reach_ref = groups[g]
            state, running = carried[g]
            key = gap_ref[...] * jax.nn.sigmoid(-forget_ref[at, :].astype(jnp.float32))
            decay = jnp.log1p(-key) + fades[g, at, :]
            query = jax.nn.silu(query_ref[at, :].astype(jnp.float32)) * key.shape[1] ** (-0.5)
            prefix = jnp.dot(
                ones, decay, preferred_element_type=jnp.float32, precision=EXACT_PRECISION
            )
            out, reach, total, state = centred_block(
                query, key, values[g, at, :], prefix, mask, state
            )
            out_ref[at, :] = out
            reach_ref[at, :] = (reach * jnp.exp(running)).astype(jnp.bfloat16)
            left.append((state, running + total))
        return tuple(left)

    start = tuple(
        (
            jnp.zeros((values.shape[2], group[0].shape[1]), jnp.float32),
            jnp.zeros((1, group[0].shape[1]), jnp.float32),
        )
        for group in groups
    )
    wide, narrow = lax.fori_loop(0, wide_query.shape[0] // BLOCK, advance, start, unroll=4)
    wide_state[...], wide_log[...] = wide
    narrow_state[...], narrow_log[...] = narrow


def local_recurrence(wide_query, wide_forget, wide_gap, narrow_query, narrow_forget, narrow_gap, values, fades):
    length, width = (wide_query.shape[0], values.shape[2])
    vmem = pl.BlockSpec(memory_space=pltpu.VMEM)
    shapes = []
    for query in (wide_query, narrow_query):
        keys = query.shape[1]
        shapes += [
            jax.ShapeDtypeStruct((length, width), jnp.float32),
            jax.ShapeDtypeStruct((length, keys), jnp.bfloat16),
            jax.ShapeDtypeStruct((width, keys), jnp.float32),
            jax.ShapeDtypeStruct((1, keys), jnp.float32),
        ]
    return pl.pallas_call(
        recurrence_kernel,
        out_shape=tuple(shapes),
        in_specs=[vmem] * 8,
        out_specs=(vmem,) * 8,
        cost_estimate=pl.CostEstimate(flops=10**10, bytes_accessed=4 * 10**6, transcendentals=10**6),
    )(
        wide_query,
        wide_forget,
        wide_gap.reshape(1, -1),
        narrow_query,
        narrow_forget,
        narrow_gap.reshape(1, -1),
        values,
        fades,
    )


def head_norm(output_rows, channel_norm_scale, gate_rows):
    inverse = lax.rsqrt(jnp.mean(output_rows * output_rows, axis=2, keepdims=True) + EPSILON)
    normed = (output_rows * inverse * channel_norm_scale).reshape(output_rows.shape[0], -1)
    return (normed * jax.nn.silu(gate_rows.astype(jnp.float32))).astype(jnp.bfloat16)


def combine(earlier, later):
    wide_early, wide_state_early, narrow_early, narrow_state_early = earlier
    wide_late, wide_state_late, narrow_late, narrow_state_late = later
    return (
        wide_early + wide_late,
        jnp.exp(wide_late) * wide_state_early + wide_state_late,
        narrow_early + narrow_late,
        jnp.exp(narrow_late) * narrow_state_early + narrow_state_late,
    )


def local(
    layer_source,
    broad_probe_tensor,
    broad_retention_preact,
    broad_floor_margin,
    slim_probe_tensor,
    slim_retention_preact,
    slim_floor_margin,
    branch_content_tensor,
    emitted_switch_preact,
    extra_log_fades,
    channel_norm_scale,
    emission_projection,
    mlp_norm_scale,
    switch_projection,
    expand_projection,
    shrink_projection,
):
    tp_count = lax.axis_size("tp")
    row_count = layer_source.shape[0]
    gate_full = lax.all_gather(switch_projection, SP, axis=0, tiled=True)
    up_full = lax.all_gather(expand_projection, SP, axis=0, tiled=True)
    down_full = lax.all_gather(shrink_projection.T, SP, axis=0, tiled=True)
    found = local_recurrence(
        broad_probe_tensor,
        broad_retention_preact,
        broad_floor_margin,
        slim_probe_tensor,
        slim_retention_preact,
        slim_floor_margin,
        branch_content_tensor,
        extra_log_fades,
    )
    wide_out, wide_reach, wide_state, wide_log, narrow_out, narrow_reach, narrow_state, narrow_log = found
    identity = jax.tree.map(jnp.zeros_like, (wide_log, wide_state, narrow_log, narrow_state))
    carried = entering((wide_log, wide_state, narrow_log, narrow_state), SP, combine, identity)
    mixed_parts = []
    for g, (output_rows, reach, state) in enumerate(
        ((wide_out, wide_reach, carried[1]), (narrow_out, narrow_reach, carried[3]))
    ):
        output_rows = output_rows + lax.dot_general(
            reach,
            state.astype(jnp.bfloat16),
            (((1,), (1,)), ((), ())),
            preferred_element_type=jnp.float32,
        )
        mixed_parts.append(
            head_norm(output_rows[:, None, :], channel_norm_scale, emitted_switch_preact[g])
        )
    mixed = jnp.concatenate(mixed_parts, axis=1)
    group_width = branch_content_tensor.shape[2]
    model_width = emission_projection.shape[2]
    regrouped = lax.all_to_all(mixed, "tp", split_axis=0, concat_axis=1, tiled=True)
    shaped = regrouped.reshape(row_count, tp_count, 2, group_width)
    branch = jnp.einsum(
        "rtgc,gtcd->rd",
        shaped,
        emission_projection.reshape(2, tp_count, group_width, model_width),
        preferred_element_type=jnp.float32,
    )
    updated = layer_source.astype(jnp.float32) + branch
    inverse = lax.rsqrt(jnp.mean(updated * updated, axis=1, keepdims=True) + EPSILON)
    normed = (updated * inverse * mlp_norm_scale).astype(jnp.bfloat16)
    row_piece = collect(normed, "tp", 0)
    gate_part = jnp.dot(row_piece, gate_full, preferred_element_type=jnp.float32)
    up_part = jnp.dot(row_piece, up_full, preferred_element_type=jnp.float32)
    hidden = (jax.nn.silu(gate_part) * up_part).astype(jnp.bfloat16)
    ffn_sum = lax.psum_scatter(
        lax.dot_general(
            hidden, down_full, (((1,), (1,)), ((), ())), preferred_element_type=jnp.float32
        ).astype(jnp.bfloat16),
        "tp",
        scatter_dimension=0,
        tiled=True,
    ).astype(jnp.float32)
    return (updated + 0.5 * ffn_sum).astype(jnp.bfloat16)


def solution(mesh):
    torus = Mesh(mesh.devices.reshape(4, 4, 2, mesh.shape["tp"]), ("sp_0", "sp_1", "sp_2", "tp"))
    placed = (
        P(SP_TP, None),
        P(SP, "tp"),
        P(SP, "tp"),
        P("tp"),
        P(SP, "tp"),
        P(SP, "tp"),
        P("tp"),
        P(None, SP, "tp"),
        P(None, SP, "tp"),
        P(None, SP, "tp"),
        P(),
        P(),
        P(),
        P(SP, "tp"),
        P(SP, "tp"),
        P("tp", SP),
    )
    return jax.shard_map(
        local, mesh=torus, in_specs=placed, out_specs=P(SP_TP, None), check_vma=False
    )
```

```python
import jax
import jax.numpy as jnp
from jax import lax
from jax.experimental import pallas as pl
from jax.experimental.pallas import tpu as pltpu
from jax.sharding import Mesh
from jax.sharding import PartitionSpec as P

BLOCK = 64
RING = 4
SP = ("sp_0", "sp_1", "sp_2")
SP_TP = ("sp_0", "sp_1", "sp_2", "tp")

EPSILON = 1e-06
EXACT_PRECISION = lax.Precision.HIGHEST
BF16 = jnp.bfloat16
F32 = jnp.float32
NT = (((1,), (1,)), ((), ()))
TN = (((0,), (0,)), ((), ()))
MESH = pl.DeviceIdType.MESH

ARRIVALS = (
    (3, 0, 0),
    (1, 0, 1),
    (0, 3, 0),
    (0, 1, 1),
    (3, 0, 1),
    (1, 0, 0),
    (0, 3, 1),
    (0, 1, 0),
    (2, 0, 0),
    (2, 0, 1),
    (3, 3, 0),
    (3, 1, 1),
    (1, 3, 0),
    (1, 1, 1),
    (3, 3, 1),
    (3, 1, 0),
    (0, 2, 0),
    (0, 2, 1),
    (1, 3, 1),
    (1, 1, 0),
    (2, 3, 0),
    (2, 1, 1),
    (2, 3, 1),
    (2, 1, 0),
    (3, 2, 0),
    (3, 2, 1),
    (1, 2, 0),
    (1, 2, 1),
    (2, 2, 0),
    (2, 2, 1),
)


def turn(value, step):
    return lax.rem(value + step, RING)


def dot(a, b, dims=(((1,), (0,)), ((), ())), precision=None):
    return lax.dot_general(a, b, dims, preferred_element_type=F32, precision=precision)


def combine(earlier, later):
    wide_early, narrow_early, wide_state_early, narrow_state_early = earlier
    wide_late, narrow_late, wide_state_late, narrow_state_late = later
    return (
        wide_early + wide_late,
        narrow_early + narrow_late,
        jnp.exp(wide_late) * wide_state_early + wide_state_late,
        jnp.exp(narrow_late) * narrow_state_early + narrow_state_late,
    )


def split_log(log):
    first = log.astype(BF16).astype(F32)
    second = (log - first).astype(BF16).astype(F32)
    return [first, second, log - first - second]


def store_state(ref, at, state):
    wide, narrow, wide_state, narrow_state = state
    ref[at, 0:128, :] = wide_state.astype(BF16)
    ref[at, 128:192, :] = narrow_state.astype(BF16)
    lines = split_log(wide) + split_log(narrow)
    lines.append(jnp.zeros((10, wide.shape[1]), F32))
    ref[at, 192:208, :] = jnp.concatenate(lines, axis=0).astype(BF16)


def load_state(ref, at):
    lines = ref[at, 192:208, :].astype(F32)
    wide = lines[0:1] + lines[1:2] + lines[2:3]
    narrow = lines[3:4] + lines[4:5] + lines[5:6]
    return (wide, narrow, ref[at, 0:128, :].astype(F32), ref[at, 128:192, :].astype(F32))


def selected(passed, new, old):
    return jax.tree.map(lambda a, b: jnp.where(passed, a, b), new, old)


def block_step(query, key, value, prefix, mask, state):
    half = BLOCK // 2
    middle, total = (prefix[half - 1 : half, :], prefix[BLOCK - 1 : BLOCK, :])
    query_in = query * jnp.exp(prefix - middle)
    key_in = key * jnp.exp(middle - prefix)
    scores = dot(query_in.astype(BF16), key_in.astype(BF16), NT)
    scores = jnp.where(mask, scores, 0.0).astype(BF16)
    inside = dot(scores, value)
    reach = query_in * jnp.exp(middle)
    earlier = dot(reach.astype(BF16), state.astype(BF16), NT)
    leaving = (key_in * jnp.exp(total - middle)).astype(BF16)
    state = state * jnp.exp(total) + dot(value, leaving, TN)
    return (inside + earlier, reach, total, state)


def layer_kernel(
    layer_source,
    wide_query,
    wide_forget,
    wide_gap,
    narrow_query,
    narrow_forget,
    narrow_gap,
    values,
    switches,
    fades,
    channel_norm_scale,
    emission,
    mlp_scale,
    gate_shard,
    up_shard,
    down_shard,
    layer_out,
    weights,
    sources,
    mixed,
    projection,
    updated,
    normed,
    hidden,
    partial,
    own_part,
    passing,
    landed,
    narrow_q,
    narrow_f,
    wide_out,
    narrow_out,
    wide_reach,
    narrow_reach,
    core_states,
    y_states,
    z_states,
    load_sem,
    w_send,
    w_recv,
    d_send,
    d_recv,
    x_send,
    x_recv,
    s_send,
    s_recv,
    r_send,
    r_recv,
):
    z, y, core, x = (lax.axis_index(name) for name in SP_TP)
    other = 1 - core
    rows, model = layer_source.shape
    length = wide_query.shape[0]
    ff = gate_shard.shape[1]
    depth = gate_shard.shape[0]
    sent = []

    def send(src, dst, send_sem, recv_sem, to):
        copy = pltpu.make_async_remote_copy(
            src_ref=src,
            dst_ref=dst,
            send_sem=send_sem,
            recv_sem=recv_sem,
            device_id=to,
            device_id_type=MESH,
        )
        copy.start()
        sent.append(copy)

    partner = {"sp_2": other}

    def arrived(ref, sem):
        pltpu.make_async_remote_copy(
            src_ref=ref,
            dst_ref=ref,
            send_sem=sem,
            recv_sem=sem,
            device_id=partner,
            device_id_type=MESH,
        ).wait_recv()

    def place(i, j, of_core):
        first = jnp.where(of_core == 0, y, z)
        second = jnp.where(of_core == 0, z, y)
        first, second = (turn(first, i), turn(second, j))
        return (
            jnp.where(of_core == 0, second, first),
            jnp.where(of_core == 0, first, second),
        )

    def slot(i, j, of_core):
        at_z, at_y = place(i, j, of_core)
        return at_z * 8 + at_y * 2 + of_core

    half_depth = depth // 2

    def shard(i, j, h, of_core):
        return weights.at[slot(i, j, of_core), pl.ds(h * half_depth, half_depth), :]

    def toward(i, j):
        at_z, at_y = place(i, j, core)
        return {"sp_0": at_z, "sp_1": at_y}

    def mark(i, j, h):
        return (i * 4 + j) * 2 + h

    counts = {"w": 0, "d": 0, "x": 0}

    def next_of(name):
        counts[name] += 1
        return counts[name] - 1

    def forward(i, j, h, step, landing):
        src = shard(i, j, h, core)
        send(src, src, w_send.at[next_of("w")], w_recv.at[mark(*landing, h)], toward(*step))

    def hand_over(i, j, h):
        src = shard(i, j, h, core)
        send(src, src, d_send.at[next_of("d")], d_recv.at[mark(i, j, h)], partner)

    def spread_second(i, h):
        forward(i, 0, h, (0, 1), (i, 3))
        forward(i, 0, h, (0, 3), (i, 1))

    def pump(events):
        for i, j, h in events:
            arrived(shard(i, j, h, core), w_recv.at[mark(i, j, h)])
            if j == 0:
                if (i, h) == (3, 0):
                    forward(i, 0, h, (1, 0), (2, 0))
                if (i, h) == (1, 1):
                    forward(i, 0, h, (3, 0), (2, 0))
                spread_second(i, h)
            else:
                if (j, h) == (3, 0):
                    forward(i, j, h, (0, 1), (i, 2))
                if (j, h) == (1, 1):
                    forward(i, j, h, (0, 3), (i, 2))
            hand_over(i, j, h)

    def x_piece(buffer, step, h):
        half = buffer.shape[1] // 2
        return buffer.at[turn(x, step), pl.ds(h * half, half), :]

    def x_forward(buffer, base, step, h, to, landing):
        src = x_piece(buffer, step, h)
        send(src, src, x_send.at[next_of("x")], x_recv.at[base + landing * 2 + h], {"tp": turn(x, to)})

    def x_wait(buffer, base, step, h):
        arrived(x_piece(buffer, step, h), x_recv.at[base + step * 2 + h])

    def x_start(buffer, base, h):
        x_forward(buffer, base, 0, h, 1, 3)
        x_forward(buffer, base, 0, h, 3, 1)

    def x_relay(buffer, base):
        x_wait(buffer, base, 3, 0)
        x_forward(buffer, base, 3, 0, 1, 2)
        x_wait(buffer, base, 1, 1)
        x_forward(buffer, base, 1, 1, 3, 2)

    def x_finish(buffer, base):
        for step, h in ((3, 1), (1, 0), (2, 0), (2, 1)):
            x_wait(buffer, base, step, h)

    me = slot(0, 0, core)
    loads = []

    def load(src, dst):
        copy = pltpu.make_async_copy(src, dst, load_sem.at[len(loads)])
        copy.start()
        loads.append(copy)

    for n in range(ff // 128):
        cols = pl.ds(n * 128, 128)
        load(gate_shard.at[:, cols], weights.at[me, :, pl.ds(n * 256, 128)])
        load(up_shard.at[:, cols], weights.at[me, :, pl.ds(n * 256 + 128, 128)])
    load(down_shard, weights.at[me, :, pl.ds(2 * ff, ff)])
    load(layer_source, sources.at[x])
    first_loads = len(loads)
    for t in range(RING):
        for g in range(2):
            load(emission.at[g, pl.ds(t * 128, 128), :], projection.at[t, pl.ds(g * 128, 128), :])

    barrier = pltpu.get_barrier_semaphore()
    pl.semaphore_signal(barrier, inc=1, device_id=partner, device_id_type=MESH)
    for name, here in (("sp_0", z), ("sp_1", y), ("tp", x)):
        for step in (1, 2, 3):
            pl.semaphore_signal(
                barrier, inc=1, device_id={name: turn(here, step)}, device_id_type=MESH
            )
    pl.semaphore_wait(barrier, 10)

    for copy in loads[:first_loads]:
        copy.wait()
    for h in range(2):
        forward(0, 0, h, (1, 0), (3, 0))
        forward(0, 0, 1 - h, (3, 0), (1, 0))
        forward(0, 0, h, (0, 1), (0, 3))
        forward(0, 0, 1 - h, (0, 3), (0, 1))
        x_forward(sources, 0, 0, h, 1, 3)
        x_forward(sources, 0, 0, 1 - h, 3, 1)
    for h in range(2):
        hand_over(0, 0, h)

    for n in range(length // 128):
        cols = pl.ds(n * 128, 128)
        narrow_q[cols, :] = narrow_query[:, cols].astype(F32).T
        narrow_f[cols, :] = narrow_forget[:, cols].astype(F32).T
    line = lax.broadcasted_iota(jnp.int32, (BLOCK, BLOCK), 0)
    column = lax.broadcasted_iota(jnp.int32, (BLOCK, BLOCK), 1)
    mask = line >= column
    ones = jnp.where(mask, 1.0, 0.0)
    groups = (
        (wide_query, wide_forget, wide_gap, wide_out, wide_reach),
        (narrow_q, narrow_f, narrow_gap, narrow_out, narrow_reach),
    )

    def advance(block, carried):
        at = pl.ds(pl.multiple_of(block * BLOCK, BLOCK), BLOCK)
        left = []
        for g in range(2):
            query_ref, forget_ref, gap_ref, out_ref, reach_ref = groups[g]
            state, running = carried[g]
            key = gap_ref[...] * jax.nn.sigmoid(-forget_ref[at, :].astype(F32))
            decay = jnp.log1p(-key)
            query = jax.nn.silu(query_ref[at, :].astype(F32)) * key.shape[1] ** (-0.5)
            faded = jnp.sum(ones * fades[g, pl.ds(block, 1), :], axis=1, keepdims=True)
            prefix = dot(ones, decay, precision=EXACT_PRECISION) + faded
            out, reach, total, state = block_step(query, key, values[g, at, :], prefix, mask, state)
            out_ref[at, :] = out
            reach_ref[at, :] = (reach * jnp.exp(running)).astype(BF16)
            left.append((state, running + total))
        return tuple(left)

    start = tuple(
        (
            jnp.zeros((values.shape[2], group[2].shape[1]), F32),
            jnp.zeros((1, group[2].shape[1]), F32),
        )
        for group in groups
    )
    (wide_state, wide_log), (narrow_state, narrow_log) = lax.fori_loop(
        0, length // BLOCK, advance, start, unroll=4
    )
    packed = jnp.concatenate([narrow_state[0:64], narrow_state[64:128]], axis=1)
    narrow_log = jnp.concatenate([narrow_log, narrow_log], axis=1)

    store_state(core_states, core, (wide_log, narrow_log, wide_state, packed))
    src = core_states.at[core]
    send(src, src, s_send.at[0], s_recv.at[0], partner)
    x_relay(sources, 0)
    arrived(core_states.at[other], s_recv.at[0])
    first = load_state(core_states, 0)
    nothing = jax.tree.map(jnp.zeros_like, first)
    entering = selected(core == 1, first, nothing)
    total = combine(first, load_state(core_states, 1))
    for base, ref, name, here in ((1, y_states, "sp_1", y), (5, z_states, "sp_0", z)):
        store_state(ref, here, total)
        src = ref.at[here]
        for step in (1, 3, 2):
            send(src, src, s_send.at[base + step - 1], s_recv.at[base + here], {name: turn(here, step)})
        if base == 5:
            pump(ARRIVALS[0:8])
        for step in (1, 3, 2):
            peer = turn(here, step)
            arrived(ref.at[peer], s_recv.at[base + peer])
        inside, total = (nothing, nothing)
        for k in range(RING):
            total = combine(total, load_state(ref, k))
            inside = selected(k < here, total, inside)
        entering = combine(inside, entering)
    _, _, wide_state, packed = entering
    narrow_state = jnp.concatenate([packed[:, 0:64], packed[:, 64:128]], axis=0).astype(BF16)
    wide_state = wide_state.astype(BF16)

    for n in range(RING):
        at = pl.ds(n * rows, rows)
        parts = []
        for g, (out_ref, reach_ref, state) in enumerate(
            ((wide_out, wide_reach, wide_state), (narrow_out, narrow_reach, narrow_state))
        ):
            out = out_ref[at, :] + dot(reach_ref[at, :], state, NT)
            inverse = lax.rsqrt(jnp.mean(out * out, axis=1, keepdims=True) + EPSILON)
            out = out * inverse * channel_norm_scale[...]
            parts.append((out * jax.nn.silu(switches[g, at, :].astype(F32))).astype(BF16))
        mixed[x, at, :] = jnp.concatenate(parts, axis=1)
        if n % 2 == 1:
            x_start(mixed, 8, n // 2)

    pump(ARRIVALS[8:22])
    x_relay(mixed, 8)
    pump(ARRIVALS[22:])
    x_finish(sources, 0)
    x_finish(mixed, 8)
    for copy in loads[first_loads:]:
        copy.wait()

    def emit(owner):
        at = pl.ds(pl.multiple_of(owner * rows, rows), rows)
        left = jnp.concatenate([mixed[t, at, :] for t in range(RING)], axis=1)

        def tile(n, squares):
            cols = pl.ds(pl.multiple_of(n * 512, 512), 512)
            found = dot(left, projection[:, :, cols].reshape(4 * 256, 512))
            found = found + sources[owner, :, cols].astype(F32)
            updated[:, cols] = found
            found = found * found
            return squares + (
                (found[:, 0:128] + found[:, 128:256]) + (found[:, 256:384] + found[:, 384:512])
            )

        squares = lax.fori_loop(0, model // 512, tile, jnp.zeros((rows, 128), F32))
        mean = jnp.sum(squares, axis=1, keepdims=True) / model
        inverse = lax.rsqrt(mean + EPSILON)

        def scale(n, carry):
            cols = pl.ds(pl.multiple_of(n * 512, 512), 512)
            normed[:, cols] = (updated[:, cols] * inverse * mlp_scale[:, cols]).astype(BF16)
            return carry

        lax.fori_loop(0, model // 512, scale, 0)

    def feed_forward(out_ref):
        def widen(n, carry):
            cols = pl.ds(pl.multiple_of(n * 256, 256), 256)
            both = dot(normed[...], weights[:, :, cols].reshape(model, 256))
            found = (jax.nn.silu(both[:, 0:128]) * both[:, 128:256]).astype(BF16)
            hidden[:, pl.ds(pl.multiple_of(n * 128, 128), 128)] = found
            return carry

        lax.fori_loop(0, ff // 128, widen, 0)

        def shrink(n, carry):
            cols = pl.ds(pl.multiple_of(n * 256, 256), 256)
            four = weights[pl.ds(n * 4, 4), :, pl.ds(2 * ff, ff)].reshape(256, ff)
            out_ref[:, cols] = dot(hidden[...], four, NT).astype(out_ref.dtype)
            return carry

        lax.fori_loop(0, model // 256, shrink, 0)

    half = rows // 2
    upper, lower = (pl.ds(0, half), pl.ds(half, half))

    emit(turn(x, 2))
    for i in range(RING):
        for j in range(RING):
            for h in range(2):
                arrived(shard(i, j, h, other), d_recv.at[mark(i, j, h)])
    feed_forward(partial.at[0])
    send(partial.at[0, upper], passing.at[0], r_send.at[0], r_recv.at[0], {"tp": turn(x, 1)})
    send(partial.at[0, lower], passing.at[1], r_send.at[1], r_recv.at[1], {"tp": turn(x, 3)})
    emit(turn(x, 1))
    feed_forward(partial.at[1])
    send(partial.at[1, lower], landed.at[0, lower], r_send.at[2], r_recv.at[2], {"tp": turn(x, 1)})
    arrived(passing.at[0], r_recv.at[0])
    partial[1, upper, :] = (
        partial[1, upper, :].astype(F32) + passing[0].astype(F32)
    ).astype(BF16)
    send(partial.at[1, upper], landed.at[0, upper], r_send.at[3], r_recv.at[3], {"tp": turn(x, 1)})
    emit(turn(x, 3))
    feed_forward(partial.at[2])
    send(partial.at[2, upper], landed.at[1, upper], r_send.at[4], r_recv.at[4], {"tp": turn(x, 3)})
    arrived(passing.at[1], r_recv.at[1])
    partial[2, lower, :] = (
        partial[2, lower, :].astype(F32) + passing[1].astype(F32)
    ).astype(BF16)
    send(partial.at[2, lower], landed.at[1, lower], r_send.at[5], r_recv.at[5], {"tp": turn(x, 3)})
    emit(x)
    feed_forward(own_part)
    for n, (k, part) in enumerate(((0, lower), (0, upper), (1, upper), (1, lower))):
        arrived(landed.at[k, part], r_recv.at[2 + n])

    def finish(n, carry):
        cols = pl.ds(pl.multiple_of(n * 256, 256), 256)
        summed = own_part[:, cols] + (landed[0, :, cols].astype(F32) + landed[1, :, cols].astype(F32))
        layer_out[:, cols] = (updated[:, cols] + 0.5 * summed).astype(BF16)
        return carry

    lax.fori_loop(0, model // 256, finish, 0)
    for copy in sent:
        copy.wait_send()


def local(
    layer_source,
    broad_probe_tensor,
    broad_retention_preact,
    broad_floor_margin,
    slim_probe_tensor,
    slim_retention_preact,
    slim_floor_margin,
    branch_content_tensor,
    emitted_switch_preact,
    extra_log_fades,
    channel_norm_scale,
    emission_projection,
    mlp_norm_scale,
    switch_projection,
    expand_projection,
    shrink_projection,
):
    rows, model = layer_source.shape
    length = broad_probe_tensor.shape[0]
    depth, ff = switch_projection.shape
    vmem = pl.BlockSpec(memory_space=pltpu.VMEM)
    far = pl.BlockSpec(memory_space=pl.ANY)
    dma = pltpu.SemaphoreType.DMA
    return pl.pallas_call(
        layer_kernel,
        out_shape=jax.ShapeDtypeStruct((rows, model), BF16),
        in_specs=[far] + [vmem] * 10 + [far, vmem, far, far, far],
        out_specs=vmem,
        scratch_shapes=[
            pltpu.VMEM((32, depth, 3 * ff), BF16),
            pltpu.VMEM((RING, rows, model), BF16),
            pltpu.VMEM((RING, length, 256), BF16),
            pltpu.VMEM((RING, 256, model), BF16),
            pltpu.VMEM((rows, model), F32),
            pltpu.VMEM((rows, model), BF16),
            pltpu.VMEM((rows, ff), BF16),
            pltpu.VMEM((3, rows, model), BF16),
            pltpu.VMEM((rows, model), F32),
            pltpu.VMEM((2, rows // 2, model), BF16),
            pltpu.VMEM((2, rows, model), BF16),
            pltpu.VMEM((length, 64), F32),
            pltpu.VMEM((length, 64), F32),
            pltpu.VMEM((length, 128), F32),
            pltpu.VMEM((length, 128), F32),
            pltpu.VMEM((length, 128), BF16),
            pltpu.VMEM((length, 64), BF16),
            pltpu.VMEM((2, 208, 128), BF16),
            pltpu.VMEM((RING, 208, 128), BF16),
            pltpu.VMEM((RING, 208, 128), BF16),
            dma((32,)),
            dma((30,)),
            dma((32,)),
            dma((32,)),
            dma((32,)),
            dma((12,)),
            dma((16,)),
            dma((9,)),
            dma((9,)),
            dma((6,)),
            dma((6,)),
        ],
        compiler_params=pltpu.CompilerParams(
            collective_id=0, has_side_effects=True, vmem_limit_bytes=62 * 1024 * 1024
        ),
    )(
        layer_source,
        broad_probe_tensor,
        broad_retention_preact,
        broad_floor_margin.reshape(1, -1),
        slim_probe_tensor.T,
        slim_retention_preact.T,
        slim_floor_margin.reshape(1, -1),
        branch_content_tensor,
        emitted_switch_preact,
        extra_log_fades.reshape(2, length // BLOCK, BLOCK),
        channel_norm_scale.reshape(1, -1),
        emission_projection,
        mlp_norm_scale.reshape(1, -1),
        switch_projection,
        expand_projection,
        shrink_projection.T,
    )


def solution(mesh):
    torus = Mesh(mesh.devices.reshape(4, 4, 2, mesh.shape["tp"]), SP_TP)
    placed = (
        P(SP_TP, None),
        P(SP, "tp"),
        P(SP, "tp"),
        P("tp"),
        P(SP, "tp"),
        P(SP, "tp"),
        P("tp"),
        P(None, SP, "tp"),
        P(None, SP, "tp"),
        P(None, SP, "tp"),
        P(),
        P(),
        P(),
        P(SP, "tp"),
        P(SP, "tp"),
        P("tp", SP),
    )
    return jax.shard_map(
        local, mesh=torus, in_specs=placed, out_specs=P(SP_TP, None), check_vma=False
    )
```

```python
import jax
import jax.numpy as jnp
from jax import lax
from jax.experimental import pallas as pl
from jax.experimental.pallas import tpu as pltpu
from jax.sharding import Mesh
from jax.sharding import PartitionSpec as P

BLOCK = 64
RING = 4
SP = ("sp_0", "sp_1", "sp_2")
SP_TP = ("sp_0", "sp_1", "sp_2", "tp")

EPSILON = 1e-06
EXACT_PRECISION = lax.Precision.HIGHEST
BF16 = jnp.bfloat16
F32 = jnp.float32
NT = (((1,), (1,)), ((), ()))
TN = (((0,), (0,)), ((), ()))
MESH = pl.DeviceIdType.MESH

ARRIVALS = (
    (3, 0, 0),
    (1, 0, 1),
    (0, 3, 0),
    (0, 1, 1),
    (3, 0, 1),
    (1, 0, 0),
    (0, 3, 1),
    (0, 1, 0),
    (2, 0, 0),
    (2, 0, 1),
    (3, 3, 0),
    (3, 1, 1),
    (1, 3, 0),
    (1, 1, 1),
    (3, 3, 1),
    (3, 1, 0),
    (0, 2, 0),
    (0, 2, 1),
    (1, 3, 1),
    (1, 1, 0),
    (2, 3, 0),
    (2, 1, 1),
    (2, 3, 1),
    (2, 1, 0),
    (3, 2, 0),
    (3, 2, 1),
    (1, 2, 0),
    (1, 2, 1),
    (2, 2, 0),
    (2, 2, 1),
)


def turn(value, step):
    return lax.rem(value + step, RING)


def dot(a, b, dims=(((1,), (0,)), ((), ())), precision=None):
    return lax.dot_general(a, b, dims, preferred_element_type=F32, precision=precision)


def combine(earlier, later):
    wide_early, narrow_early, wide_state_early, narrow_state_early = earlier
    wide_late, narrow_late, wide_state_late, narrow_state_late = later
    return (
        wide_early + wide_late,
        narrow_early + narrow_late,
        jnp.exp(wide_late) * wide_state_early + wide_state_late,
        jnp.exp(narrow_late) * narrow_state_early + narrow_state_late,
    )


def split_log(log):
    first = log.astype(BF16).astype(F32)
    second = (log - first).astype(BF16).astype(F32)
    return [first, second, log - first - second]


def store_state(ref, at, state):
    wide, narrow, wide_state, narrow_state = state
    ref[at, 0:128, :] = wide_state.astype(BF16)
    ref[at, 128:192, :] = narrow_state.astype(BF16)
    lines = split_log(wide) + split_log(narrow)
    lines.append(jnp.zeros((10, wide.shape[1]), F32))
    ref[at, 192:208, :] = jnp.concatenate(lines, axis=0).astype(BF16)


def load_state(ref, at):
    lines = ref[at, 192:208, :].astype(F32)
    wide = lines[0:1] + lines[1:2] + lines[2:3]
    narrow = lines[3:4] + lines[4:5] + lines[5:6]
    return (wide, narrow, ref[at, 0:128, :].astype(F32), ref[at, 128:192, :].astype(F32))


def selected(passed, new, old):
    return jax.tree.map(lambda a, b: jnp.where(passed, a, b), new, old)


def block_step(query, key, value, prefix, mask, state):
    half = BLOCK // 2
    middle, total = (prefix[half - 1 : half, :], prefix[BLOCK - 1 : BLOCK, :])
    query_in = query * jnp.exp(prefix - middle)
    key_in = key * jnp.exp(middle - prefix)
    scores = dot(query_in.astype(BF16), key_in.astype(BF16), NT)
    scores = jnp.where(mask, scores, 0.0).astype(BF16)
    inside = dot(scores, value)
    reach = query_in * jnp.exp(middle)
    earlier = dot(reach.astype(BF16), state.astype(BF16), NT)
    leaving = (key_in * jnp.exp(total - middle)).astype(BF16)
    state = state * jnp.exp(total) + dot(value, leaving, TN)
    return (inside + earlier, reach, total, state)


def layer_kernel(
    layer_source,
    wide_query,
    wide_forget,
    wide_gap,
    narrow_query,
    narrow_forget,
    narrow_gap,
    values,
    switches,
    fades,
    channel_norm_scale,
    emission,
    mlp_scale,
    gate_shard,
    up_shard,
    down_shard,
    layer_out,
    weights,
    sources,
    mixed,
    projection,
    updated,
    normed,
    hidden,
    partial,
    own_part,
    passing,
    landed,
    narrow_q,
    narrow_f,
    wide_out,
    narrow_out,
    wide_reach,
    narrow_reach,
    core_states,
    y_states,
    z_states,
    load_sem,
    w_send,
    w_recv,
    d_send,
    d_recv,
    x_send,
    x_recv,
    s_send,
    s_recv,
    r_send,
    r_recv,
):
    z, y, core, x = (lax.axis_index(name) for name in SP_TP)
    other = 1 - core
    rows, model = layer_source.shape
    length = wide_query.shape[0]
    ff = gate_shard.shape[1]
    depth = gate_shard.shape[0]
    sent = []

    def send(src, dst, send_sem, recv_sem, to):
        copy = pltpu.make_async_remote_copy(
            src_ref=src,
            dst_ref=dst,
            send_sem=send_sem,
            recv_sem=recv_sem,
            device_id=to,
            device_id_type=MESH,
        )
        copy.start()
        sent.append(copy)

    partner = {"sp_2": other}

    def arrived(ref, sem):
        pltpu.make_async_remote_copy(
            src_ref=ref,
            dst_ref=ref,
            send_sem=sem,
            recv_sem=sem,
            device_id=partner,
            device_id_type=MESH,
        ).wait_recv()

    def place(i, j, of_core):
        first = jnp.where(of_core == 0, y, z)
        second = jnp.where(of_core == 0, z, y)
        first, second = (turn(first, i), turn(second, j))
        return (
            jnp.where(of_core == 0, second, first),
            jnp.where(of_core == 0, first, second),
        )

    def slot(i, j, of_core):
        at_z, at_y = place(i, j, of_core)
        return at_z * 8 + at_y * 2 + of_core

    half_depth = depth // 2

    columns_of = (pl.ds(0, 2 * ff), pl.ds(2 * ff, ff))

    def shard(i, j, h, part, of_core):
        lines = pl.ds(h * half_depth, half_depth)
        return weights.at[slot(i, j, of_core), lines, columns_of[part]]

    def shard_part(i, j, part, of_core):
        return weights.at[slot(i, j, of_core), :, columns_of[part]]

    def toward(i, j):
        at_z, at_y = place(i, j, core)
        return {"sp_0": at_z, "sp_1": at_y}

    def mark(i, j, h, part):
        return part * 32 + (i * 4 + j) * 2 + h

    counts = {"w": 0, "x": 0}

    def next_of(name):
        counts[name] += 1
        return counts[name] - 1

    def forward(i, j, h, part, step, landing):
        src = shard(i, j, h, part, core)
        at = w_recv.at[mark(*landing, h, part)]
        send(src, src, w_send.at[next_of("w")], at, toward(*step))

    def hand_over(i, j, part):
        src = shard_part(i, j, part, core)
        k = part * 16 + i * 4 + j
        send(src, src, d_send.at[k], d_recv.at[k], partner)

    handed = {}

    def pump(part, first, last):
        for i, j, h in ARRIVALS[first:last]:
            arrived(shard(i, j, h, part, core), w_recv.at[mark(i, j, h, part)])
            if j == 0:
                if (i, h) == (3, 0):
                    forward(i, 0, h, part, (1, 0), (2, 0))
                if (i, h) == (1, 1):
                    forward(i, 0, h, part, (3, 0), (2, 0))
                forward(i, 0, h, part, (0, 1), (i, 3))
                forward(i, 0, h, part, (0, 3), (i, 1))
            else:
                if (j, h) == (3, 0):
                    forward(i, j, h, part, (0, 1), (i, 2))
                if (j, h) == (1, 1):
                    forward(i, j, h, part, (0, 3), (i, 2))
            handed[(i, j, part)] = handed.get((i, j, part), 0) + 1
            if handed[(i, j, part)] == 2:
                hand_over(i, j, part)

    def start_weights(part):
        for h in range(2):
            forward(0, 0, h, part, (1, 0), (3, 0))
            forward(0, 0, 1 - h, part, (3, 0), (1, 0))
            forward(0, 0, h, part, (0, 1), (0, 3))
            forward(0, 0, 1 - h, part, (0, 3), (0, 1))
        hand_over(0, 0, part)

    def wait_partner(part):
        for i in range(RING):
            for j in range(RING):
                arrived(shard_part(i, j, part, other), d_recv.at[part * 16 + i * 4 + j])

    def x_piece(buffer, step, h):
        half = buffer.shape[1] // 2
        return buffer.at[turn(x, step), pl.ds(h * half, half), :]

    def x_forward(buffer, base, step, h, to, landing):
        src = x_piece(buffer, step, h)
        send(src, src, x_send.at[next_of("x")], x_recv.at[base + landing * 2 + h], {"tp": turn(x, to)})

    def x_wait(buffer, base, step, h):
        arrived(x_piece(buffer, step, h), x_recv.at[base + step * 2 + h])

    def x_first(buffer, base):
        x_forward(buffer, base, 0, 0, 1, 3)
        x_forward(buffer, base, 0, 1, 3, 1)

    def x_second(buffer, base):
        x_forward(buffer, base, 0, 1, 1, 3)
        x_forward(buffer, base, 0, 0, 3, 1)

    def x_relay(buffer, base):
        x_wait(buffer, base, 3, 0)
        x_forward(buffer, base, 3, 0, 1, 2)
        x_wait(buffer, base, 1, 1)
        x_forward(buffer, base, 1, 1, 3, 2)

    def x_opposite(buffer, base):
        x_wait(buffer, base, 2, 0)
        x_wait(buffer, base, 2, 1)

    def x_rest(buffer, base):
        x_wait(buffer, base, 3, 1)
        x_wait(buffer, base, 1, 0)

    me = slot(0, 0, core)
    loads = []

    def load(src, dst):
        copy = pltpu.make_async_copy(src, dst, load_sem.at[len(loads)])
        copy.start()
        loads.append(copy)

    for n in range(ff // 128):
        cols = pl.ds(n * 128, 128)
        load(gate_shard.at[:, cols], weights.at[me, :, pl.ds(n * 256, 128)])
        load(up_shard.at[:, cols], weights.at[me, :, pl.ds(n * 256 + 128, 128)])
    load(down_shard, weights.at[me, :, pl.ds(2 * ff, ff)])
    load(layer_source, sources.at[x])
    first_loads = len(loads)
    for t in range(RING):
        for g in range(2):
            load(emission.at[g, pl.ds(t * 128, 128), :], projection.at[t, pl.ds(g * 128, 128), :])

    barrier = pltpu.get_barrier_semaphore()
    pl.semaphore_signal(barrier, inc=1, device_id=partner, device_id_type=MESH)
    for name, here in (("sp_0", z), ("sp_1", y), ("tp", x)):
        for step in (1, 2, 3):
            pl.semaphore_signal(
                barrier, inc=1, device_id={name: turn(here, step)}, device_id_type=MESH
            )
    pl.semaphore_wait(barrier, 10)

    for copy in loads[:first_loads]:
        copy.wait()
    start_weights(0)
    x_first(sources, 0)
    for n in range(length // 128):
        cols = pl.ds(n * 128, 128)
        narrow_q[cols, :] = narrow_query[:, cols].astype(F32).T
        narrow_f[cols, :] = narrow_forget[:, cols].astype(F32).T
    line = lax.broadcasted_iota(jnp.int32, (BLOCK, BLOCK), 0)
    column = lax.broadcasted_iota(jnp.int32, (BLOCK, BLOCK), 1)
    mask = line >= column
    ones = jnp.where(mask, 1.0, 0.0)
    groups = (
        (wide_query, wide_forget, wide_gap, wide_out, wide_reach),
        (narrow_q, narrow_f, narrow_gap, narrow_out, narrow_reach),
    )

    def advance(pair, carried):
        for b in range(2):
            at = pl.ds(pl.multiple_of((pair * 2 + b) * BLOCK, BLOCK), BLOCK)
            left = []
            for g in range(2):
                query_ref, forget_ref, gap_ref, out_ref, reach_ref = groups[g]
                state, running = carried[g]
                key = gap_ref[...] * jax.nn.sigmoid(-forget_ref[at, :].astype(F32))
                decay = jnp.log1p(-key)
                query = jax.nn.silu(query_ref[at, :].astype(F32)) * key.shape[1] ** (-0.5)
                fade = fades[g, :, pl.ds(pl.multiple_of(pair * 2 * BLOCK, 2 * BLOCK), 2 * BLOCK)]
                faded = jnp.sum(ones * fade[:, b * BLOCK : (b + 1) * BLOCK], axis=1, keepdims=True)
                prefix = dot(ones, decay, precision=EXACT_PRECISION) + faded
                out, reach, total, state = block_step(
                    query, key, values[g, at, :], prefix, mask, state
                )
                out_ref[at, :] = out
                reach_ref[at, :] = (reach * jnp.exp(running)).astype(BF16)
                left.append((state, running + total))
            carried = tuple(left)
        return carried

    start = tuple(
        (
            jnp.zeros((values.shape[2], group[2].shape[1]), F32),
            jnp.zeros((1, group[2].shape[1]), F32),
        )
        for group in groups
    )
    pairs = length // (2 * BLOCK)
    middle = lax.fori_loop(0, pairs // 2, advance, start, unroll=2)
    pump(0, 0, 4)
    (wide_state, wide_log), (narrow_state, narrow_log) = lax.fori_loop(
        pairs // 2, pairs, advance, middle, unroll=2
    )
    packed = jnp.concatenate([narrow_state[0:64], narrow_state[64:128]], axis=1)
    narrow_log = jnp.concatenate([narrow_log, narrow_log], axis=1)

    store_state(core_states, core, (wide_log, narrow_log, wide_state, packed))
    src = core_states.at[core]
    send(src, src, s_send.at[0], s_recv.at[0], partner)
    arrived(core_states.at[other], s_recv.at[0])
    first = load_state(core_states, 0)
    nothing = jax.tree.map(jnp.zeros_like, first)
    entering = selected(core == 1, first, nothing)
    total = combine(first, load_state(core_states, 1))
    for base, ref, name, here in ((1, y_states, "sp_1", y), (5, z_states, "sp_0", z)):
        store_state(ref, here, total)
        src = ref.at[here]
        for step in (1, 3, 2):
            send(src, src, s_send.at[base + step - 1], s_recv.at[base + here], {name: turn(here, step)})
        if base == 1:
            x_relay(sources, 0)
        else:
            start_weights(1)
            pump(0, 4, 10)
        for step in (1, 3, 2):
            peer = turn(here, step)
            arrived(ref.at[peer], s_recv.at[base + peer])
        inside, total = (nothing, nothing)
        for k in range(RING):
            total = combine(total, load_state(ref, k))
            inside = selected(k < here, total, inside)
        entering = combine(inside, entering)
    _, _, wide_state, packed = entering
    narrow_state = jnp.concatenate([packed[:, 0:64], packed[:, 64:128]], axis=0).astype(BF16)
    wide_state = wide_state.astype(BF16)

    for n in range(RING):
        at = pl.ds(n * rows, rows)
        parts = []
        for g, (out_ref, reach_ref, state) in enumerate(
            ((wide_out, wide_reach, wide_state), (narrow_out, narrow_reach, narrow_state))
        ):
            out = out_ref[at, :] + dot(reach_ref[at, :], state, NT)
            inverse = lax.rsqrt(jnp.mean(out * out, axis=1, keepdims=True) + EPSILON)
            out = out * inverse * channel_norm_scale[...]
            parts.append((out * jax.nn.silu(switches[g, at, :].astype(F32))).astype(BF16))
        mixed[x, at, :] = jnp.concatenate(parts, axis=1)

    x_first(mixed, 8)
    x_second(mixed, 8)

    pump(0, 10, 24)
    x_relay(mixed, 8)
    x_second(sources, 0)
    pump(0, 24, 30)
    pump(1, 0, 18)
    x_rest(mixed, 8)
    x_opposite(mixed, 8)
    x_opposite(sources, 0)
    for copy in loads[first_loads:]:
        copy.wait()

    half = rows // 2
    upper, lower = (pl.ds(0, half), pl.ds(half, half))

    def emit(pieces):
        def lines(owner, h):
            return pl.ds(pl.multiple_of(owner * rows + h * half, half), half)

        left = jnp.concatenate(
            [
                jnp.concatenate([mixed[t, lines(owner, h), :] for owner, h in pieces], axis=0)
                for t in range(RING)
            ],
            axis=1,
        )

        def tile(n, squares):
            cols = pl.ds(pl.multiple_of(n * 512, 512), 512)
            found = dot(left, projection[:, :, cols].reshape(4 * 256, 512))
            source = [sources[owner, pl.ds(h * half, half), cols] for owner, h in pieces]
            found = found + jnp.concatenate(source, axis=0).astype(F32)
            updated[:, cols] = found
            found = found * found
            return squares + (
                (found[:, 0:128] + found[:, 128:256]) + (found[:, 256:384] + found[:, 384:512])
            )

        squares = lax.fori_loop(0, model // 512, tile, jnp.zeros((rows, 128), F32))
        mean = jnp.sum(squares, axis=1, keepdims=True) / model
        inverse = lax.rsqrt(mean + EPSILON)

        def scale(n, carry):
            cols = pl.ds(pl.multiple_of(n * 512, 512), 512)
            normed[:, cols] = (updated[:, cols] * inverse * mlp_scale[:, cols]).astype(BF16)
            return carry

        lax.fori_loop(0, model // 512, scale, 0)

    def widen_all():
        def widen(n, carry):
            cols = pl.ds(pl.multiple_of(n * 256, 256), 256)
            both = dot(normed[...], weights[:, :, cols].reshape(model, 256))
            found = (jax.nn.silu(both[:, 0:128]) * both[:, 128:256]).astype(BF16)
            hidden[:, pl.ds(pl.multiple_of(n * 128, 128), 128)] = found
            return carry

        lax.fori_loop(0, ff // 128, widen, 0)

    def shrink_all(out_ref, passed=False):
        def shrink(n, carry):
            cols = pl.ds(pl.multiple_of(n * 256, 256), 256)
            four = weights[pl.ds(n * 4, 4), :, pl.ds(2 * ff, ff)].reshape(256, ff)
            found = dot(hidden[...], four, NT)
            if passed:
                found = found + jnp.concatenate(
                    [passing[0, :, cols], passing[1, :, cols]], axis=0
                ).astype(F32)
            out_ref[:, cols] = found.astype(out_ref.dtype)
            return carry

        lax.fori_loop(0, model // 256, shrink, 0)

    def send_sum(src, dst, k, step):
        send(src, dst, r_send.at[k], r_recv.at[k], {"tp": turn(x, step)})

    left_x, right_x = (turn(x, 3), turn(x, 1))

    emit(((turn(x, 2), 0), (turn(x, 2), 1)))
    pump(1, 18, 30)
    wait_partner(0)
    widen_all()
    wait_partner(1)
    shrink_all(partial.at[0])
    send_sum(partial.at[0, upper], passing.at[0], 0, 1)
    send_sum(partial.at[0, lower], passing.at[1], 1, 3)
    emit(((right_x, 1), (left_x, 0)))
    widen_all()
    shrink_all(partial.at[1])
    send_sum(partial.at[1, upper], landed.at[0, lower], 2, 1)
    send_sum(partial.at[1, lower], landed.at[1, upper], 3, 3)
    x_rest(sources, 0)
    emit(((right_x, 0), (left_x, 1)))
    widen_all()
    arrived(passing.at[0], r_recv.at[0])
    arrived(passing.at[1], r_recv.at[1])
    shrink_all(partial.at[2], passed=True)
    send_sum(partial.at[2, upper], landed.at[0, upper], 4, 1)
    send_sum(partial.at[2, lower], landed.at[1, lower], 5, 3)
    emit(((x, 0), (x, 1)))
    widen_all()
    shrink_all(own_part)
    for n, (k, part) in enumerate(((0, lower), (1, upper), (0, upper), (1, lower))):
        arrived(landed.at[k, part], r_recv.at[2 + n])

    def finish(n, carry):
        cols = pl.ds(pl.multiple_of(n * 256, 256), 256)
        summed = own_part[:, cols] + (landed[0, :, cols].astype(F32) + landed[1, :, cols].astype(F32))
        layer_out[:, cols] = (updated[:, cols] + 0.5 * summed).astype(BF16)
        return carry

    lax.fori_loop(0, model // 256, finish, 0)
    for copy in sent:
        copy.wait_send()


def local(
    layer_source,
    broad_probe_tensor,
    broad_retention_preact,
    broad_floor_margin,
    slim_probe_tensor,
    slim_retention_preact,
    slim_floor_margin,
    branch_content_tensor,
    emitted_switch_preact,
    extra_log_fades,
    channel_norm_scale,
    emission_projection,
    mlp_norm_scale,
    switch_projection,
    expand_projection,
    shrink_projection,
):
    rows, model = layer_source.shape
    length = broad_probe_tensor.shape[0]
    depth, ff = switch_projection.shape
    vmem = pl.BlockSpec(memory_space=pltpu.VMEM)
    far = pl.BlockSpec(memory_space=pl.ANY)
    dma = pltpu.SemaphoreType.DMA
    return pl.pallas_call(
        layer_kernel,
        out_shape=jax.ShapeDtypeStruct((rows, model), BF16),
        in_specs=[far] + [vmem] * 10 + [far, vmem, far, far, far],
        out_specs=vmem,
        scratch_shapes=[
            pltpu.VMEM((32, depth, 3 * ff), BF16),
            pltpu.VMEM((RING, rows, model), BF16),
            pltpu.VMEM((RING, length, 256), BF16),
            pltpu.VMEM((RING, 256, model), BF16),
            pltpu.VMEM((rows, model), F32),
            pltpu.VMEM((rows, model), BF16),
            pltpu.VMEM((rows, ff), BF16),
            pltpu.VMEM((3, rows, model), BF16),
            pltpu.VMEM((rows, model), F32),
            pltpu.VMEM((2, rows // 2, model), BF16),
            pltpu.VMEM((2, rows, model), BF16),
            pltpu.VMEM((length, 64), F32),
            pltpu.VMEM((length, 64), F32),
            pltpu.VMEM((length, 128), F32),
            pltpu.VMEM((length, 128), F32),
            pltpu.VMEM((length, 128), BF16),
            pltpu.VMEM((length, 64), BF16),
            pltpu.VMEM((2, 208, 128), BF16),
            pltpu.VMEM((RING, 208, 128), BF16),
            pltpu.VMEM((RING, 208, 128), BF16),
            dma((32,)),
            dma((60,)),
            dma((64,)),
            dma((32,)),
            dma((32,)),
            dma((12,)),
            dma((16,)),
            dma((9,)),
            dma((9,)),
            dma((6,)),
            dma((6,)),
        ],
        compiler_params=pltpu.CompilerParams(
            collective_id=0, has_side_effects=True, vmem_limit_bytes=62 * 1024 * 1024
        ),
    )(
        layer_source,
        broad_probe_tensor,
        broad_retention_preact,
        broad_floor_margin.reshape(1, -1),
        slim_probe_tensor.T,
        slim_retention_preact.T,
        slim_floor_margin.reshape(1, -1),
        branch_content_tensor,
        emitted_switch_preact,
        jnp.swapaxes(extra_log_fades, 1, 2),
        channel_norm_scale.reshape(1, -1),
        emission_projection,
        mlp_norm_scale.reshape(1, -1),
        switch_projection,
        expand_projection,
        shrink_projection.T,
    )


def solution(mesh):
    torus = Mesh(mesh.devices.reshape(4, 4, 2, mesh.shape["tp"]), SP_TP)
    placed = (
        P(SP_TP, None),
        P(SP, "tp"),
        P(SP, "tp"),
        P("tp"),
        P(SP, "tp"),
        P(SP, "tp"),
        P("tp"),
        P(None, SP, "tp"),
        P(None, SP, "tp"),
        P(None, SP, "tp"),
        P(),
        P(),
        P(),
        P(SP, "tp"),
        P(SP, "tp"),
        P("tp", SP),
    )
    return jax.shard_map(
        local, mesh=torus, in_specs=placed, out_specs=P(SP_TP, None), check_vma=False
    )
```

```python
import jax
import jax.numpy as jnp
from jax import lax
from jax.experimental import pallas as pl
from jax.experimental.pallas import tpu as pltpu
from jax.sharding import Mesh
from jax.sharding import PartitionSpec as P

BLOCK = 64
RING = 4
SP = ("sp_0", "sp_1", "sp_2")
SP_TP = ("sp_0", "sp_1", "sp_2", "tp")

EPSILON = 1e-06
EXACT_PRECISION = lax.Precision.HIGHEST
BF16 = jnp.bfloat16
F32 = jnp.float32
NT = (((1,), (1,)), ((), ()))
TN = (((0,), (0,)), ((), ()))
MESH = pl.DeviceIdType.MESH

NEAR = ((3, 0, 0), (1, 0, 1), (0, 3, 0), (0, 1, 1), (3, 0, 1), (1, 0, 0))
ACROSS = ((2, 0, 0), (2, 0, 1))
CORNERS = ((3, 3, 0), (3, 1, 1), (1, 3, 0), (1, 1, 1), (2, 3, 0), (2, 1, 1))
SIDES = ((0, 3, 1), (0, 1, 0))
EDGES = ((3, 3, 1), (3, 1, 0), (0, 2, 0), (0, 2, 1), (1, 3, 1), (1, 1, 0))
ENDS = ((2, 3, 1), (2, 1, 0), (3, 2, 0), (3, 2, 1))
FAR = ((1, 2, 0), (1, 2, 1), (2, 2, 0), (2, 2, 1))


def turn(value, step):
    return lax.rem(value + step, RING)


def dot(a, b, dims=(((1,), (0,)), ((), ())), precision=None):
    return lax.dot_general(a, b, dims, preferred_element_type=F32, precision=precision)


def combine(earlier, later):
    wide_early, narrow_early, wide_state_early, narrow_state_early = earlier
    wide_late, narrow_late, wide_state_late, narrow_state_late = later
    return (
        wide_early + wide_late,
        narrow_early + narrow_late,
        jnp.exp(wide_late) * wide_state_early + wide_state_late,
        jnp.exp(narrow_late) * narrow_state_early + narrow_state_late,
    )


def split_log(log):
    first = log.astype(BF16).astype(F32)
    second = (log - first).astype(BF16).astype(F32)
    return [first, second, log - first - second]


def store_state(ref, at, state):
    wide, narrow, wide_state, narrow_state = state
    ref[at, 0:128, :] = wide_state.astype(BF16)
    ref[at, 128:192, :] = narrow_state.astype(BF16)
    lines = split_log(wide) + split_log(narrow)
    lines.append(jnp.zeros((10, wide.shape[1]), F32))
    ref[at, 192:208, :] = jnp.concatenate(lines, axis=0).astype(BF16)


def load_state(ref, at):
    lines = ref[at, 192:208, :].astype(F32)
    wide = lines[0:1] + lines[1:2] + lines[2:3]
    narrow = lines[3:4] + lines[4:5] + lines[5:6]
    return (wide, narrow, ref[at, 0:128, :].astype(F32), ref[at, 128:192, :].astype(F32))


def selected(passed, new, old):
    return jax.tree.map(lambda a, b: jnp.where(passed, a, b), new, old)


def block_step(query, key, value, prefix, mask, state):
    half = BLOCK // 2
    middle, total = (prefix[half - 1 : half, :], prefix[BLOCK - 1 : BLOCK, :])
    query_in = query * jnp.exp(prefix - middle)
    key_in = key * jnp.exp(middle - prefix)
    scores = dot(query_in.astype(BF16), key_in.astype(BF16), NT)
    scores = jnp.where(mask, scores, 0.0).astype(BF16)
    inside = dot(scores, value)
    reach = query_in * jnp.exp(middle)
    earlier = dot(reach.astype(BF16), state.astype(BF16), NT)
    leaving = (key_in * jnp.exp(total - middle)).astype(BF16)
    state = state * jnp.exp(total) + dot(value, leaving, TN)
    return (inside + earlier, reach, total, state)


def layer_kernel(
    layer_source,
    wide_query,
    wide_forget,
    wide_gap,
    narrow_query,
    narrow_forget,
    narrow_gap,
    values,
    switches,
    fades,
    channel_norm_scale,
    emission,
    mlp_scale,
    gate_shard,
    up_shard,
    down_shard,
    layer_out,
    weights,
    sources,
    mixed,
    projection,
    updated,
    normed,
    hidden,
    partial,
    own_part,
    passing,
    landed,
    narrow_q,
    narrow_f,
    wide_out,
    narrow_out,
    wide_reach,
    narrow_reach,
    core_states,
    y_states,
    z_states,
    load_sem,
    w_send,
    w_recv,
    d_send,
    d_recv,
    x_send,
    x_recv,
    s_send,
    s_recv,
    r_send,
    r_recv,
):
    z, y, core, x = (lax.axis_index(name) for name in SP_TP)
    other = 1 - core
    rows, model = layer_source.shape
    length = wide_query.shape[0]
    ff = gate_shard.shape[1]
    depth = gate_shard.shape[0]
    sent = []

    def send(src, dst, send_sem, recv_sem, to):
        copy = pltpu.make_async_remote_copy(
            src_ref=src,
            dst_ref=dst,
            send_sem=send_sem,
            recv_sem=recv_sem,
            device_id=to,
            device_id_type=MESH,
        )
        copy.start()
        sent.append(copy)

    partner = {"sp_2": other}

    def arrived(ref, sem):
        pltpu.make_async_remote_copy(
            src_ref=ref,
            dst_ref=ref,
            send_sem=sem,
            recv_sem=sem,
            device_id=partner,
            device_id_type=MESH,
        ).wait_recv()

    def place(i, j, of_core):
        first = jnp.where(of_core == 0, y, z)
        second = jnp.where(of_core == 0, z, y)
        first, second = (turn(first, i), turn(second, j))
        return (
            jnp.where(of_core == 0, second, first),
            jnp.where(of_core == 0, first, second),
        )

    def slot(i, j, of_core):
        at_z, at_y = place(i, j, of_core)
        return at_z * 8 + at_y * 2 + of_core

    half_depth = depth // 2

    columns_of = (pl.ds(0, 2 * ff), pl.ds(2 * ff, ff))

    def shard(i, j, h, part, of_core):
        lines = pl.ds(h * half_depth, half_depth)
        return weights.at[slot(i, j, of_core), lines, columns_of[part]]

    def shard_part(i, j, part, of_core):
        return weights.at[slot(i, j, of_core), :, columns_of[part]]

    def toward(i, j):
        at_z, at_y = place(i, j, core)
        return {"sp_0": at_z, "sp_1": at_y}

    def mark(i, j, h, part):
        return part * 32 + (i * 4 + j) * 2 + h

    counts = {"w": 0, "x": 0}

    def next_of(name):
        counts[name] += 1
        return counts[name] - 1

    def forward(i, j, h, part, step, landing):
        src = shard(i, j, h, part, core)
        at = w_recv.at[mark(*landing, h, part)]
        send(src, src, w_send.at[next_of("w")], at, toward(*step))

    def hand_over(i, j, part):
        src = shard_part(i, j, part, core)
        k = part * 16 + i * 4 + j
        send(src, src, d_send.at[k], d_recv.at[k], partner)

    handed = {}

    def pump(part, arrivals):
        for i, j, h in arrivals:
            arrived(shard(i, j, h, part, core), w_recv.at[mark(i, j, h, part)])
            if j == 0:
                if (i, h) == (3, 0):
                    forward(i, 0, h, part, (1, 0), (2, 0))
                if (i, h) == (1, 1):
                    forward(i, 0, h, part, (3, 0), (2, 0))
                forward(i, 0, h, part, (0, 1), (i, 3))
                forward(i, 0, h, part, (0, 3), (i, 1))
            else:
                if (j, h) == (3, 0):
                    forward(i, j, h, part, (0, 1), (i, 2))
                if (j, h) == (1, 1):
                    forward(i, j, h, part, (0, 3), (i, 2))
            handed[(i, j, part)] = handed.get((i, j, part), 0) + 1
            if handed[(i, j, part)] == 2:
                hand_over(i, j, part)

    def start_weights(part):
        for h in range(2):
            forward(0, 0, h, part, (1, 0), (3, 0))
            forward(0, 0, 1 - h, part, (3, 0), (1, 0))
            forward(0, 0, h, part, (0, 1), (0, 3))
            forward(0, 0, 1 - h, part, (0, 3), (0, 1))
        hand_over(0, 0, part)

    def wait_partner(part):
        for i in range(RING):
            for j in range(RING):
                arrived(shard_part(i, j, part, other), d_recv.at[part * 16 + i * 4 + j])

    def x_piece(buffer, step, h):
        half = buffer.shape[1] // 2
        return buffer.at[turn(x, step), pl.ds(h * half, half), :]

    def x_forward(buffer, base, step, h, to, landing):
        src = x_piece(buffer, step, h)
        send(src, src, x_send.at[next_of("x")], x_recv.at[base + landing * 2 + h], {"tp": turn(x, to)})

    def x_wait(buffer, base, step, h):
        arrived(x_piece(buffer, step, h), x_recv.at[base + step * 2 + h])

    def x_first(buffer, base):
        x_forward(buffer, base, 0, 0, 1, 3)
        x_forward(buffer, base, 0, 1, 3, 1)

    def x_second(buffer, base):
        x_forward(buffer, base, 0, 1, 1, 3)
        x_forward(buffer, base, 0, 0, 3, 1)

    def x_relay(buffer, base):
        x_wait(buffer, base, 3, 0)
        x_forward(buffer, base, 3, 0, 1, 2)
        x_wait(buffer, base, 1, 1)
        x_forward(buffer, base, 1, 1, 3, 2)

    def x_opposite(buffer, base):
        x_wait(buffer, base, 2, 0)
        x_wait(buffer, base, 2, 1)

    def x_rest(buffer, base):
        x_wait(buffer, base, 3, 1)
        x_wait(buffer, base, 1, 0)

    me = slot(0, 0, core)
    loads = []

    def load(src, dst):
        copy = pltpu.make_async_copy(src, dst, load_sem.at[len(loads)])
        copy.start()
        loads.append(copy)

    for n in range(ff // 128):
        cols = pl.ds(n * 128, 128)
        load(gate_shard.at[:, cols], weights.at[me, :, pl.ds(n * 256, 128)])
        load(up_shard.at[:, cols], weights.at[me, :, pl.ds(n * 256 + 128, 128)])
    load(down_shard, weights.at[me, :, pl.ds(2 * ff, ff)])
    load(layer_source, sources.at[x])
    first_loads = len(loads)
    for t in range(RING):
        for g in range(2):
            load(emission.at[g, pl.ds(t * 128, 128), :], projection.at[t, pl.ds(g * 128, 128), :])

    barrier = pltpu.get_barrier_semaphore()
    pl.semaphore_signal(barrier, inc=1, device_id=partner, device_id_type=MESH)
    for name, here in (("sp_0", z), ("sp_1", y), ("tp", x)):
        for step in (1, 2, 3):
            pl.semaphore_signal(
                barrier, inc=1, device_id={name: turn(here, step)}, device_id_type=MESH
            )
    pl.semaphore_wait(barrier, 10)

    for copy in loads[:first_loads]:
        copy.wait()
    start_weights(0)
    x_first(sources, 0)
    for n in range(length // 128):
        cols = pl.ds(n * 128, 128)
        narrow_q[cols, :] = narrow_query[:, cols].astype(F32).T
        narrow_f[cols, :] = narrow_forget[:, cols].astype(F32).T
    line = lax.broadcasted_iota(jnp.int32, (BLOCK, BLOCK), 0)
    column = lax.broadcasted_iota(jnp.int32, (BLOCK, BLOCK), 1)
    mask = line >= column
    ones = jnp.where(mask, 1.0, 0.0)
    groups = (
        (wide_query, wide_forget, wide_gap, wide_out, wide_reach),
        (narrow_q, narrow_f, narrow_gap, narrow_out, narrow_reach),
    )

    def advance(pair, carried):
        for b in range(2):
            at = pl.ds(pl.multiple_of((pair * 2 + b) * BLOCK, BLOCK), BLOCK)
            left = []
            for g in range(2):
                query_ref, forget_ref, gap_ref, out_ref, reach_ref = groups[g]
                state, running = carried[g]
                key = gap_ref[...] * jax.nn.sigmoid(-forget_ref[at, :].astype(F32))
                decay = jnp.log1p(-key)
                query = jax.nn.silu(query_ref[at, :].astype(F32)) * key.shape[1] ** (-0.5)
                fade = fades[g, :, pl.ds(pl.multiple_of(pair * 2 * BLOCK, 2 * BLOCK), 2 * BLOCK)]
                faded = jnp.sum(ones * fade[:, b * BLOCK : (b + 1) * BLOCK], axis=1, keepdims=True)
                prefix = dot(ones, decay, precision=EXACT_PRECISION) + faded
                out, reach, total, state = block_step(
                    query, key, values[g, at, :], prefix, mask, state
                )
                out_ref[at, :] = out
                reach_ref[at, :] = (reach * jnp.exp(running)).astype(BF16)
                left.append((state, running + total))
            carried = tuple(left)
        return carried

    start = tuple(
        (
            jnp.zeros((values.shape[2], group[2].shape[1]), F32),
            jnp.zeros((1, group[2].shape[1]), F32),
        )
        for group in groups
    )
    (wide_state, wide_log), (narrow_state, narrow_log) = lax.fori_loop(
        0, length // (2 * BLOCK), advance, start, unroll=2
    )
    packed = jnp.concatenate([narrow_state[0:64], narrow_state[64:128]], axis=1)
    narrow_log = jnp.concatenate([narrow_log, narrow_log], axis=1)

    store_state(core_states, core, (wide_log, narrow_log, wide_state, packed))
    src = core_states.at[core]
    send(src, src, s_send.at[0], s_recv.at[0], partner)
    arrived(core_states.at[other], s_recv.at[0])
    first = load_state(core_states, 0)
    nothing = jax.tree.map(jnp.zeros_like, first)
    entering = selected(core == 1, first, nothing)
    total = combine(first, load_state(core_states, 1))
    for base, ref, name, here in ((1, y_states, "sp_1", y), (5, z_states, "sp_0", z)):
        store_state(ref, here, total)
        src = ref.at[here]
        for step in (1, 3, 2):
            send(src, src, s_send.at[base + step - 1], s_recv.at[base + here], {name: turn(here, step)})
        if base == 1:
            pump(0, NEAR[0:4])
        else:
            pump(0, NEAR[4:6])
            x_relay(sources, 0)
            start_weights(1)
        for step in (1, 3, 2):
            peer = turn(here, step)
            arrived(ref.at[peer], s_recv.at[base + peer])
        inside, total = (nothing, nothing)
        for k in range(RING):
            total = combine(total, load_state(ref, k))
            inside = selected(k < here, total, inside)
        entering = combine(inside, entering)
    _, _, wide_state, packed = entering
    narrow_state = jnp.concatenate([packed[:, 0:64], packed[:, 64:128]], axis=0).astype(BF16)
    wide_state = wide_state.astype(BF16)

    for n in range(RING):
        at = pl.ds(n * rows, rows)
        parts = []
        for g, (out_ref, reach_ref, state) in enumerate(
            ((wide_out, wide_reach, wide_state), (narrow_out, narrow_reach, narrow_state))
        ):
            out = out_ref[at, :] + dot(reach_ref[at, :], state, NT)
            inverse = lax.rsqrt(jnp.mean(out * out, axis=1, keepdims=True) + EPSILON)
            out = out * inverse * channel_norm_scale[...]
            parts.append((out * jax.nn.silu(switches[g, at, :].astype(F32))).astype(BF16))
        mixed[x, at, :] = jnp.concatenate(parts, axis=1)

    x_first(mixed, 8)
    x_second(mixed, 8)

    pump(0, ACROSS + SIDES + CORNERS[0:2])
    pump(1, NEAR)
    pump(0, CORNERS[2:4] + EDGES + CORNERS[4:6])
    pump(1, ACROSS)
    x_relay(mixed, 8)
    x_second(sources, 0)
    pump(1, SIDES)
    pump(0, ENDS[0:2])
    pump(1, CORNERS[0:2])
    pump(0, ENDS[2:4])
    pump(1, CORNERS[2:4])
    pump(0, FAR)
    pump(1, EDGES + CORNERS[4:6])
    x_rest(mixed, 8)
    x_opposite(mixed, 8)
    x_opposite(sources, 0)
    for copy in loads[first_loads:]:
        copy.wait()

    half = rows // 2
    upper, lower = (pl.ds(0, half), pl.ds(half, half))

    def emit(pieces):
        def lines(owner, h):
            return pl.ds(pl.multiple_of(owner * rows + h * half, half), half)

        left = jnp.concatenate(
            [
                jnp.concatenate([mixed[t, lines(owner, h), :] for owner, h in pieces], axis=0)
                for t in range(RING)
            ],
            axis=1,
        )

        def tile(n, squares):
            cols = pl.ds(pl.multiple_of(n * 512, 512), 512)
            found = dot(left, projection[:, :, cols].reshape(4 * 256, 512))
            source = [sources[owner, pl.ds(h * half, half), cols] for owner, h in pieces]
            found = found + jnp.concatenate(source, axis=0).astype(F32)
            updated[:, cols] = found
            found = found * found
            return squares + (
                (found[:, 0:128] + found[:, 128:256]) + (found[:, 256:384] + found[:, 384:512])
            )

        squares = lax.fori_loop(0, model // 512, tile, jnp.zeros((rows, 128), F32))
        mean = jnp.sum(squares, axis=1, keepdims=True) / model
        inverse = lax.rsqrt(mean + EPSILON)

        def scale(n, carry):
            cols = pl.ds(pl.multiple_of(n * 512, 512), 512)
            normed[:, cols] = (updated[:, cols] * inverse * mlp_scale[:, cols]).astype(BF16)
            return carry

        lax.fori_loop(0, model // 512, scale, 0)

    def widen_all():
        def widen(n, carry):
            cols = pl.ds(pl.multiple_of(n * 256, 256), 256)
            both = dot(normed[...], weights[:, :, cols].reshape(model, 256))
            found = (jax.nn.silu(both[:, 0:128]) * both[:, 128:256]).astype(BF16)
            hidden[:, pl.ds(pl.multiple_of(n * 128, 128), 128)] = found
            return carry

        lax.fori_loop(0, ff // 128, widen, 0, unroll=4)

    def shrink_all(out_ref, passed=False, first=0, last=model // 256):
        def shrink(n, carry):
            cols = pl.ds(pl.multiple_of(n * 256, 256), 256)
            four = weights[pl.ds(n * 4, 4), :, pl.ds(2 * ff, ff)].reshape(256, ff)
            found = dot(hidden[...], four, NT)
            if passed:
                found = found + jnp.concatenate(
                    [passing[0, :, cols], passing[1, :, cols]], axis=0
                ).astype(F32)
            out_ref[:, cols] = found.astype(out_ref.dtype)
            return carry

        lax.fori_loop(first, last, shrink, 0, unroll=4)

    def send_sum(src, dst, k, step):
        send(src, dst, r_send.at[k], r_recv.at[k], {"tp": turn(x, step)})

    left_x, right_x = (turn(x, 3), turn(x, 1))

    emit(((turn(x, 2), 0), (turn(x, 2), 1)))
    pump(1, ENDS)
    wait_partner(0)
    widen_all()
    pump(1, FAR)
    wait_partner(1)
    for k in range(2):
        shrink_all(partial.at[0], first=k * (model // 512), last=(k + 1) * (model // 512))
        cols = pl.ds(k * (model // 2), model // 2)
        send_sum(partial.at[0, upper, cols], passing.at[0, :, cols], k, 1)
        send_sum(partial.at[0, lower, cols], passing.at[1, :, cols], 2 + k, 3)
    emit(((right_x, 1), (left_x, 0)))
    widen_all()
    shrink_all(partial.at[1])
    send_sum(partial.at[1, upper], landed.at[0, lower], 4, 1)
    send_sum(partial.at[1, lower], landed.at[1, upper], 5, 3)
    x_rest(sources, 0)
    emit(((right_x, 0), (left_x, 1)))
    widen_all()
    for k in range(2):
        cols = pl.ds(k * (model // 2), model // 2)
        arrived(passing.at[0, :, cols], r_recv.at[k])
        arrived(passing.at[1, :, cols], r_recv.at[2 + k])
    shrink_all(partial.at[2], passed=True)
    send_sum(partial.at[2, upper], landed.at[0, upper], 6, 1)
    send_sum(partial.at[2, lower], landed.at[1, lower], 7, 3)
    emit(((x, 0), (x, 1)))
    widen_all()
    shrink_all(own_part)
    for n, (k, part) in enumerate(((0, lower), (1, upper), (0, upper), (1, lower))):
        arrived(landed.at[k, part], r_recv.at[4 + n])

    def finish(n, carry):
        cols = pl.ds(pl.multiple_of(n * 256, 256), 256)
        summed = own_part[:, cols] + (landed[0, :, cols].astype(F32) + landed[1, :, cols].astype(F32))
        layer_out[:, cols] = (updated[:, cols] + 0.5 * summed).astype(BF16)
        return carry

    lax.fori_loop(0, model // 256, finish, 0)
    for copy in sent:
        copy.wait_send()


def local(
    layer_source,
    broad_probe_tensor,
    broad_retention_preact,
    broad_floor_margin,
    slim_probe_tensor,
    slim_retention_preact,
    slim_floor_margin,
    branch_content_tensor,
    emitted_switch_preact,
    extra_log_fades,
    channel_norm_scale,
    emission_projection,
    mlp_norm_scale,
    switch_projection,
    expand_projection,
    shrink_projection,
):
    rows, model = layer_source.shape
    length = broad_probe_tensor.shape[0]
    depth, ff = switch_projection.shape
    vmem = pl.BlockSpec(memory_space=pltpu.VMEM)
    far = pl.BlockSpec(memory_space=pl.ANY)
    dma = pltpu.SemaphoreType.DMA
    return pl.pallas_call(
        layer_kernel,
        out_shape=jax.ShapeDtypeStruct((rows, model), BF16),
        in_specs=[far] + [vmem] * 10 + [far, vmem, far, far, far],
        out_specs=vmem,
        scratch_shapes=[
            pltpu.VMEM((32, depth, 3 * ff), BF16),
            pltpu.VMEM((RING, rows, model), BF16),
            pltpu.VMEM((RING, length, 256), BF16),
            pltpu.VMEM((RING, 256, model), BF16),
            pltpu.VMEM((rows, model), F32),
            pltpu.VMEM((rows, model), BF16),
            pltpu.VMEM((rows, ff), BF16),
            pltpu.VMEM((3, rows, model), BF16),
            pltpu.VMEM((rows, model), F32),
            pltpu.VMEM((2, rows // 2, model), BF16),
            pltpu.VMEM((2, rows, model), BF16),
            pltpu.VMEM((length, 64), F32),
            pltpu.VMEM((length, 64), F32),
            pltpu.VMEM((length, 128), F32),
            pltpu.VMEM((length, 128), F32),
            pltpu.VMEM((length, 128), BF16),
            pltpu.VMEM((length, 64), BF16),
            pltpu.VMEM((2, 208, 128), BF16),
            pltpu.VMEM((RING, 208, 128), BF16),
            pltpu.VMEM((RING, 208, 128), BF16),
            dma((32,)),
            dma((60,)),
            dma((64,)),
            dma((32,)),
            dma((32,)),
            dma((12,)),
            dma((16,)),
            dma((9,)),
            dma((9,)),
            dma((8,)),
            dma((8,)),
        ],
        compiler_params=pltpu.CompilerParams(
            collective_id=0, has_side_effects=True, vmem_limit_bytes=62 * 1024 * 1024
        ),
    )(
        layer_source,
        broad_probe_tensor,
        broad_retention_preact,
        broad_floor_margin.reshape(1, -1),
        slim_probe_tensor.T,
        slim_retention_preact.T,
        slim_floor_margin.reshape(1, -1),
        branch_content_tensor,
        emitted_switch_preact,
        jnp.swapaxes(extra_log_fades, 1, 2),
        channel_norm_scale.reshape(1, -1),
        emission_projection,
        mlp_norm_scale.reshape(1, -1),
        switch_projection,
        expand_projection,
        shrink_projection.T,
    )


def solution(mesh):
    torus = Mesh(mesh.devices.reshape(4, 4, 2, mesh.shape["tp"]), SP_TP)
    placed = (
        P(SP_TP, None),
        P(SP, "tp"),
        P(SP, "tp"),
        P("tp"),
        P(SP, "tp"),
        P(SP, "tp"),
        P("tp"),
        P(None, SP, "tp"),
        P(None, SP, "tp"),
        P(None, SP, "tp"),
        P(),
        P(),
        P(),
        P(SP, "tp"),
        P(SP, "tp"),
        P("tp", SP),
    )
    return jax.shard_map(
        local, mesh=torus, in_specs=placed, out_specs=P(SP_TP, None), check_vma=False
    )
```

```python
import jax
import jax.numpy as jnp
from jax import lax
from jax.experimental import pallas as pl
from jax.experimental.pallas import tpu as pltpu
from jax.sharding import Mesh
from jax.sharding import PartitionSpec as P

BLOCK = 64
RING = 4
SP = ("sp_0", "sp_1", "sp_2")
SP_TP = ("sp_0", "sp_1", "sp_2", "tp")

EPSILON = 1e-06
EXACT_PRECISION = lax.Precision.HIGHEST
BF16 = jnp.bfloat16
F32 = jnp.float32
NT = (((1,), (1,)), ((), ()))
TN = (((0,), (0,)), ((), ()))
MESH = pl.DeviceIdType.MESH

NEAR = ((3, 0, 0), (1, 0, 1), (0, 3, 0), (0, 1, 1), (3, 0, 1), (1, 0, 0))
ACROSS = ((2, 0, 0), (2, 0, 1))
CORNERS = ((3, 3, 0), (3, 1, 1), (1, 3, 0), (1, 1, 1), (2, 3, 0), (2, 1, 1))
SIDES = ((0, 3, 1), (0, 1, 0))
EDGES = ((3, 3, 1), (3, 1, 0), (0, 2, 0), (0, 2, 1), (1, 3, 1), (1, 1, 0))
ENDS = ((2, 3, 1), (2, 1, 0), (3, 2, 0), (3, 2, 1))
FAR = ((1, 2, 0), (1, 2, 1), (2, 2, 0), (2, 2, 1))


def turn(value, step):
    return lax.rem(value + step, RING)


def dot(a, b, dims=(((1,), (0,)), ((), ())), precision=None):
    return lax.dot_general(a, b, dims, preferred_element_type=F32, precision=precision)


def combine(earlier, later):
    wide_early, narrow_early, wide_state_early, narrow_state_early = earlier
    wide_late, narrow_late, wide_state_late, narrow_state_late = later
    return (
        wide_early + wide_late,
        narrow_early + narrow_late,
        jnp.exp(wide_late) * wide_state_early + wide_state_late,
        jnp.exp(narrow_late) * narrow_state_early + narrow_state_late,
    )


def split_log(log):
    first = log.astype(BF16).astype(F32)
    second = (log - first).astype(BF16).astype(F32)
    return [first, second, log - first - second]


def store_state(ref, at, state):
    wide, narrow, wide_state, narrow_state = state
    ref[at, 0:128, :] = wide_state.astype(BF16)
    ref[at, 128:192, :] = narrow_state.astype(BF16)
    lines = split_log(wide) + split_log(narrow)
    lines.append(jnp.zeros((10, wide.shape[1]), F32))
    ref[at, 192:208, :] = jnp.concatenate(lines, axis=0).astype(BF16)


def load_state(ref, at):
    lines = ref[at, 192:208, :].astype(F32)
    wide = lines[0:1] + lines[1:2] + lines[2:3]
    narrow = lines[3:4] + lines[4:5] + lines[5:6]
    return (wide, narrow, ref[at, 0:128, :].astype(F32), ref[at, 128:192, :].astype(F32))


def selected(passed, new, old):
    return jax.tree.map(lambda a, b: jnp.where(passed, a, b), new, old)


def block_step(query, key, value, prefix, mask, state):
    half = BLOCK // 2
    middle, total = (prefix[half - 1 : half, :], prefix[BLOCK - 1 : BLOCK, :])
    query_in = query * jnp.exp(prefix - middle)
    key_in = key * jnp.exp(middle - prefix)
    scores = dot(query_in.astype(BF16), key_in.astype(BF16), NT)
    scores = jnp.where(mask, scores, 0.0).astype(BF16)
    inside = dot(scores, value)
    reach = query_in * jnp.exp(middle)
    earlier = dot(reach.astype(BF16), state.astype(BF16), NT)
    leaving = (key_in * jnp.exp(total - middle)).astype(BF16)
    state = state * jnp.exp(total) + dot(value, leaving, TN)
    return (inside + earlier, reach, total, state)


def layer_kernel(
    layer_source,
    wide_query_far,
    wide_forget_far,
    wide_gap_far,
    narrow_query_far,
    narrow_forget_far,
    narrow_gap_far,
    values_far,
    switches_far,
    fades_far,
    channel_norm_scale_far,
    emission,
    mlp_scale_far,
    gate_shard,
    up_shard,
    down_shard,
    layer_out,
    weights,
    sources,
    mixed,
    projection,
    updated,
    normed,
    hidden,
    partial,
    own_part,
    passing,
    landed,
    narrow_q,
    narrow_f,
    wide_out,
    narrow_out,
    wide_reach,
    narrow_reach,
    core_states,
    y_states,
    z_states,
    z_before,
    wide_query,
    wide_forget,
    wide_gap,
    narrow_query,
    narrow_forget,
    narrow_gap,
    values,
    switches,
    fades,
    channel_norm_scale,
    mlp_scale,
    load_sem,
    w_send,
    w_recv,
    d_send,
    d_recv,
    x_send,
    x_recv,
    m_send,
    m_recv,
    n_send,
    n_recv,
    s_send,
    s_recv,
    r_send,
    r_recv,
):
    z, y, core, x = (lax.axis_index(name) for name in SP_TP)
    other = 1 - core
    rows, model = layer_source.shape
    length = wide_query.shape[0]
    ff = gate_shard.shape[1]
    depth = gate_shard.shape[0]
    sent = []

    def send(src, dst, send_sem, recv_sem, to, alone=True):
        copy = pltpu.make_async_remote_copy(
            src_ref=src,
            dst_ref=dst,
            send_sem=send_sem,
            recv_sem=recv_sem,
            device_id=to,
            device_id_type=MESH,
        )
        copy.start()
        if alone:
            sent.append(copy)

    partner = {"sp_2": other}

    def arrived(ref, sem):
        pltpu.make_async_remote_copy(
            src_ref=ref,
            dst_ref=ref,
            send_sem=sem,
            recv_sem=sem,
            device_id=partner,
            device_id_type=MESH,
        ).wait_recv()

    def place(i, j, of_core):
        first = jnp.where(of_core == 0, y, z)
        second = jnp.where(of_core == 0, z, y)
        first, second = (turn(first, i), turn(second, j))
        return (
            jnp.where(of_core == 0, second, first),
            jnp.where(of_core == 0, first, second),
        )

    def slot(i, j, of_core):
        at_z, at_y = place(i, j, of_core)
        return at_z * 8 + at_y * 2 + of_core

    half_depth = depth // 2

    columns_of = (pl.ds(0, 2 * ff), pl.ds(2 * ff, ff))

    def shard(i, j, h, part, of_core):
        lines = pl.ds(h * half_depth, half_depth)
        return weights.at[slot(i, j, of_core), lines, columns_of[part]]

    def shard_part(i, j, part, of_core):
        return weights.at[slot(i, j, of_core), :, columns_of[part]]

    def toward(i, j):
        at_z, at_y = place(i, j, core)
        return {"sp_0": at_z, "sp_1": at_y}

    def mark(i, j, h, part):
        return part * 32 + (i * 4 + j) * 2 + h

    counts = {"x": 0}

    def next_of(name):
        counts[name] += 1
        return counts[name] - 1

    def forward(i, j, h, part, step, landing):
        src = shard(i, j, h, part, core)
        at = w_recv.at[mark(*landing, h, part)]
        send(src, src, w_send.at[0], at, toward(*step), False)

    def hand_over(i, j, part):
        src = shard_part(i, j, part, core)
        send(src, src, d_send.at[0], d_recv.at[part], partner, False)

    handed = {}

    def pump(part, arrivals):
        for i, j, h in arrivals:
            arrived(shard(i, j, h, part, core), w_recv.at[mark(i, j, h, part)])
            if j == 0:
                if (i, h) == (3, 0):
                    forward(i, 0, h, part, (1, 0), (2, 0))
                if (i, h) == (1, 1):
                    forward(i, 0, h, part, (3, 0), (2, 0))
                forward(i, 0, h, part, (0, 1), (i, 3))
                forward(i, 0, h, part, (0, 3), (i, 1))
            else:
                if (j, h) == (3, 0):
                    forward(i, j, h, part, (0, 1), (i, 2))
                if (j, h) == (1, 1):
                    forward(i, j, h, part, (0, 3), (i, 2))
            handed[(i, j, part)] = handed.get((i, j, part), 0) + 1
            if handed[(i, j, part)] == 2:
                hand_over(i, j, part)

    def start_weights(part):
        for h in range(2):
            forward(0, 0, h, part, (1, 0), (3, 0))
            forward(0, 0, 1 - h, part, (3, 0), (1, 0))
            forward(0, 0, h, part, (0, 1), (0, 3))
            forward(0, 0, 1 - h, part, (0, 3), (0, 1))
        hand_over(0, 0, part)

    def wait_partner(part):
        arrived(weights.at[pl.ds(0, 16), :, columns_of[part]], d_recv.at[part])

    def x_piece(buffer, step, h):
        half = buffer.shape[1] // 2
        return buffer.at[turn(x, step), pl.ds(h * half, half), :]

    def x_forward(buffer, base, step, h, to, landing):
        src = x_piece(buffer, step, h)
        send(src, src, x_send.at[next_of("x")], x_recv.at[base + landing * 2 + h], {"tp": turn(x, to)})

    def x_wait(buffer, base, step, h):
        arrived(x_piece(buffer, step, h), x_recv.at[base + step * 2 + h])

    def x_first(buffer, base):
        x_forward(buffer, base, 0, 0, 1, 3)
        x_forward(buffer, base, 0, 1, 3, 1)

    def x_relay(buffer, base):
        x_wait(buffer, base, 3, 0)
        x_forward(buffer, base, 3, 0, 1, 2)
        x_wait(buffer, base, 1, 1)
        x_forward(buffer, base, 1, 1, 3, 2)

    def x_opposite(buffer, base):
        x_wait(buffer, base, 2, 0)
        x_wait(buffer, base, 2, 1)

    def head_piece(sender, r, h):
        owner = turn(x, (sender + r) % RING)
        at = owner * rows + (0 if h is None else h * (rows // 2))
        count = rows if h is None else rows // 2
        return mixed.at[turn(x, sender), pl.ds(pl.multiple_of(at, 128), count), :]

    def heads_to(sender, r, h, k, step):
        src = head_piece(sender, r, h)
        send(src, src, m_send.at[k], m_recv.at[k], {"tp": turn(x, step)})

    def heads_wait(sender, r, h, k):
        arrived(head_piece(sender, r, h), m_recv.at[k])

    barrier = pltpu.get_barrier_semaphore()
    pl.semaphore_signal(barrier, inc=1, device_id=partner, device_id_type=MESH)
    for name, here in (("sp_0", z), ("sp_1", y), ("tp", x)):
        for step in (1, 2, 3):
            pl.semaphore_signal(
                barrier, inc=1, device_id={name: turn(here, step)}, device_id_type=MESH
            )

    me = slot(0, 0, core)
    loads = []

    def load(src, dst, shared=None):
        sem = load_sem.at[2 + len(loads) if shared is None else shared]
        copy = pltpu.make_async_copy(src, dst, sem)
        copy.start()
        if shared is None:
            loads.append(copy)

    for n in range(ff // 128):
        cols = pl.ds(n * 128, 128)
        load(gate_shard.at[:, cols], weights.at[me, :, pl.ds(n * 256, 128)], 0)
        load(up_shard.at[:, cols], weights.at[me, :, pl.ds(n * 256 + 128, 128)], 0)
    load(down_shard, weights.at[me, :, pl.ds(2 * ff, ff)], 0)
    load(layer_source, sources.at[x])
    shard_loads = len(loads)
    for src, dst in (
        (wide_query_far, wide_query),
        (wide_forget_far, wide_forget),
        (wide_gap_far, wide_gap),
        (narrow_query_far, narrow_query),
        (narrow_forget_far, narrow_forget),
        (narrow_gap_far, narrow_gap),
        (values_far, values),
        (fades_far, fades),
    ):
        load(src, dst)
    first_loads = len(loads)
    load(switches_far, switches)
    load(channel_norm_scale_far, channel_norm_scale)
    mixed_loads = len(loads)
    load(mlp_scale_far, mlp_scale)
    for t in range(RING):
        for g in range(2):
            load(emission.at[g, pl.ds(t * 128, 128), :], projection.at[t, pl.ds(g * 128, 128), :], 1)

    pl.semaphore_wait(barrier, 10)

    pltpu.make_async_copy(weights.at[me], weights.at[me], load_sem.at[0]).wait()
    for copy in loads[:shard_loads]:
        copy.wait()
    start_weights(0)
    x_first(sources, 0)
    for copy in loads[shard_loads:first_loads]:
        copy.wait()
    for n in range(length // 128):
        cols = pl.ds(n * 128, 128)
        narrow_q[cols, :] = narrow_query[:, cols].astype(F32).T
        narrow_f[cols, :] = narrow_forget[:, cols].astype(F32).T
    line = lax.broadcasted_iota(jnp.int32, (BLOCK, BLOCK), 0)
    column = lax.broadcasted_iota(jnp.int32, (BLOCK, BLOCK), 1)
    mask = line >= column
    ones = jnp.where(mask, 1.0, 0.0)
    groups = (
        (wide_query, wide_forget, wide_gap, wide_out, wide_reach),
        (narrow_q, narrow_f, narrow_gap, narrow_out, narrow_reach),
    )

    def advance(pair, carried):
        for b in range(2):
            at = pl.ds(pl.multiple_of((pair * 2 + b) * BLOCK, BLOCK), BLOCK)
            left = []
            for g in range(2):
                query_ref, forget_ref, gap_ref, out_ref, reach_ref = groups[g]
                state, running = carried[g]
                key = gap_ref[...] * jax.nn.sigmoid(-forget_ref[at, :].astype(F32))
                decay = jnp.log1p(-key)
                query = jax.nn.silu(query_ref[at, :].astype(F32)) * key.shape[1] ** (-0.5)
                fade = fades[g, :, pl.ds(pl.multiple_of(pair * 2 * BLOCK, 2 * BLOCK), 2 * BLOCK)]
                faded = jnp.sum(ones * fade[:, b * BLOCK : (b + 1) * BLOCK], axis=1, keepdims=True)
                prefix = dot(ones, decay, precision=EXACT_PRECISION) + faded
                out, reach, total, state = block_step(
                    query, key, values[g, at, :], prefix, mask, state
                )
                out_ref[at, :] = out
                reach_ref[at, :] = (reach * jnp.exp(running)).astype(BF16)
                left.append((state, running + total))
            carried = tuple(left)
        return carried

    start = tuple(
        (
            jnp.zeros((values.shape[2], group[2].shape[1]), F32),
            jnp.zeros((1, group[2].shape[1]), F32),
        )
        for group in groups
    )
    (wide_state, wide_log), (narrow_state, narrow_log) = lax.fori_loop(
        0, length // (2 * BLOCK), advance, start, unroll=2
    )
    packed = jnp.concatenate([narrow_state[0:64], narrow_state[64:128]], axis=1)
    narrow_log = jnp.concatenate([narrow_log, narrow_log], axis=1)

    store_state(core_states, core, (wide_log, narrow_log, wide_state, packed))
    src = core_states.at[core]
    send(src, src, s_send.at[0], s_recv.at[0], partner)
    arrived(core_states.at[other], s_recv.at[0])
    first = load_state(core_states, 0)
    nothing = jax.tree.map(jnp.zeros_like, first)
    entering = selected(core == 1, first, nothing)
    total = combine(first, load_state(core_states, 1))
    store_state(y_states, y, total)
    src = y_states.at[y]
    for step in (1, 3, 2):
        send(src, src, s_send.at[step], s_recv.at[1 + y], {"sp_1": turn(y, step)})
    pump(0, NEAR[0:4])
    start_weights(1)
    for step in (1, 3, 2):
        if step == 2:
            x_relay(sources, 0)
        arrived(y_states.at[turn(y, step)], s_recv.at[1 + turn(y, step)])

    def before(ref, here):
        inside, total = (nothing, nothing)
        for k in range(RING):
            total = combine(total, load_state(ref, k))
            inside = selected(k < here, total, inside)
        return (inside, total)

    inside, total = before(y_states, y)
    entering = combine(inside, entering)
    src = z_states.at[z]
    z_copies = [
        pltpu.make_async_remote_copy(
            src_ref=src,
            dst_ref=src,
            send_sem=s_send.at[3 + step],
            recv_sem=s_recv.at[5 + z],
            device_id={"sp_0": turn(z, step)},
            device_id_type=MESH,
        )
        for step in (1, 3, 2)
    ]
    told = pltpu.make_async_remote_copy(
        src_ref=z_before.at[0],
        dst_ref=z_before.at[0],
        send_sem=s_send.at[7],
        recv_sem=s_recv.at[9],
        device_id=partner,
        device_id_type=MESH,
    )

    @pl.when(core == 1)
    def _():
        store_state(z_states, z, total)
        for copy in z_copies:
            copy.start()

    pump(0, NEAR[4:6] + ACROSS + SIDES)

    @pl.when(core == 1)
    def _():
        for step in (1, 3, 2):
            arrived(z_states.at[turn(z, step)], s_recv.at[5 + turn(z, step)])
        store_state(z_before, 0, before(z_states, z)[0])
        told.start()

    @pl.when(core == 0)
    def _():
        told.wait_recv()

    entering = combine(load_state(z_before, 0), entering)
    _, _, wide_state, packed = entering
    narrow_state = jnp.concatenate([packed[:, 0:64], packed[:, 64:128]], axis=0).astype(BF16)
    wide_state = wide_state.astype(BF16)

    for copy in loads[first_loads:mixed_loads]:
        copy.wait()
    for n in range(RING):
        at = pl.ds(n * rows, rows)
        parts = []
        for g, (out_ref, reach_ref, state) in enumerate(
            ((wide_out, wide_reach, wide_state), (narrow_out, narrow_reach, narrow_state))
        ):
            out = out_ref[at, :] + dot(reach_ref[at, :], state, NT)
            inverse = lax.rsqrt(jnp.mean(out * out, axis=1, keepdims=True) + EPSILON)
            out = out * inverse * channel_norm_scale[...]
            parts.append((out * jax.nn.silu(switches[g, at, :].astype(F32))).astype(BF16))
        mixed[x, at, :] = jnp.concatenate(parts, axis=1)

    for k, (right, left) in enumerate((((2, 1), (2, 0)), ((0, 0), (0, 1)), ((1, None), (3, None)), ((3, None), (1, None)))):
        heads_to(0, *right, k, 1)
        heads_to(0, *left, 4 + k, 3)

    pump(0, CORNERS[0:2])
    pump(1, NEAR[0:4])
    pump(0, CORNERS[2:4] + EDGES)
    pump(1, NEAR[4:6])
    for k, (right, left) in enumerate((((2, 1), (2, 0)), ((0, 0), (0, 1)))):
        heads_wait(3, *right, k)
        heads_to(3, *right, 8 + k, 1)
        heads_wait(1, *left, 4 + k)
        heads_to(1, *left, 11 + k, 3)
    pump(0, CORNERS[4:6])
    pump(1, ACROSS)
    pltpu.make_async_copy(projection, projection, load_sem.at[1]).wait()
    for copy in loads[mixed_loads:]:
        copy.wait()
    heads_wait(3, 1, None, 2)
    heads_wait(1, 3, None, 6)
    heads_wait(2, 2, 1, 8)
    heads_wait(2, 2, 0, 11)

    half = rows // 2
    upper, lower = (pl.ds(0, half), pl.ds(half, half))

    def emit(pieces, chunk, raw):
        def lines(owner, h):
            return pl.ds(pl.multiple_of(owner * rows + h * half, half), half)

        left = jnp.concatenate(
            [
                jnp.concatenate([mixed[t, lines(owner, h), :] for owner, h in pieces], axis=0)
                for t in range(RING)
            ],
            axis=1,
        )

        def tile(n, squares):
            cols = pl.ds(pl.multiple_of(n * 512, 512), 512)
            found = dot(left, projection[:, :, cols].reshape(4 * 256, 512))
            source = [sources[owner, pl.ds(h * half, half), cols] for owner, h in pieces]
            found = found + jnp.concatenate(source, axis=0).astype(F32)
            raw[:, cols] = found
            found = found * found
            return squares + (
                (found[:, 0:128] + found[:, 128:256]) + (found[:, 256:384] + found[:, 384:512])
            )

        squares = lax.fori_loop(0, model // 512, tile, jnp.zeros((rows, 128), F32))
        mean = jnp.sum(squares, axis=1, keepdims=True) / model
        inverse = lax.rsqrt(mean + EPSILON)

        def scale(n, carry):
            cols = pl.ds(pl.multiple_of(n * 512, 512), 512)
            normed[chunk, :, cols] = (raw[:, cols] * inverse * mlp_scale[:, cols]).astype(BF16)
            return carry

        lax.fori_loop(0, model // 512, scale, 0)

    def widen_all(chunk, first=0, last=ff // 128):
        def widen(n, carry):
            cols = pl.ds(pl.multiple_of(n * 256, 256), 256)
            both = dot(normed[chunk], weights[:, :, cols].reshape(model, 256))
            found = (jax.nn.silu(both[:, 0:128]) * both[:, 128:256]).astype(BF16)
            hidden[:, pl.ds(pl.multiple_of(n * 128, 128), 128)] = found
            return carry

        lax.fori_loop(first, last, widen, 0, unroll=4)

    def shrink_all(out_ref, passed=False, first=0, last=model // 256):
        def shrink(n, carry):
            cols = pl.ds(pl.multiple_of(n * 256, 256), 256)
            four = weights[pl.ds(n * 4, 4), :, pl.ds(2 * ff, ff)].reshape(256, ff)
            found = dot(hidden[...], four, NT)
            if passed:
                found = found + jnp.concatenate(
                    [passing[0, :, cols], passing[1, :, cols]], axis=0
                ).astype(F32)
            out_ref[:, cols] = found.astype(out_ref.dtype)
            return carry

        lax.fori_loop(first, last, shrink, 0, unroll=4)

    def send_sum(src, dst, k, step):
        send(src, dst, r_send.at[k], r_recv.at[k], {"tp": turn(x, step)})

    left_x, right_x = (turn(x, 3), turn(x, 1))

    emit(((x, 0), (x, 1)), 3, updated)
    send(normed.at[3, lower], normed.at[2, lower], n_send.at[0], n_recv.at[0], {"tp": right_x})
    send(normed.at[3, upper], normed.at[2, upper], n_send.at[1], n_recv.at[1], {"tp": left_x})
    heads_wait(3, 3, None, 3)
    heads_to(3, 3, 1, 10, 1)
    heads_wait(1, 1, None, 7)
    heads_to(1, 1, 0, 13, 3)
    pump(1, SIDES)
    pump(0, ENDS[0:2])
    pump(1, CORNERS[0:2])
    pump(0, ENDS[2:4])
    pump(1, CORNERS[2:4])
    pump(0, FAR)
    heads_wait(2, 0, 0, 9)
    heads_wait(2, 0, 1, 12)
    x_opposite(sources, 0)
    emit(((turn(x, 2), 0), (turn(x, 2), 1)), 0, own_part)
    pump(1, EDGES + CORNERS[4:6])
    wait_partner(0)
    widen_all(0, 0, 8)
    pump(1, ENDS + FAR)
    widen_all(0, 8, ff // 128)
    wait_partner(1)
    for k in range(2):
        shrink_all(partial.at[0], first=k * (model // 512), last=(k + 1) * (model // 512))
        cols = pl.ds(k * (model // 2), model // 2)
        send_sum(partial.at[0, upper, cols], passing.at[0, :, cols], k, 1)
        send_sum(partial.at[0, lower, cols], passing.at[1, :, cols], 2 + k, 3)
    heads_wait(2, 3, 1, 10)
    heads_wait(2, 1, 0, 13)
    emit(((right_x, 1), (left_x, 0)), 1, own_part)
    widen_all(1)
    shrink_all(partial.at[1])
    send_sum(partial.at[1, upper], landed.at[0, lower], 4, 1)
    send_sum(partial.at[1, lower], landed.at[1, upper], 5, 3)
    arrived(normed.at[2, lower], n_recv.at[0])
    arrived(normed.at[2, upper], n_recv.at[1])
    widen_all(2)
    for k in range(2):
        cols = pl.ds(k * (model // 2), model // 2)
        arrived(passing.at[0, :, cols], r_recv.at[k])
        arrived(passing.at[1, :, cols], r_recv.at[2 + k])
    shrink_all(partial.at[2], passed=True)
    send_sum(partial.at[2, upper], landed.at[0, upper], 6, 1)
    send_sum(partial.at[2, lower], landed.at[1, lower], 7, 3)
    widen_all(3)
    shrink_all(own_part)
    for n, (k, part) in enumerate(((0, lower), (1, upper), (0, upper), (1, lower))):
        arrived(landed.at[k, part], r_recv.at[4 + n])

    def finish(n, carry):
        cols = pl.ds(pl.multiple_of(n * 256, 256), 256)
        summed = own_part[:, cols] + (landed[0, :, cols].astype(F32) + landed[1, :, cols].astype(F32))
        layer_out[:, cols] = (updated[:, cols] + 0.5 * summed).astype(BF16)
        return carry

    lax.fori_loop(0, model // 256, finish, 0)
    for copy in sent:
        copy.wait_send()
    for count, sem in ((15, w_send), (16, d_send)):
        shards = weights.at[pl.ds(0, count)]
        pltpu.make_async_remote_copy(
            src_ref=shards,
            dst_ref=shards,
            send_sem=sem.at[0],
            recv_sem=sem.at[0],
            device_id=partner,
            device_id_type=MESH,
        ).wait_send()

    @pl.when(core == 1)
    def _():
        for copy in z_copies:
            copy.wait_send()
        told.wait_send()


def local(
    layer_source,
    broad_probe_tensor,
    broad_retention_preact,
    broad_floor_margin,
    slim_probe_tensor,
    slim_retention_preact,
    slim_floor_margin,
    branch_content_tensor,
    emitted_switch_preact,
    extra_log_fades,
    channel_norm_scale,
    emission_projection,
    mlp_norm_scale,
    switch_projection,
    expand_projection,
    shrink_projection,
):
    rows, model = layer_source.shape
    length = broad_probe_tensor.shape[0]
    depth, ff = switch_projection.shape
    vmem = pl.BlockSpec(memory_space=pltpu.VMEM)
    far = pl.BlockSpec(memory_space=pl.ANY)
    dma = pltpu.SemaphoreType.DMA
    return pl.pallas_call(
        layer_kernel,
        out_shape=pltpu.VMEM((rows, model), BF16),
        in_specs=[far] * 16,
        out_specs=vmem,
        scratch_shapes=[
            pltpu.VMEM((32, depth, 3 * ff), BF16),
            pltpu.VMEM((RING, rows, model), BF16),
            pltpu.VMEM((RING, length, 256), BF16),
            pltpu.VMEM((RING, 256, model), BF16),
            pltpu.VMEM((rows, model), F32),
            pltpu.VMEM((RING, rows, model), BF16),
            pltpu.VMEM((rows, ff), BF16),
            pltpu.VMEM((3, rows, model), BF16),
            pltpu.VMEM((rows, model), F32),
            pltpu.VMEM((2, rows // 2, model), BF16),
            pltpu.VMEM((2, rows, model), BF16),
            pltpu.VMEM((length, 64), F32),
            pltpu.VMEM((length, 64), F32),
            pltpu.VMEM((length, 128), F32),
            pltpu.VMEM((length, 128), F32),
            pltpu.VMEM((length, 128), BF16),
            pltpu.VMEM((length, 64), BF16),
            pltpu.VMEM((2, 208, 128), BF16),
            pltpu.VMEM((RING, 208, 128), BF16),
            pltpu.VMEM((RING, 208, 128), BF16),
            pltpu.VMEM((1, 208, 128), BF16),
            pltpu.VMEM((length, 128), BF16),
            pltpu.VMEM((length, 128), BF16),
            pltpu.VMEM((1, 128), F32),
            pltpu.VMEM((64, length), BF16),
            pltpu.VMEM((64, length), BF16),
            pltpu.VMEM((1, 64), F32),
            pltpu.VMEM((2, length, 128), BF16),
            pltpu.VMEM((2, length, 128), BF16),
            pltpu.VMEM((2, 1, length), F32),
            pltpu.VMEM((1, 128), F32),
            pltpu.VMEM((1, model), F32),
            dma((14,)),
            dma((1,)),
            dma((64,)),
            dma((1,)),
            dma((2,)),
            dma((4,)),
            dma((8,)),
            dma((14,)),
            dma((14,)),
            dma((2,)),
            dma((2,)),
            dma((8,)),
            dma((10,)),
            dma((8,)),
            dma((8,)),
        ],
        compiler_params=pltpu.CompilerParams(
            collective_id=0, has_side_effects=True, vmem_limit_bytes=62 * 1024 * 1024
        ),
    )(
        layer_source,
        broad_probe_tensor,
        broad_retention_preact,
        broad_floor_margin.reshape(1, -1),
        slim_probe_tensor.T,
        slim_retention_preact.T,
        slim_floor_margin.reshape(1, -1),
        branch_content_tensor,
        emitted_switch_preact,
        jnp.swapaxes(extra_log_fades, 1, 2),
        channel_norm_scale.reshape(1, -1),
        emission_projection,
        mlp_norm_scale.reshape(1, -1),
        switch_projection,
        expand_projection,
        shrink_projection.T,
    )


def solution(mesh):
    torus = Mesh(mesh.devices.reshape(4, 4, 2, mesh.shape["tp"]), SP_TP)
    placed = (
        P(SP_TP, None),
        P(SP, "tp"),
        P(SP, "tp"),
        P("tp"),
        P(SP, "tp"),
        P(SP, "tp"),
        P("tp"),
        P(None, SP, "tp"),
        P(None, SP, "tp"),
        P(None, SP, "tp"),
        P(),
        P(),
        P(),
        P(SP, "tp"),
        P(SP, "tp"),
        P("tp", SP),
    )
    return jax.shard_map(
        local, mesh=torus, in_specs=placed, out_specs=P(SP_TP, None), check_vma=False
    )
```

```python
import jax
import jax.numpy as jnp
from jax import lax
from jax.experimental import pallas as pl
from jax.experimental.pallas import tpu as pltpu
from jax.sharding import Mesh
from jax.sharding import PartitionSpec as P

BLOCK = 64
RING = 4
SP = ("sp_0", "sp_1", "sp_2")
SP_TP = ("sp_0", "sp_1", "sp_2", "tp")

EPSILON = 1e-06
EXACT_PRECISION = lax.Precision.HIGHEST
BF16 = jnp.bfloat16
F32 = jnp.float32
NT = (((1,), (1,)), ((), ()))
TN = (((0,), (0,)), ((), ()))
MESH = pl.DeviceIdType.MESH

NEAR = ((3, 0, 0), (1, 0, 1), (0, 3, 0), (0, 1, 1), (3, 0, 1), (1, 0, 0))
ACROSS = ((2, 0, 0), (2, 0, 1))
CORNERS = ((3, 3, 0), (3, 1, 1), (1, 3, 0), (1, 1, 1), (2, 3, 0), (2, 1, 1))
SIDES = ((0, 3, 1), (0, 1, 0))
EDGES = ((3, 3, 1), (3, 1, 0), (0, 2, 0), (0, 2, 1), (1, 3, 1), (1, 1, 0))
ENDS = ((2, 3, 1), (2, 1, 0), (3, 2, 0), (3, 2, 1))
FAR = ((1, 2, 0), (1, 2, 1), (2, 2, 0), (2, 2, 1))


PASSED = NEAR + ACROSS + CORNERS
GROUPS = (SIDES, EDGES, ENDS, FAR)


def turn(value, step):
    return lax.rem(value + step, RING)


def dot(a, b, dims=(((1,), (0,)), ((), ())), precision=None):
    return lax.dot_general(a, b, dims, preferred_element_type=F32, precision=precision)


def combine(earlier, later):
    wide_early, narrow_early, wide_state_early, narrow_state_early = earlier
    wide_late, narrow_late, wide_state_late, narrow_state_late = later
    return (
        wide_early + wide_late,
        narrow_early + narrow_late,
        jnp.exp(wide_late) * wide_state_early + wide_state_late,
        jnp.exp(narrow_late) * narrow_state_early + narrow_state_late,
    )


def split_log(log):
    first = log.astype(BF16).astype(F32)
    second = (log - first).astype(BF16).astype(F32)
    return [first, second, log - first - second]


def store_state(ref, at, state):
    wide, narrow, wide_state, narrow_state = state
    ref[at, 0:128, :] = wide_state.astype(BF16)
    ref[at, 128:192, :] = narrow_state.astype(BF16)
    lines = split_log(wide) + split_log(narrow)
    lines.append(jnp.zeros((10, wide.shape[1]), F32))
    ref[at, 192:208, :] = jnp.concatenate(lines, axis=0).astype(BF16)


def load_state(ref, at):
    lines = ref[at, 192:208, :].astype(F32)
    wide = lines[0:1] + lines[1:2] + lines[2:3]
    narrow = lines[3:4] + lines[4:5] + lines[5:6]
    return (wide, narrow, ref[at, 0:128, :].astype(F32), ref[at, 128:192, :].astype(F32))


def selected(passed, new, old):
    return jax.tree.map(lambda a, b: jnp.where(passed, a, b), new, old)


def block_step(query, key, value, prefix, mask, state):
    half = BLOCK // 2
    middle, total = (prefix[half - 1 : half, :], prefix[BLOCK - 1 : BLOCK, :])
    query_in = query * jnp.exp(prefix - middle)
    key_in = key * jnp.exp(middle - prefix)
    scores = dot(query_in.astype(BF16), key_in.astype(BF16), NT)
    scores = jnp.where(mask, scores, 0.0).astype(BF16)
    inside = dot(scores, value)
    reach = query_in * jnp.exp(middle)
    earlier = dot(reach.astype(BF16), state.astype(BF16), NT)
    leaving = (key_in * jnp.exp(total - middle)).astype(BF16)
    state = state * jnp.exp(total) + dot(value, leaving, TN)
    return (inside + earlier, reach, total, state)


def layer_kernel(
    layer_source,
    wide_query_far,
    wide_forget_far,
    wide_gap_far,
    narrow_query_far,
    narrow_forget_far,
    narrow_gap_far,
    values_far,
    switches_far,
    fades_far,
    channel_norm_scale_far,
    emission,
    mlp_scale_far,
    gate_shard,
    up_shard,
    down_shard,
    layer_out,
    weights,
    sources,
    mixed,
    projection,
    updated,
    normed,
    hidden,
    partial,
    own_part,
    passing,
    landed,
    narrow_q,
    narrow_f,
    wide_out,
    narrow_out,
    wide_reach,
    narrow_reach,
    core_states,
    y_states,
    z_states,
    z_before,
    wide_query,
    wide_forget,
    wide_gap,
    narrow_query,
    narrow_forget,
    narrow_gap,
    values,
    switches,
    fades,
    channel_norm_scale,
    mlp_scale,
    load_sem,
    w_send,
    w_recv,
    d_send,
    d_recv,
    x_send,
    x_recv,
    m_send,
    m_recv,
    n_send,
    n_recv,
    s_send,
    s_recv,
    r_send,
    r_recv,
):
    z, y, core, x = (lax.axis_index(name) for name in SP_TP)
    other = 1 - core
    rows, model = layer_source.shape
    length = wide_query.shape[0]
    ff = gate_shard.shape[1]
    depth = gate_shard.shape[0]
    sent = []

    def send(src, dst, send_sem, recv_sem, to, alone=True):
        copy = pltpu.make_async_remote_copy(
            src_ref=src,
            dst_ref=dst,
            send_sem=send_sem,
            recv_sem=recv_sem,
            device_id=to,
            device_id_type=MESH,
        )
        copy.start()
        if alone:
            sent.append(copy)

    partner = {"sp_2": other}

    def arrived(ref, sem):
        pltpu.make_async_remote_copy(
            src_ref=ref,
            dst_ref=ref,
            send_sem=sem,
            recv_sem=sem,
            device_id=partner,
            device_id_type=MESH,
        ).wait_recv()

    def place(i, j, of_core):
        first = jnp.where(of_core == 0, y, z)
        second = jnp.where(of_core == 0, z, y)
        first, second = (turn(first, i), turn(second, j))
        return (
            jnp.where(of_core == 0, second, first),
            jnp.where(of_core == 0, first, second),
        )

    def slot(i, j, of_core):
        at_z, at_y = place(i, j, of_core)
        return at_z * 8 + at_y * 2 + of_core

    half_depth = depth // 2

    columns_of = (pl.ds(0, 2 * ff), pl.ds(2 * ff, ff))

    def shard(i, j, h, part, of_core):
        lines = pl.ds(h * half_depth, half_depth)
        return weights.at[slot(i, j, of_core), lines, columns_of[part]]

    def shard_part(i, j, part, of_core):
        return weights.at[slot(i, j, of_core), :, columns_of[part]]

    def toward(i, j):
        at_z, at_y = place(i, j, core)
        return {"sp_0": at_z, "sp_1": at_y}

    def mark(i, j, h, part):
        if (i, j, h) in PASSED:
            return part * 18 + PASSED.index((i, j, h))
        return part * 18 + 14 + [(i, j, h) in group for group in GROUPS].index(True)

    def forward(i, j, h, part, step, landing):
        src = shard(i, j, h, part, core)
        at = w_recv.at[mark(*landing, h, part)]
        send(src, src, w_send.at[0], at, toward(*step), False)

    def hand_over(i, j, part):
        src = shard_part(i, j, part, core)
        send(src, src, d_send.at[0], d_recv.at[part], partner, False)

    def spread(i, h, part, passed_on):
        if (h == 0) == passed_on:
            forward(i, 0, h, part, (0, 1), (i, 3))
        else:
            forward(i, 0, h, part, (0, 3), (i, 1))

    handed = {}

    def pump(part, arrivals):
        for i, j, h in arrivals:
            arrived(shard(i, j, h, part, core), w_recv.at[mark(i, j, h, part)])
            if j == 0:
                if (i, h) == (3, 0):
                    forward(i, 0, h, part, (1, 0), (2, 0))
                if (i, h) == (1, 1):
                    forward(i, 0, h, part, (3, 0), (2, 0))
                spread(i, h, part, True)
                if part == 0:
                    spread(i, h, part, False)
            else:
                if (j, h) == (3, 0):
                    forward(i, j, h, part, (0, 1), (i, 2))
                if (j, h) == (1, 1):
                    forward(i, j, h, part, (0, 3), (i, 2))
            seen(i, j, part)

    def seen(i, j, part):
        handed[(i, j, part)] = handed.get((i, j, part), 0) + 1
        if handed[(i, j, part)] == 2:
            hand_over(i, j, part)

    def pump_group(part, group):
        halves = weights.at[pl.ds(0, len(group) // 2), :, columns_of[part]]
        arrived(halves, w_recv.at[mark(*group[0], part)])
        for i, j, _ in group:
            seen(i, j, part)

    def start_weights(part):
        for h in range(2):
            forward(0, 0, h, part, (1, 0), (3, 0))
            forward(0, 0, 1 - h, part, (3, 0), (1, 0))
            forward(0, 0, h, part, (0, 1), (0, 3))
            forward(0, 0, 1 - h, part, (0, 3), (0, 1))
        hand_over(0, 0, part)

    def wait_partner(part):
        arrived(weights.at[pl.ds(0, 16), :, columns_of[part]], d_recv.at[part])

    def rows_piece(step, q):
        quarter = rows // 4
        return sources.at[turn(x, step), pl.ds(q * quarter, quarter), :]

    def rows_to(step, q, landing, to):
        src = rows_piece(step, q)
        at = x_recv.at[min(landing, 4)]
        send(src, src, x_send.at[0], at, {"tp": turn(x, to)}, False)

    def rows_start():
        for k in range(2):
            rows_to(0, k, k, 1)
            rows_to(0, 2 + k, 2 + k, 3)

    def rows_relay(k):
        arrived(rows_piece(3, k), x_recv.at[k])
        rows_to(3, k, 4 + k, 1)
        arrived(rows_piece(1, 2 + k), x_recv.at[2 + k])
        rows_to(1, 2 + k, 6 + k, 3)

    def rows_opposite():
        arrived(sources.at[turn(x, 2)], x_recv.at[4])

    def head_piece(sender, r, h):
        owner = turn(x, (sender + r) % RING)
        at = owner * rows + (0 if h is None else h * (rows // 2))
        count = rows if h is None else rows // 2
        return mixed.at[turn(x, sender), pl.ds(pl.multiple_of(at, 128), count), :]

    def heads_to(sender, r, h, k, step):
        src = head_piece(sender, r, h)
        send(src, src, m_send.at[0], m_recv.at[k], {"tp": turn(x, step)}, False)

    def heads_wait_all(count, k):
        arrived(mixed.at[0, pl.ds(0, count), :], m_recv.at[k])

    def heads_wait(sender, r, h, k):
        arrived(head_piece(sender, r, h), m_recv.at[k])

    barrier = pltpu.get_barrier_semaphore()
    pl.semaphore_signal(barrier, inc=1, device_id=partner, device_id_type=MESH)
    for name, here in (("sp_0", z), ("sp_1", y), ("tp", x)):
        for step in (1, 2, 3):
            pl.semaphore_signal(
                barrier, inc=1, device_id={name: turn(here, step)}, device_id_type=MESH
            )

    me = slot(0, 0, core)
    loads = []

    def load(src, dst, shared=None):
        sem = load_sem.at[2 + len(loads) if shared is None else shared]
        copy = pltpu.make_async_copy(src, dst, sem)
        copy.start()
        if shared is None:
            loads.append(copy)

    for n in range(ff // 128):
        cols = pl.ds(n * 128, 128)
        load(gate_shard.at[:, cols], weights.at[me, :, pl.ds(n * 256, 128)], 0)
        load(up_shard.at[:, cols], weights.at[me, :, pl.ds(n * 256 + 128, 128)], 0)
    load(down_shard, weights.at[me, :, pl.ds(2 * ff, ff)], 0)
    load(layer_source, sources.at[x])
    shard_loads = len(loads)
    for src, dst in (
        (wide_query_far, wide_query),
        (wide_forget_far, wide_forget),
        (wide_gap_far, wide_gap),
        (narrow_query_far, narrow_query),
        (narrow_forget_far, narrow_forget),
        (narrow_gap_far, narrow_gap),
        (values_far, values),
        (fades_far, fades),
    ):
        load(src, dst)
    first_loads = len(loads)
    load(switches_far, switches)
    load(channel_norm_scale_far, channel_norm_scale)
    mixed_loads = len(loads)
    load(mlp_scale_far, mlp_scale)
    for t in range(RING):
        for g in range(2):
            load(emission.at[g, pl.ds(t * 128, 128), :], projection.at[t, pl.ds(g * 128, 128), :], 1)

    pl.semaphore_wait(barrier, 10)

    pltpu.make_async_copy(weights.at[me], weights.at[me], load_sem.at[0]).wait()
    for copy in loads[:shard_loads]:
        copy.wait()
    start_weights(0)
    rows_start()
    for copy in loads[shard_loads:first_loads]:
        copy.wait()
    for n in range(length // 128):
        cols = pl.ds(n * 128, 128)
        narrow_q[cols, :] = narrow_query[:, cols].astype(F32).T
        narrow_f[cols, :] = narrow_forget[:, cols].astype(F32).T
    line = lax.broadcasted_iota(jnp.int32, (BLOCK, BLOCK), 0)
    column = lax.broadcasted_iota(jnp.int32, (BLOCK, BLOCK), 1)
    mask = line >= column
    ones = jnp.where(mask, 1.0, 0.0)
    groups = (
        (wide_query, wide_forget, wide_gap, wide_out, wide_reach),
        (narrow_q, narrow_f, narrow_gap, narrow_out, narrow_reach),
    )

    def advance(pair, carried):
        for b in range(2):
            at = pl.ds(pl.multiple_of((pair * 2 + b) * BLOCK, BLOCK), BLOCK)
            left = []
            for g in range(2):
                query_ref, forget_ref, gap_ref, out_ref, reach_ref = groups[g]
                state, running = carried[g]
                key = gap_ref[...] * jax.nn.sigmoid(-forget_ref[at, :].astype(F32))
                decay = jnp.log1p(-key)
                query = jax.nn.silu(query_ref[at, :].astype(F32)) * key.shape[1] ** (-0.5)
                fade = fades[g, :, pl.ds(pl.multiple_of(pair * 2 * BLOCK, 2 * BLOCK), 2 * BLOCK)]
                faded = jnp.sum(ones * fade[:, b * BLOCK : (b + 1) * BLOCK], axis=1, keepdims=True)
                prefix = dot(ones, decay, precision=EXACT_PRECISION) + faded
                out, reach, total, state = block_step(
                    query, key, values[g, at, :], prefix, mask, state
                )
                out_ref[at, :] = out
                reach_ref[at, :] = (reach * jnp.exp(running)).astype(BF16)
                left.append((state, running + total))
            carried = tuple(left)
        return carried

    start = tuple(
        (
            jnp.zeros((values.shape[2], group[2].shape[1]), F32),
            jnp.zeros((1, group[2].shape[1]), F32),
        )
        for group in groups
    )
    (wide_state, wide_log), (narrow_state, narrow_log) = lax.fori_loop(
        0, length // (2 * BLOCK), advance, start, unroll=2
    )
    packed = jnp.concatenate([narrow_state[0:64], narrow_state[64:128]], axis=1)
    narrow_log = jnp.concatenate([narrow_log, narrow_log], axis=1)

    store_state(core_states, core, (wide_log, narrow_log, wide_state, packed))
    src = core_states.at[core]
    send(src, src, s_send.at[0], s_recv.at[0], partner)
    arrived(core_states.at[other], s_recv.at[0])
    first = load_state(core_states, 0)
    nothing = jax.tree.map(jnp.zeros_like, first)
    entering = selected(core == 1, first, nothing)
    total = combine(first, load_state(core_states, 1))
    store_state(y_states, y, total)
    src = y_states.at[y]
    for step in (1, 3, 2):
        send(src, src, s_send.at[step], s_recv.at[1 + y], {"sp_1": turn(y, step)})
    pump(0, NEAR[0:4])
    start_weights(1)
    rows_relay(0)
    for step in (1, 3, 2):
        if step == 2:
            rows_relay(1)
        arrived(y_states.at[turn(y, step)], s_recv.at[1 + turn(y, step)])

    def before(ref, here):
        inside, total = (nothing, nothing)
        for k in range(RING):
            total = combine(total, load_state(ref, k))
            inside = selected(k < here, total, inside)
        return (inside, total)

    inside, total = before(y_states, y)
    entering = combine(inside, entering)
    src = z_states.at[z]
    z_copies = [
        pltpu.make_async_remote_copy(
            src_ref=src,
            dst_ref=src,
            send_sem=s_send.at[3 + step],
            recv_sem=s_recv.at[5 + z],
            device_id={"sp_0": turn(z, step)},
            device_id_type=MESH,
        )
        for step in (1, 3, 2)
    ]
    told = pltpu.make_async_remote_copy(
        src_ref=z_before.at[0],
        dst_ref=z_before.at[0],
        send_sem=s_send.at[7],
        recv_sem=s_recv.at[9],
        device_id=partner,
        device_id_type=MESH,
    )

    @pl.when(core == 1)
    def _():
        store_state(z_states, z, total)
        for copy in z_copies:
            copy.start()

    pump(0, NEAR[4:6] + ACROSS)
    pump_group(0, SIDES)

    @pl.when(core == 1)
    def _():
        for step in (1, 3, 2):
            arrived(z_states.at[turn(z, step)], s_recv.at[5 + turn(z, step)])
        store_state(z_before, 0, before(z_states, z)[0])
        told.start()

    @pl.when(core == 0)
    def _():
        told.wait_recv()

    entering = combine(load_state(z_before, 0), entering)
    _, _, wide_state, packed = entering
    narrow_state = jnp.concatenate([packed[:, 0:64], packed[:, 64:128]], axis=0).astype(BF16)
    wide_state = wide_state.astype(BF16)

    for copy in loads[first_loads:mixed_loads]:
        copy.wait()
    for n in range(RING):
        at = pl.ds(n * rows, rows)
        parts = []
        for g, (out_ref, reach_ref, state) in enumerate(
            ((wide_out, wide_reach, wide_state), (narrow_out, narrow_reach, narrow_state))
        ):
            out = out_ref[at, :] + dot(reach_ref[at, :], state, NT)
            inverse = lax.rsqrt(jnp.mean(out * out, axis=1, keepdims=True) + EPSILON)
            out = out * inverse * channel_norm_scale[...]
            parts.append((out * jax.nn.silu(switches[g, at, :].astype(F32))).astype(BF16))
        mixed[x, at, :] = jnp.concatenate(parts, axis=1)

    own_half, across_half = (((2, 1), (2, 0)), ((0, 0), (0, 1)))
    own_rows, across_rows = (((1, None), (3, None)), ((3, None), (1, None)))
    for (right, left), to_right, to_left in (
        (own_half, 3, 4),
        (own_rows, 0, 0),
        (across_half, 5, 6),
        (across_rows, 7, 8),
    ):
        heads_to(0, *right, to_right, 1)
        heads_to(0, *left, to_left, 3)

    def heads_relay(k, landing, right, left):
        heads_wait(3, *right, k)
        heads_to(3, *right, landing, 1)
        heads_wait(1, *left, k + 1)
        heads_to(1, *left, landing, 3)

    pump(0, CORNERS[0:2])
    pump(1, NEAR[0:4])
    heads_relay(3, 0, *own_half)
    pump(0, CORNERS[2:4])
    pump_group(0, EDGES)
    pump(1, NEAR[4:6])
    pump(0, CORNERS[4:6])
    pump(1, ACROSS)
    for i in (3, 1, 2):
        for h in range(2):
            spread(i, h, 1, False)
    heads_relay(5, 1, *across_half)
    pltpu.make_async_copy(projection, projection, load_sem.at[1]).wait()
    for copy in loads[mixed_loads:]:
        copy.wait()
    heads_wait_all(768, 0)

    half = rows // 2
    upper, lower = (pl.ds(0, half), pl.ds(half, half))

    def emit(pieces, chunk, raw):
        def lines(owner, h):
            return pl.ds(pl.multiple_of(owner * rows + h * half, half), half)

        left = jnp.concatenate(
            [
                jnp.concatenate([mixed[t, lines(owner, h), :] for owner, h in pieces], axis=0)
                for t in range(RING)
            ],
            axis=1,
        )

        def tile(n, squares):
            cols = pl.ds(pl.multiple_of(n * 512, 512), 512)
            found = dot(left, projection[:, :, cols].reshape(4 * 256, 512))
            source = [sources[owner, pl.ds(h * half, half), cols] for owner, h in pieces]
            found = found + jnp.concatenate(source, axis=0).astype(F32)
            raw[:, cols] = found
            found = found * found
            return squares + (
                (found[:, 0:128] + found[:, 128:256]) + (found[:, 256:384] + found[:, 384:512])
            )

        squares = lax.fori_loop(0, model // 512, tile, jnp.zeros((rows, 128), F32))
        mean = jnp.sum(squares, axis=1, keepdims=True) / model
        inverse = lax.rsqrt(mean + EPSILON)

        def scale(n, carry):
            cols = pl.ds(pl.multiple_of(n * 512, 512), 512)
            normed[chunk, :, cols] = (raw[:, cols] * inverse * mlp_scale[:, cols]).astype(BF16)
            return carry

        lax.fori_loop(0, model // 512, scale, 0)

    def widen_all(chunk, first=0, last=ff // 128):
        def widen(n, carry):
            cols = pl.ds(pl.multiple_of(n * 256, 256), 256)
            both = dot(normed[chunk], weights[:, :, cols].reshape(model, 256))
            found = (jax.nn.silu(both[:, 0:128]) * both[:, 128:256]).astype(BF16)
            hidden[:, pl.ds(pl.multiple_of(n * 128, 128), 128)] = found
            return carry

        lax.fori_loop(first, last, widen, 0, unroll=4)

    def shrink_all(out_ref, passed=False, first=0, last=model // 256):
        def shrink(n, carry):
            cols = pl.ds(pl.multiple_of(n * 256, 256), 256)
            four = weights[pl.ds(n * 4, 4), :, pl.ds(2 * ff, ff)].reshape(256, ff)
            found = dot(hidden[...], four, NT)
            if passed:
                found = found + jnp.concatenate(
                    [passing[0, :, cols], passing[1, :, cols]], axis=0
                ).astype(F32)
            out_ref[:, cols] = found.astype(out_ref.dtype)
            return carry

        lax.fori_loop(first, last, shrink, 0, unroll=4)

    def send_sum(src, dst, k, step):
        send(src, dst, r_send.at[0], r_recv.at[k], {"tp": turn(x, step)}, False)

    left_x, right_x = (turn(x, 3), turn(x, 1))

    emit(((x, 0), (x, 1)), 3, updated)
    send(normed.at[3, lower], normed.at[2, lower], n_send.at[0], n_recv.at[0], {"tp": right_x}, False)
    send(normed.at[3, upper], normed.at[2, upper], n_send.at[0], n_recv.at[0], {"tp": left_x}, False)
    heads_wait(3, 3, None, 7)
    heads_to(3, 3, 1, 2, 1)
    heads_wait(1, 1, None, 8)
    heads_to(1, 1, 0, 2, 3)
    pump_group(1, SIDES)
    pump(1, CORNERS[0:2])
    heads_wait_all(256, 1)
    rows_opposite()
    emit(((turn(x, 2), 0), (turn(x, 2), 1)), 0, own_part)
    pump(1, CORNERS[2:4])
    pump_group(0, ENDS)
    pump(1, CORNERS[4:6])
    pump_group(0, FAR)
    pump_group(1, EDGES)
    wait_partner(0)
    widen_all(0, 0, 8)
    pump_group(1, ENDS)
    pump_group(1, FAR)
    widen_all(0, 8, ff // 128)
    wait_partner(1)
    for k in range(2):
        shrink_all(partial.at[0], first=k * (model // 512), last=(k + 1) * (model // 512))
        cols = pl.ds(k * (model // 2), model // 2)
        send_sum(partial.at[0, upper, cols], passing.at[0, :, cols], 0, 1)
        send_sum(partial.at[0, lower, cols], passing.at[1, :, cols], 0, 3)
    heads_wait_all(256, 2)
    emit(((right_x, 1), (left_x, 0)), 1, own_part)
    widen_all(1)
    shrink_all(partial.at[1])
    send_sum(partial.at[1, upper], landed.at[0, lower], 1, 1)
    send_sum(partial.at[1, lower], landed.at[1, upper], 1, 3)
    arrived(normed.at[2], n_recv.at[0])
    widen_all(2)
    arrived(passing, r_recv.at[0])
    shrink_all(partial.at[2], passed=True)
    for k in range(2):
        cols = pl.ds(k * (model // 2), model // 2)
        send_sum(partial.at[2, upper, cols], landed.at[0, upper, cols], 2 + k, 1)
        send_sum(partial.at[2, lower, cols], landed.at[1, lower, cols], 2 + k, 3)
    widen_all(3)
    shrink_all(own_part)
    arrived(landed.at[0], r_recv.at[1])

    def gather_early(n, carry):
        cols = pl.ds(pl.multiple_of(n * 256, 256), 256)
        early = jnp.concatenate([landed[1, upper, cols], landed[0, lower, cols]], axis=0)
        summed = own_part[:, cols] + early.astype(F32)
        updated[:, cols] = updated[:, cols] + 0.5 * summed
        return carry

    lax.fori_loop(0, model // 256, gather_early, 0)

    def finish(n, carry):
        cols = pl.ds(pl.multiple_of(n * 256, 256), 256)
        late = jnp.concatenate([landed[0, upper, cols], landed[1, lower, cols]], axis=0)
        layer_out[:, cols] = (updated[:, cols] + 0.5 * late.astype(F32)).astype(BF16)
        return carry

    for k in range(2):
        arrived(landed.at[0, :, pl.ds(0, model // 2)], r_recv.at[2 + k])
        lax.fori_loop(k * (model // 512), (k + 1) * (model // 512), finish, 0, unroll=2)
    for copy in sent:
        copy.wait_send()
    for shards, sem in (
        (weights.at[pl.ds(0, 15)], w_send),
        (weights.at[pl.ds(0, 16)], d_send),
        (sources.at[pl.ds(0, 2)], x_send),
        (mixed.at[pl.ds(0, 3), pl.ds(0, 3 * rows), :], m_send),
        (normed.at[0], n_send),
        (partial, r_send),
    ):
        pltpu.make_async_remote_copy(
            src_ref=shards,
            dst_ref=shards,
            send_sem=sem.at[0],
            recv_sem=sem.at[0],
            device_id=partner,
            device_id_type=MESH,
        ).wait_send()

    @pl.when(core == 1)
    def _():
        for copy in z_copies:
            copy.wait_send()
        told.wait_send()


def local(
    layer_source,
    broad_probe_tensor,
    broad_retention_preact,
    broad_floor_margin,
    slim_probe_tensor,
    slim_retention_preact,
    slim_floor_margin,
    branch_content_tensor,
    emitted_switch_preact,
    extra_log_fades,
    channel_norm_scale,
    emission_projection,
    mlp_norm_scale,
    switch_projection,
    expand_projection,
    shrink_projection,
):
    rows, model = layer_source.shape
    length = broad_probe_tensor.shape[0]
    depth, ff = switch_projection.shape
    vmem = pl.BlockSpec(memory_space=pltpu.VMEM)
    far = pl.BlockSpec(memory_space=pl.ANY)
    dma = pltpu.SemaphoreType.DMA
    return pl.pallas_call(
        layer_kernel,
        out_shape=pltpu.VMEM((rows, model), BF16),
        in_specs=[far] * 16,
        out_specs=vmem,
        scratch_shapes=[
            pltpu.VMEM((32, depth, 3 * ff), BF16),
            pltpu.VMEM((RING, rows, model), BF16),
            pltpu.VMEM((RING, length, 256), BF16),
            pltpu.VMEM((RING, 256, model), BF16),
            pltpu.VMEM((rows, model), F32),
            pltpu.VMEM((RING, rows, model), BF16),
            pltpu.VMEM((rows, ff), BF16),
            pltpu.VMEM((3, rows, model), BF16),
            pltpu.VMEM((rows, model), F32),
            pltpu.VMEM((2, rows // 2, model), BF16),
            pltpu.VMEM((2, rows, model), BF16),
            pltpu.VMEM((length, 64), F32),
            pltpu.VMEM((length, 64), F32),
            pltpu.VMEM((length, 128), F32),
            pltpu.VMEM((length, 128), F32),
            pltpu.VMEM((length, 128), BF16),
            pltpu.VMEM((length, 64), BF16),
            pltpu.VMEM((2, 208, 128), BF16),
            pltpu.VMEM((RING, 208, 128), BF16),
            pltpu.VMEM((RING, 208, 128), BF16),
            pltpu.VMEM((1, 208, 128), BF16),
            pltpu.VMEM((length, 128), BF16),
            pltpu.VMEM((length, 128), BF16),
            pltpu.VMEM((1, 128), F32),
            pltpu.VMEM((64, length), BF16),
            pltpu.VMEM((64, length), BF16),
            pltpu.VMEM((1, 64), F32),
            pltpu.VMEM((2, length, 128), BF16),
            pltpu.VMEM((2, length, 128), BF16),
            pltpu.VMEM((2, 1, length), F32),
            pltpu.VMEM((1, 128), F32),
            pltpu.VMEM((1, model), F32),
            dma((14,)),
            dma((1,)),
            dma((36,)),
            dma((1,)),
            dma((2,)),
            dma((1,)),
            dma((5,)),
            dma((1,)),
            dma((9,)),
            dma((1,)),
            dma((1,)),
            dma((8,)),
            dma((10,)),
            dma((1,)),
            dma((4,)),
        ],
        compiler_params=pltpu.CompilerParams(
            collective_id=0, has_side_effects=True, vmem_limit_bytes=62 * 1024 * 1024
        ),
    )(
        layer_source,
        broad_probe_tensor,
        broad_retention_preact,
        broad_floor_margin.reshape(1, -1),
        slim_probe_tensor.T,
        slim_retention_preact.T,
        slim_floor_margin.reshape(1, -1),
        branch_content_tensor,
        emitted_switch_preact,
        jnp.swapaxes(extra_log_fades, 1, 2),
        channel_norm_scale.reshape(1, -1),
        emission_projection,
        mlp_norm_scale.reshape(1, -1),
        switch_projection,
        expand_projection,
        shrink_projection.T,
    )


def solution(mesh):
    torus = Mesh(mesh.devices.reshape(4, 4, 2, mesh.shape["tp"]), SP_TP)
    placed = (
        P(SP_TP, None),
        P(SP, "tp"),
        P(SP, "tp"),
        P("tp"),
        P(SP, "tp"),
        P(SP, "tp"),
        P("tp"),
        P(None, SP, "tp"),
        P(None, SP, "tp"),
        P(None, SP, "tp"),
        P(),
        P(),
        P(),
        P(SP, "tp"),
        P(SP, "tp"),
        P("tp", SP),
    )
    return jax.shard_map(
        local, mesh=torus, in_specs=placed, out_specs=P(SP_TP, None), check_vma=False
    )
```

```python
import jax
import jax.numpy as jnp
from jax import lax
from jax.experimental import pallas as pl
from jax.experimental.pallas import tpu as pltpu
from jax.sharding import Mesh
from jax.sharding import PartitionSpec as P

BLOCK = 64
RING = 4
SP = ("sp_0", "sp_1", "sp_2")
SP_TP = ("sp_0", "sp_1", "sp_2", "tp")

EPSILON = 1e-06
EXACT_PRECISION = lax.Precision.HIGHEST
BF16 = jnp.bfloat16
F32 = jnp.float32
NT = (((1,), (1,)), ((), ()))
TN = (((0,), (0,)), ((), ()))
MESH = pl.DeviceIdType.MESH

NEAR = ((3, 0, 0), (1, 0, 1), (0, 3, 0), (0, 1, 1), (3, 0, 1), (1, 0, 0))
ACROSS = ((2, 0, 0), (2, 0, 1))
CORNERS = ((3, 3, 0), (3, 1, 1), (1, 3, 0), (1, 1, 1), (2, 3, 0), (2, 1, 1))
SIDES = ((0, 3, 1), (0, 1, 0))
EDGES = ((3, 3, 1), (3, 1, 0), (0, 2, 0), (0, 2, 1), (1, 3, 1), (1, 1, 0))
ENDS = ((2, 3, 1), (2, 1, 0), (3, 2, 0), (3, 2, 1))
FAR = ((1, 2, 0), (1, 2, 1), (2, 2, 0), (2, 2, 1))


PASSED = NEAR + ACROSS + CORNERS
GROUPS = (SIDES, EDGES, ENDS, FAR)


def turn(value, step):
    return lax.rem(value + step, RING)


def dot(a, b, dims=(((1,), (0,)), ((), ())), precision=None):
    return lax.dot_general(a, b, dims, preferred_element_type=F32, precision=precision)


def combine(earlier, later):
    wide_early, narrow_early, wide_state_early, narrow_state_early = earlier
    wide_late, narrow_late, wide_state_late, narrow_state_late = later
    return (
        wide_early + wide_late,
        narrow_early + narrow_late,
        jnp.exp(wide_late) * wide_state_early + wide_state_late,
        jnp.exp(narrow_late) * narrow_state_early + narrow_state_late,
    )


def split_log(log):
    first = log.astype(BF16).astype(F32)
    second = (log - first).astype(BF16).astype(F32)
    return [first, second, log - first - second]


def store_state(ref, at, state):
    wide, narrow, wide_state, narrow_state = state
    ref[at, 0:128, :] = wide_state.astype(BF16)
    ref[at, 128:192, :] = narrow_state.astype(BF16)
    lines = split_log(wide) + split_log(narrow)
    lines.append(jnp.zeros((10, wide.shape[1]), F32))
    ref[at, 192:208, :] = jnp.concatenate(lines, axis=0).astype(BF16)


def load_state(ref, at):
    lines = ref[at, 192:208, :].astype(F32)
    wide = lines[0:1] + lines[1:2] + lines[2:3]
    narrow = lines[3:4] + lines[4:5] + lines[5:6]
    return (wide, narrow, ref[at, 0:128, :].astype(F32), ref[at, 128:192, :].astype(F32))


def selected(passed, new, old):
    return jax.tree.map(lambda a, b: jnp.where(passed, a, b), new, old)


def block_step(query, key, value, prefix, mask, state):
    half = BLOCK // 2
    middle, total = (prefix[half - 1 : half, :], prefix[BLOCK - 1 : BLOCK, :])
    query_in = query * jnp.exp(prefix - middle)
    key_in = key * jnp.exp(middle - prefix)
    scores = dot(query_in.astype(BF16), key_in.astype(BF16), NT)
    scores = jnp.where(mask, scores, 0.0).astype(BF16)
    inside = dot(scores, value)
    reach = query_in * jnp.exp(middle)
    earlier = dot(reach.astype(BF16), state.astype(BF16), NT)
    leaving = (key_in * jnp.exp(total - middle)).astype(BF16)
    state = state * jnp.exp(total) + dot(value, leaving, TN)
    return (inside + earlier, reach, total, state)


def layer_kernel(
    layer_source,
    wide_query_far,
    wide_forget_far,
    wide_gap_far,
    narrow_query_far,
    narrow_forget_far,
    narrow_gap_far,
    values_far,
    switches_far,
    fades_far,
    channel_norm_scale_far,
    emission,
    mlp_scale_far,
    gate_shard,
    up_shard,
    down_shard,
    layer_out,
    weights,
    sources,
    mixed,
    projection,
    updated,
    normed,
    hidden,
    partial,
    own_part,
    passing,
    landed,
    narrow_q,
    narrow_f,
    wide_out,
    narrow_out,
    wide_reach,
    narrow_reach,
    core_states,
    y_states,
    z_states,
    z_before,
    wide_query,
    wide_forget,
    wide_gap,
    narrow_query,
    narrow_forget,
    narrow_gap,
    values,
    switches,
    fades,
    channel_norm_scale,
    mlp_scale,
    load_sem,
    w_send,
    w_recv,
    d_send,
    d_recv,
    x_send,
    x_recv,
    m_send,
    m_recv,
    n_send,
    n_recv,
    s_send,
    s_recv,
    r_send,
    r_recv,
):
    z, y, core, x = (lax.axis_index(name) for name in SP_TP)
    other = 1 - core
    rows, model = layer_source.shape
    length = wide_query.shape[0]
    ff = gate_shard.shape[1]
    depth = gate_shard.shape[0]
    sent = []

    def send(src, dst, send_sem, recv_sem, to, alone=True):
        copy = pltpu.make_async_remote_copy(
            src_ref=src,
            dst_ref=dst,
            send_sem=send_sem,
            recv_sem=recv_sem,
            device_id=to,
            device_id_type=MESH,
        )
        copy.start()
        if alone:
            sent.append(copy)

    partner = {"sp_2": other}

    def arrived(ref, sem):
        pltpu.make_async_remote_copy(
            src_ref=ref,
            dst_ref=ref,
            send_sem=sem,
            recv_sem=sem,
            device_id=partner,
            device_id_type=MESH,
        ).wait_recv()

    def place(i, j, of_core):
        first = jnp.where(of_core == 0, y, z)
        second = jnp.where(of_core == 0, z, y)
        first, second = (turn(first, i), turn(second, j))
        return (
            jnp.where(of_core == 0, second, first),
            jnp.where(of_core == 0, first, second),
        )

    def slot(i, j, of_core):
        at_z, at_y = place(i, j, of_core)
        return at_z * 8 + at_y * 2 + of_core

    half_depth = depth // 2

    columns_of = (pl.ds(0, 2 * ff), pl.ds(2 * ff, ff))

    def shard(i, j, h, part, of_core):
        lines = pl.ds(h * half_depth, half_depth)
        return weights.at[slot(i, j, of_core), lines, columns_of[part]]

    def shard_part(i, j, part, of_core):
        return weights.at[slot(i, j, of_core), :, columns_of[part]]

    def toward(i, j):
        at_z, at_y = place(i, j, core)
        return {"sp_0": at_z, "sp_1": at_y}

    def mark(i, j, h, part):
        if (i, j, h) in PASSED:
            return part * 18 + PASSED.index((i, j, h))
        return part * 18 + 14 + [(i, j, h) in group for group in GROUPS].index(True)

    def forward(i, j, h, part, step, landing):
        src = shard(i, j, h, part, core)
        at = w_recv.at[mark(*landing, h, part)]
        send(src, src, w_send.at[0], at, toward(*step), False)

    def hand_over(i, j, part):
        src = shard_part(i, j, part, core)
        landing = part
        if part == 1:
            landing = jnp.where(core == 0, 1 if j in (0, 3) else 2, 1 if i in (0, 3) else 2)
        send(src, src, d_send.at[0], d_recv.at[landing], partner, False)

    def spread(i, h, part, passed_on):
        if (h == 0) == passed_on:
            forward(i, 0, h, part, (0, 1), (i, 3))
        else:
            forward(i, 0, h, part, (0, 3), (i, 1))

    handed = {}

    def pump(part, arrivals):
        for i, j, h in arrivals:
            arrived(shard(i, j, h, part, core), w_recv.at[mark(i, j, h, part)])
            if j == 0:
                if (i, h) == (3, 0):
                    forward(i, 0, h, part, (1, 0), (2, 0))
                if (i, h) == (1, 1):
                    forward(i, 0, h, part, (3, 0), (2, 0))
                spread(i, h, part, True)
                if part == 0:
                    spread(i, h, part, False)
            else:
                if (j, h) == (3, 0):
                    forward(i, j, h, part, (0, 1), (i, 2))
                if (j, h) == (1, 1):
                    forward(i, j, h, part, (0, 3), (i, 2))
            seen(i, j, part)

    def seen(i, j, part):
        handed[(i, j, part)] = handed.get((i, j, part), 0) + 1
        if handed[(i, j, part)] == 2:
            hand_over(i, j, part)

    def pump_group(part, group):
        halves = weights.at[pl.ds(0, len(group) // 2), :, columns_of[part]]
        arrived(halves, w_recv.at[mark(*group[0], part)])
        for i, j, _ in group:
            seen(i, j, part)

    def start_weights(part):
        for h in range(2):
            forward(0, 0, h, part, (1, 0), (3, 0))
            forward(0, 0, 1 - h, part, (3, 0), (1, 0))
            forward(0, 0, h, part, (0, 1), (0, 3))
            forward(0, 0, 1 - h, part, (0, 3), (0, 1))
        hand_over(0, 0, part)

    def wait_partner(part):
        arrived(weights.at[pl.ds(0, 16), :, columns_of[part]], d_recv.at[part])

    def wait_partner_half(near):
        arrived(weights.at[pl.ds(0, 8), :, columns_of[1]], d_recv.at[1 if near else 2])

    def rows_piece(step, q):
        quarter = rows // 4
        return sources.at[turn(x, step), pl.ds(q * quarter, quarter), :]

    def rows_to(step, q, landing, to):
        src = rows_piece(step, q)
        at = x_recv.at[min(landing, 4)]
        send(src, src, x_send.at[0], at, {"tp": turn(x, to)}, False)

    def rows_start():
        for k in range(2):
            rows_to(0, k, k, 1)
            rows_to(0, 2 + k, 2 + k, 3)

    def rows_relay(k):
        arrived(rows_piece(3, k), x_recv.at[k])
        rows_to(3, k, 4 + k, 1)
        arrived(rows_piece(1, 2 + k), x_recv.at[2 + k])
        rows_to(1, 2 + k, 6 + k, 3)

    def rows_opposite():
        arrived(sources.at[turn(x, 2)], x_recv.at[4])

    def head_piece(sender, r, h):
        owner = turn(x, (sender + r) % RING)
        at = owner * rows + (0 if h is None else h * (rows // 2))
        count = rows if h is None else rows // 2
        return mixed.at[turn(x, sender), pl.ds(pl.multiple_of(at, 128), count), :]

    def heads_to(sender, r, h, k, step):
        src = head_piece(sender, r, h)
        send(src, src, m_send.at[0], m_recv.at[k], {"tp": turn(x, step)}, False)

    def heads_wait_all(count, k):
        arrived(mixed.at[0, pl.ds(0, count), :], m_recv.at[k])

    def heads_wait(sender, r, h, k):
        arrived(head_piece(sender, r, h), m_recv.at[k])

    barrier = pltpu.get_barrier_semaphore()
    pl.semaphore_signal(barrier, inc=1, device_id=partner, device_id_type=MESH)
    for name, here in (("sp_0", z), ("sp_1", y), ("tp", x)):
        for step in (1, 2, 3):
            pl.semaphore_signal(
                barrier, inc=1, device_id={name: turn(here, step)}, device_id_type=MESH
            )

    me = slot(0, 0, core)
    loads = []

    def load(src, dst, shared=None):
        sem = load_sem.at[2 + len(loads) if shared is None else shared]
        copy = pltpu.make_async_copy(src, dst, sem)
        copy.start()
        if shared is None:
            loads.append(copy)

    for n in range(ff // 128):
        cols = pl.ds(n * 128, 128)
        load(gate_shard.at[:, cols], weights.at[me, :, pl.ds(n * 256, 128)], 0)
        load(up_shard.at[:, cols], weights.at[me, :, pl.ds(n * 256 + 128, 128)], 0)
    load(down_shard, weights.at[me, :, pl.ds(2 * ff, ff)], 0)
    load(layer_source, sources.at[x])
    shard_loads = len(loads)
    for src, dst in (
        (wide_query_far, wide_query),
        (wide_forget_far, wide_forget),
        (wide_gap_far, wide_gap),
        (narrow_query_far, narrow_query),
        (narrow_forget_far, narrow_forget),
        (narrow_gap_far, narrow_gap),
        (values_far, values),
        (fades_far, fades),
    ):
        load(src, dst)
    first_loads = len(loads)
    load(switches_far, switches)
    load(channel_norm_scale_far, channel_norm_scale)
    mixed_loads = len(loads)
    load(mlp_scale_far, mlp_scale)
    for t in range(RING):
        for g in range(2):
            load(emission.at[g, pl.ds(t * 128, 128), :], projection.at[t, pl.ds(g * 128, 128), :], 1)

    pl.semaphore_wait(barrier, 10)

    pltpu.make_async_copy(weights.at[me], weights.at[me], load_sem.at[0]).wait()
    for copy in loads[:shard_loads]:
        copy.wait()
    start_weights(0)
    rows_start()
    for copy in loads[shard_loads:first_loads]:
        copy.wait()
    for n in range(length // 128):
        cols = pl.ds(n * 128, 128)
        narrow_q[cols, :] = narrow_query[:, cols].astype(F32).T
        narrow_f[cols, :] = narrow_forget[:, cols].astype(F32).T
    line = lax.broadcasted_iota(jnp.int32, (BLOCK, BLOCK), 0)
    column = lax.broadcasted_iota(jnp.int32, (BLOCK, BLOCK), 1)
    mask = line >= column
    ones = jnp.where(mask, 1.0, 0.0)
    groups = (
        (wide_query, wide_forget, wide_gap, wide_out, wide_reach),
        (narrow_q, narrow_f, narrow_gap, narrow_out, narrow_reach),
    )

    def advance(pair, carried):
        for b in range(2):
            at = pl.ds(pl.multiple_of((pair * 2 + b) * BLOCK, BLOCK), BLOCK)
            left = []
            for g in range(2):
                query_ref, forget_ref, gap_ref, out_ref, reach_ref = groups[g]
                state, running = carried[g]
                key = gap_ref[...] * jax.nn.sigmoid(-forget_ref[at, :].astype(F32))
                decay = jnp.log1p(-key)
                query = jax.nn.silu(query_ref[at, :].astype(F32)) * key.shape[1] ** (-0.5)
                fade = fades[g, :, pl.ds(pl.multiple_of(pair * 2 * BLOCK, 2 * BLOCK), 2 * BLOCK)]
                faded = jnp.sum(ones * fade[:, b * BLOCK : (b + 1) * BLOCK], axis=1, keepdims=True)
                prefix = dot(ones, decay, precision=EXACT_PRECISION) + faded
                out, reach, total, state = block_step(
                    query, key, values[g, at, :], prefix, mask, state
                )
                out_ref[at, :] = out
                reach_ref[at, :] = (reach * jnp.exp(running)).astype(BF16)
                left.append((state, running + total))
            carried = tuple(left)
        return carried

    start = tuple(
        (
            jnp.zeros((values.shape[2], group[2].shape[1]), F32),
            jnp.zeros((1, group[2].shape[1]), F32),
        )
        for group in groups
    )
    (wide_state, wide_log), (narrow_state, narrow_log) = lax.fori_loop(
        0, length // (2 * BLOCK), advance, start, unroll=2
    )
    packed = jnp.concatenate([narrow_state[0:64], narrow_state[64:128]], axis=1)
    narrow_log = jnp.concatenate([narrow_log, narrow_log], axis=1)

    store_state(core_states, core, (wide_log, narrow_log, wide_state, packed))
    src = core_states.at[core]
    send(src, src, s_send.at[0], s_recv.at[0], partner)
    arrived(core_states.at[other], s_recv.at[0])
    first = load_state(core_states, 0)
    nothing = jax.tree.map(jnp.zeros_like, first)
    entering = selected(core == 1, first, nothing)
    total = combine(first, load_state(core_states, 1))
    store_state(y_states, y, total)
    src = y_states.at[y]
    for step in (1, 3, 2):
        send(src, src, s_send.at[step], s_recv.at[1 + y], {"sp_1": turn(y, step)})
    pump(0, NEAR[0:4])
    start_weights(1)
    rows_relay(0)
    for step in (1, 3, 2):
        if step == 2:
            rows_relay(1)
        arrived(y_states.at[turn(y, step)], s_recv.at[1 + turn(y, step)])

    def before(ref, here):
        inside, total = (nothing, nothing)
        for k in range(RING):
            total = combine(total, load_state(ref, k))
            inside = selected(k < here, total, inside)
        return (inside, total)

    inside, total = before(y_states, y)
    entering = combine(inside, entering)
    src = z_states.at[z]
    z_copies = [
        pltpu.make_async_remote_copy(
            src_ref=src,
            dst_ref=src,
            send_sem=s_send.at[3 + step],
            recv_sem=s_recv.at[5 + z],
            device_id={"sp_0": turn(z, step)},
            device_id_type=MESH,
        )
        for step in (1, 3, 2)
    ]
    told = pltpu.make_async_remote_copy(
        src_ref=z_before.at[0],
        dst_ref=z_before.at[0],
        send_sem=s_send.at[7],
        recv_sem=s_recv.at[9],
        device_id=partner,
        device_id_type=MESH,
    )

    @pl.when(core == 1)
    def _():
        store_state(z_states, z, total)
        for copy in z_copies:
            copy.start()

    pump(0, NEAR[4:6] + ACROSS)
    pump_group(0, SIDES)

    @pl.when(core == 1)
    def _():
        for step in (1, 3, 2):
            arrived(z_states.at[turn(z, step)], s_recv.at[5 + turn(z, step)])
        store_state(z_before, 0, before(z_states, z)[0])
        told.start()

    @pl.when(core == 0)
    def _():
        told.wait_recv()

    entering = combine(load_state(z_before, 0), entering)
    _, _, wide_state, packed = entering
    narrow_state = jnp.concatenate([packed[:, 0:64], packed[:, 64:128]], axis=0).astype(BF16)
    wide_state = wide_state.astype(BF16)

    for copy in loads[first_loads:mixed_loads]:
        copy.wait()
    for n in range(RING):
        at = pl.ds(n * rows, rows)
        parts = []
        for g, (out_ref, reach_ref, state) in enumerate(
            ((wide_out, wide_reach, wide_state), (narrow_out, narrow_reach, narrow_state))
        ):
            out = out_ref[at, :] + dot(reach_ref[at, :], state, NT)
            inverse = lax.rsqrt(jnp.mean(out * out, axis=1, keepdims=True) + EPSILON)
            out = out * inverse * channel_norm_scale[...]
            parts.append((out * jax.nn.silu(switches[g, at, :].astype(F32))).astype(BF16))
        mixed[x, at, :] = jnp.concatenate(parts, axis=1)

    own_half, across_half = (((2, 1), (2, 0)), ((0, 0), (0, 1)))
    own_rows, across_rows = (((1, None), (3, None)), ((3, None), (1, None)))
    for (right, left), to_right, to_left in (
        (own_half, 3, 4),
        (own_rows, 0, 0),
        (across_half, 5, 6),
        (across_rows, 7, 8),
    ):
        heads_to(0, *right, to_right, 1)
        heads_to(0, *left, to_left, 3)

    def heads_relay(k, landing, right, left):
        heads_wait(3, *right, k)
        heads_to(3, *right, landing, 1)
        heads_wait(1, *left, k + 1)
        heads_to(1, *left, landing, 3)

    pump(0, CORNERS[0:2])
    pump(1, NEAR[0:4])
    heads_relay(3, 0, *own_half)
    pump(0, CORNERS[2:4])
    pump_group(0, EDGES)
    pump(1, NEAR[4:6])
    pump(0, CORNERS[4:6])
    pump(1, ACROSS)
    for i in (3, 1, 2):
        for h in range(2):
            spread(i, h, 1, False)
    heads_relay(5, 1, *across_half)
    pltpu.make_async_copy(projection, projection, load_sem.at[1]).wait()
    for copy in loads[mixed_loads:]:
        copy.wait()
    heads_wait_all(768, 0)

    half = rows // 2
    upper, lower = (pl.ds(0, half), pl.ds(half, half))

    def emit(pieces, chunk, raw):
        def lines(owner, h):
            return pl.ds(pl.multiple_of(owner * rows + h * half, half), half)

        left = jnp.concatenate(
            [
                jnp.concatenate([mixed[t, lines(owner, h), :] for owner, h in pieces], axis=0)
                for t in range(RING)
            ],
            axis=1,
        )

        def tile(n, squares):
            cols = pl.ds(pl.multiple_of(n * 512, 512), 512)
            found = dot(left, projection[:, :, cols].reshape(4 * 256, 512))
            source = [sources[owner, pl.ds(h * half, half), cols] for owner, h in pieces]
            found = found + jnp.concatenate(source, axis=0).astype(F32)
            raw[:, cols] = found
            found = found * found
            return squares + (
                (found[:, 0:128] + found[:, 128:256]) + (found[:, 256:384] + found[:, 384:512])
            )

        squares = lax.fori_loop(0, model // 512, tile, jnp.zeros((rows, 128), F32))
        mean = jnp.sum(squares, axis=1, keepdims=True) / model
        inverse = lax.rsqrt(mean + EPSILON)

        def scale(n, carry):
            cols = pl.ds(pl.multiple_of(n * 512, 512), 512)
            normed[chunk, :, cols] = (raw[:, cols] * inverse * mlp_scale[:, cols]).astype(BF16)
            return carry

        lax.fori_loop(0, model // 512, scale, 0)

    def widen_all(chunk, first=0, last=ff // 128):
        def widen(n, carry):
            cols = pl.ds(pl.multiple_of(n * 256, 256), 256)
            both = dot(normed[chunk], weights[:, :, cols].reshape(model, 256))
            found = (jax.nn.silu(both[:, 0:128]) * both[:, 128:256]).astype(BF16)
            hidden[:, pl.ds(pl.multiple_of(n * 128, 128), 128)] = found
            return carry

        lax.fori_loop(first, last, widen, 0, unroll=4)

    def shrink_tile(out_ref, n, passed=False):
        cols = pl.ds(pl.multiple_of(n * 256, 256), 256)
        four = weights[pl.ds(n * 4, 4), :, pl.ds(2 * ff, ff)].reshape(256, ff)
        found = dot(hidden[...], four, NT)
        if passed:
            found = found + jnp.concatenate(
                [passing[0, :, cols], passing[1, :, cols]], axis=0
            ).astype(F32)
        out_ref[:, cols] = found.astype(out_ref.dtype)

    def shrink_all(out_ref, passed=False):
        def shrink(n, carry):
            shrink_tile(out_ref, n, passed)
            return carry

        lax.fori_loop(0, model // 256, shrink, 0, unroll=4)

    def send_sum(src, dst, k, step):
        send(src, dst, r_send.at[0], r_recv.at[k], {"tp": turn(x, step)}, False)

    left_x, right_x = (turn(x, 3), turn(x, 1))

    emit(((x, 0), (x, 1)), 3, updated)
    send(normed.at[3, lower], normed.at[2, lower], n_send.at[0], n_recv.at[0], {"tp": right_x}, False)
    send(normed.at[3, upper], normed.at[2, upper], n_send.at[0], n_recv.at[0], {"tp": left_x}, False)
    heads_wait(3, 3, None, 7)
    heads_to(3, 3, 1, 2, 1)
    heads_wait(1, 1, None, 8)
    heads_to(1, 1, 0, 2, 3)
    pump_group(1, SIDES)
    pump(1, CORNERS[0:2])
    heads_wait_all(256, 1)
    rows_opposite()
    emit(((turn(x, 2), 0), (turn(x, 2), 1)), 0, own_part)
    pump(1, CORNERS[2:4])
    pump_group(0, ENDS)
    pump_group(0, FAR)
    pump(1, CORNERS[4:5])
    wait_partner(0)
    widen_all(0, 0, 4)
    pump(1, CORNERS[5:6])
    pump_group(1, EDGES)
    widen_all(0, 4, 8)
    pump_group(1, ENDS)
    widen_all(0, 8, ff // 128)
    for near, steps in ((True, (0, 3)), (False, (1, 2))):
        if not near:
            pump_group(1, FAR)
        wait_partner_half(near)
        for step in steps:
            for n in range(2):
                shrink_tile(partial.at[0], turn(z, step) * 2 + n)
        for step in steps:
            cols = pl.ds(pl.multiple_of(turn(z, step) * 512, 512), 512)
            send_sum(partial.at[0, upper, cols], passing.at[0, :, cols], 0, 1)
            send_sum(partial.at[0, lower, cols], passing.at[1, :, cols], 0, 3)
    heads_wait_all(256, 2)
    emit(((right_x, 1), (left_x, 0)), 1, own_part)
    widen_all(1)
    shrink_all(partial.at[1])
    send_sum(partial.at[1, upper], landed.at[0, lower], 1, 1)
    send_sum(partial.at[1, lower], landed.at[1, upper], 1, 3)
    arrived(normed.at[2], n_recv.at[0])
    widen_all(2)
    arrived(passing, r_recv.at[0])
    shrink_all(partial.at[2], passed=True)
    for k in range(2):
        cols = pl.ds(k * (model // 2), model // 2)
        send_sum(partial.at[2, upper, cols], landed.at[0, upper, cols], 2 + k, 1)
        send_sum(partial.at[2, lower, cols], landed.at[1, lower, cols], 2 + k, 3)
    widen_all(3)
    shrink_all(own_part)
    arrived(landed.at[0], r_recv.at[1])

    def gather_early(n, carry):
        cols = pl.ds(pl.multiple_of(n * 256, 256), 256)
        early = jnp.concatenate([landed[1, upper, cols], landed[0, lower, cols]], axis=0)
        summed = own_part[:, cols] + early.astype(F32)
        updated[:, cols] = updated[:, cols] + 0.5 * summed
        return carry

    lax.fori_loop(0, model // 256, gather_early, 0)

    def finish(n, carry):
        cols = pl.ds(pl.multiple_of(n * 256, 256), 256)
        late = jnp.concatenate([landed[0, upper, cols], landed[1, lower, cols]], axis=0)
        layer_out[:, cols] = (updated[:, cols] + 0.5 * late.astype(F32)).astype(BF16)
        return carry

    for k in range(2):
        arrived(landed.at[0, :, pl.ds(0, model // 2)], r_recv.at[2 + k])
        lax.fori_loop(k * (model // 512), (k + 1) * (model // 512), finish, 0, unroll=2)
    for copy in sent:
        copy.wait_send()
    for shards, sem in (
        (weights.at[pl.ds(0, 15)], w_send),
        (weights.at[pl.ds(0, 16)], d_send),
        (sources.at[pl.ds(0, 2)], x_send),
        (mixed.at[pl.ds(0, 3), pl.ds(0, 3 * rows), :], m_send),
        (normed.at[0], n_send),
        (partial, r_send),
    ):
        pltpu.make_async_remote_copy(
            src_ref=shards,
            dst_ref=shards,
            send_sem=sem.at[0],
            recv_sem=sem.at[0],
            device_id=partner,
            device_id_type=MESH,
        ).wait_send()

    @pl.when(core == 1)
    def _():
        for copy in z_copies:
            copy.wait_send()
        told.wait_send()


def local(
    layer_source,
    broad_probe_tensor,
    broad_retention_preact,
    broad_floor_margin,
    slim_probe_tensor,
    slim_retention_preact,
    slim_floor_margin,
    branch_content_tensor,
    emitted_switch_preact,
    extra_log_fades,
    channel_norm_scale,
    emission_projection,
    mlp_norm_scale,
    switch_projection,
    expand_projection,
    shrink_projection,
):
    rows, model = layer_source.shape
    length = broad_probe_tensor.shape[0]
    depth, ff = switch_projection.shape
    vmem = pl.BlockSpec(memory_space=pltpu.VMEM)
    far = pl.BlockSpec(memory_space=pl.ANY)
    dma = pltpu.SemaphoreType.DMA
    return pl.pallas_call(
        layer_kernel,
        out_shape=pltpu.VMEM((rows, model), BF16),
        in_specs=[far] * 16,
        out_specs=vmem,
        scratch_shapes=[
            pltpu.VMEM((32, depth, 3 * ff), BF16),
            pltpu.VMEM((RING, rows, model), BF16),
            pltpu.VMEM((RING, length, 256), BF16),
            pltpu.VMEM((RING, 256, model), BF16),
            pltpu.VMEM((rows, model), F32),
            pltpu.VMEM((RING, rows, model), BF16),
            pltpu.VMEM((rows, ff), BF16),
            pltpu.VMEM((3, rows, model), BF16),
            pltpu.VMEM((rows, model), F32),
            pltpu.VMEM((2, rows // 2, model), BF16),
            pltpu.VMEM((2, rows, model), BF16),
            pltpu.VMEM((length, 64), F32),
            pltpu.VMEM((length, 64), F32),
            pltpu.VMEM((length, 128), F32),
            pltpu.VMEM((length, 128), F32),
            pltpu.VMEM((length, 128), BF16),
            pltpu.VMEM((length, 64), BF16),
            pltpu.VMEM((2, 208, 128), BF16),
            pltpu.VMEM((RING, 208, 128), BF16),
            pltpu.VMEM((RING, 208, 128), BF16),
            pltpu.VMEM((1, 208, 128), BF16),
            pltpu.VMEM((length, 128), BF16),
            pltpu.VMEM((length, 128), BF16),
            pltpu.VMEM((1, 128), F32),
            pltpu.VMEM((64, length), BF16),
            pltpu.VMEM((64, length), BF16),
            pltpu.VMEM((1, 64), F32),
            pltpu.VMEM((2, length, 128), BF16),
            pltpu.VMEM((2, length, 128), BF16),
            pltpu.VMEM((2, 1, length), F32),
            pltpu.VMEM((1, 128), F32),
            pltpu.VMEM((1, model), F32),
            dma((14,)),
            dma((1,)),
            dma((36,)),
            dma((1,)),
            dma((3,)),
            dma((1,)),
            dma((5,)),
            dma((1,)),
            dma((9,)),
            dma((1,)),
            dma((1,)),
            dma((8,)),
            dma((10,)),
            dma((1,)),
            dma((4,)),
        ],
        compiler_params=pltpu.CompilerParams(
            collective_id=0, has_side_effects=True, vmem_limit_bytes=62 * 1024 * 1024
        ),
    )(
        layer_source,
        broad_probe_tensor,
        broad_retention_preact,
        broad_floor_margin.reshape(1, -1),
        slim_probe_tensor.T,
        slim_retention_preact.T,
        slim_floor_margin.reshape(1, -1),
        branch_content_tensor,
        emitted_switch_preact,
        jnp.swapaxes(extra_log_fades, 1, 2),
        channel_norm_scale.reshape(1, -1),
        emission_projection,
        mlp_norm_scale.reshape(1, -1),
        switch_projection,
        expand_projection,
        shrink_projection.T,
    )


def solution(mesh):
    torus = Mesh(mesh.devices.reshape(4, 4, 2, mesh.shape["tp"]), SP_TP)
    placed = (
        P(SP_TP, None),
        P(SP, "tp"),
        P(SP, "tp"),
        P("tp"),
        P(SP, "tp"),
        P(SP, "tp"),
        P("tp"),
        P(None, SP, "tp"),
        P(None, SP, "tp"),
        P(None, SP, "tp"),
        P(),
        P(),
        P(),
        P(SP, "tp"),
        P(SP, "tp"),
        P("tp", SP),
    )
    return jax.shard_map(
        local, mesh=torus, in_specs=placed, out_specs=P(SP_TP, None), check_vma=False
    )
```

```python
import jax
import jax.numpy as jnp
from jax import lax
from jax.experimental import pallas as pl
from jax.experimental.pallas import tpu as pltpu
from jax.sharding import Mesh
from jax.sharding import PartitionSpec as P

BLOCK = 64
RING = 4
SP = ("sp_0", "sp_1", "sp_2")
SP_TP = ("sp_0", "sp_1", "sp_2", "tp")

EPSILON = 1e-06
EXACT_PRECISION = lax.Precision.HIGHEST
BF16 = jnp.bfloat16
F32 = jnp.float32
NT = (((1,), (1,)), ((), ()))
TN = (((0,), (0,)), ((), ()))
MESH = pl.DeviceIdType.MESH

NEAR = ((3, 0, 0), (1, 0, 1), (0, 3, 0), (0, 1, 1), (3, 0, 1), (1, 0, 0))
ACROSS = ((2, 0, 0), (2, 0, 1))
CORNERS = ((3, 3, 0), (3, 1, 1), (1, 3, 0), (1, 1, 1), (2, 3, 0), (2, 1, 1))
SIDES = ((0, 3, 1), (0, 1, 0))
EDGES = ((3, 3, 1), (3, 1, 0), (0, 2, 0), (0, 2, 1), (1, 3, 1), (1, 1, 0))
ENDS = ((2, 3, 1), (2, 1, 0), (3, 2, 0), (3, 2, 1))
FAR = ((1, 2, 0), (1, 2, 1), (2, 2, 0), (2, 2, 1))


PASSED = NEAR + ACROSS + CORNERS
GROUPS = (SIDES, EDGES, ENDS, FAR)


def turn(value, step):
    return lax.rem(value + step, RING)


def dot(a, b, dims=(((1,), (0,)), ((), ())), precision=None):
    return lax.dot_general(a, b, dims, preferred_element_type=F32, precision=precision)


def combine(earlier, later):
    wide_early, narrow_early, wide_state_early, narrow_state_early = earlier
    wide_late, narrow_late, wide_state_late, narrow_state_late = later
    return (
        wide_early + wide_late,
        narrow_early + narrow_late,
        jnp.exp(wide_late) * wide_state_early + wide_state_late,
        jnp.exp(narrow_late) * narrow_state_early + narrow_state_late,
    )


def split_log(log):
    first = log.astype(BF16).astype(F32)
    second = (log - first).astype(BF16).astype(F32)
    return [first, second, log - first - second]


def store_state(ref, at, state):
    wide, narrow, wide_state, narrow_state = state
    ref[at, 0:128, :] = wide_state.astype(BF16)
    ref[at, 128:192, :] = narrow_state.astype(BF16)
    lines = split_log(wide) + split_log(narrow)
    lines.append(jnp.zeros((10, wide.shape[1]), F32))
    ref[at, 192:208, :] = jnp.concatenate(lines, axis=0).astype(BF16)


def load_state(ref, at):
    lines = ref[at, 192:208, :].astype(F32)
    wide = lines[0:1] + lines[1:2] + lines[2:3]
    narrow = lines[3:4] + lines[4:5] + lines[5:6]
    return (wide, narrow, ref[at, 0:128, :].astype(F32), ref[at, 128:192, :].astype(F32))


def selected(passed, new, old):
    return jax.tree.map(lambda a, b: jnp.where(passed, a, b), new, old)


def block_step(query, key, value, prefix, mask, state):
    half = BLOCK // 2
    middle, total = (prefix[half - 1 : half, :], prefix[BLOCK - 1 : BLOCK, :])
    query_in = query * jnp.exp(prefix - middle)
    key_in = key * jnp.exp(middle - prefix)
    scores = dot(query_in.astype(BF16), key_in.astype(BF16), NT)
    scores = jnp.where(mask, scores, 0.0).astype(BF16)
    inside = dot(scores, value)
    reach = query_in * jnp.exp(middle)
    earlier = dot(reach.astype(BF16), state.astype(BF16), NT)
    leaving = (key_in * jnp.exp(total - middle)).astype(BF16)
    state = state * jnp.exp(total) + dot(value, leaving, TN)
    return (inside + earlier, reach, total, state)


def layer_kernel(
    layer_source,
    wide_query_far,
    wide_forget_far,
    wide_gap_far,
    narrow_query_far,
    narrow_forget_far,
    narrow_gap_far,
    values_far,
    switches_far,
    fades_far,
    channel_norm_scale_far,
    emission,
    mlp_scale_far,
    gate_shard,
    up_shard,
    down_shard,
    layer_out,
    weights,
    sources,
    mixed,
    projection,
    updated,
    normed,
    hidden,
    partial,
    own_part,
    passing,
    landed,
    narrow_q,
    narrow_f,
    wide_out,
    narrow_out,
    wide_reach,
    narrow_reach,
    core_states,
    y_states,
    z_states,
    z_before,
    wide_query,
    wide_forget,
    wide_gap,
    narrow_query,
    narrow_forget,
    narrow_gap,
    values,
    switches,
    fades,
    channel_norm_scale,
    mlp_scale,
    load_sem,
    w_send,
    w_recv,
    d_send,
    d_recv,
    x_send,
    x_recv,
    m_send,
    m_recv,
    n_send,
    n_recv,
    s_send,
    s_recv,
    r_send,
    r_recv,
):
    z, y, core, x = (lax.axis_index(name) for name in SP_TP)
    other = 1 - core
    rows, model = layer_source.shape
    length = wide_query.shape[0]
    ff = gate_shard.shape[1]
    depth = gate_shard.shape[0]
    sent = []

    def send(src, dst, send_sem, recv_sem, to, alone=True):
        copy = pltpu.make_async_remote_copy(
            src_ref=src,
            dst_ref=dst,
            send_sem=send_sem,
            recv_sem=recv_sem,
            device_id=to,
            device_id_type=MESH,
        )
        copy.start()
        if alone:
            sent.append(copy)

    partner = {"sp_2": other}

    def arrived(ref, sem):
        pltpu.make_async_remote_copy(
            src_ref=ref,
            dst_ref=ref,
            send_sem=sem,
            recv_sem=sem,
            device_id=partner,
            device_id_type=MESH,
        ).wait_recv()

    def place(i, j, of_core):
        first = jnp.where(of_core == 0, y, z)
        second = jnp.where(of_core == 0, z, y)
        first, second = (turn(first, i), turn(second, j))
        return (
            jnp.where(of_core == 0, second, first),
            jnp.where(of_core == 0, first, second),
        )

    def slot(i, j, of_core):
        at_z, at_y = place(i, j, of_core)
        return at_z * 8 + at_y * 2 + of_core

    half_depth = depth // 2

    columns_of = (pl.ds(0, 2 * ff), pl.ds(2 * ff, ff))

    def shard(i, j, h, part, of_core):
        lines = pl.ds(h * half_depth, half_depth)
        return weights.at[slot(i, j, of_core), lines, columns_of[part]]

    def shard_part(i, j, part, of_core):
        return weights.at[slot(i, j, of_core), :, columns_of[part]]

    def toward(i, j):
        at_z, at_y = place(i, j, core)
        return {"sp_0": at_z, "sp_1": at_y}

    def mark(i, j, h, part):
        if (i, j, h) in PASSED:
            return part * 18 + PASSED.index((i, j, h))
        return part * 18 + 14 + [(i, j, h) in group for group in GROUPS].index(True)

    def forward(i, j, h, part, step, landing):
        src = shard(i, j, h, part, core)
        at = w_recv.at[mark(*landing, h, part)]
        send(src, src, w_send.at[0], at, toward(*step), False)

    def hand_over(i, j, part):
        src = shard_part(i, j, part, core)
        landing = part
        if part == 1:
            landing = jnp.where(core == 0, 1 if j in (0, 3) else 2, 1 if i in (0, 3) else 2)
        send(src, src, d_send.at[0], d_recv.at[landing], partner, False)

    def spread(i, h, part, passed_on):
        if (h == 0) == passed_on:
            forward(i, 0, h, part, (0, 1), (i, 3))
        else:
            forward(i, 0, h, part, (0, 3), (i, 1))

    handed = {}

    def pump(part, arrivals):
        for i, j, h in arrivals:
            arrived(shard(i, j, h, part, core), w_recv.at[mark(i, j, h, part)])
            if j == 0:
                if (i, h) == (3, 0):
                    forward(i, 0, h, part, (1, 0), (2, 0))
                if (i, h) == (1, 1):
                    forward(i, 0, h, part, (3, 0), (2, 0))
                spread(i, h, part, True)
                if part == 0:
                    spread(i, h, part, False)
            else:
                if (j, h) == (3, 0):
                    forward(i, j, h, part, (0, 1), (i, 2))
                if (j, h) == (1, 1):
                    forward(i, j, h, part, (0, 3), (i, 2))
            seen(i, j, part)

    def seen(i, j, part):
        handed[(i, j, part)] = handed.get((i, j, part), 0) + 1
        if handed[(i, j, part)] == 2:
            hand_over(i, j, part)

    def pump_group(part, group):
        halves = weights.at[pl.ds(0, len(group) // 2), :, columns_of[part]]
        arrived(halves, w_recv.at[mark(*group[0], part)])
        for i, j, _ in group:
            seen(i, j, part)

    def start_weights(part):
        for h in range(2):
            forward(0, 0, h, part, (1, 0), (3, 0))
            forward(0, 0, 1 - h, part, (3, 0), (1, 0))
            forward(0, 0, h, part, (0, 1), (0, 3))
            forward(0, 0, 1 - h, part, (0, 3), (0, 1))
        hand_over(0, 0, part)

    def wait_partner(part):
        arrived(weights.at[pl.ds(0, 16), :, columns_of[part]], d_recv.at[part])

    def wait_partner_half(near):
        arrived(weights.at[pl.ds(0, 8), :, columns_of[1]], d_recv.at[1 if near else 2])

    def rows_piece(step, q):
        quarter = rows // 4
        return sources.at[turn(x, step), pl.ds(q * quarter, quarter), :]

    def rows_to(step, q, landing, to):
        src = rows_piece(step, q)
        at = x_recv.at[min(landing, 4)]
        send(src, src, x_send.at[0], at, {"tp": turn(x, to)}, False)

    def rows_start():
        for k in range(2):
            rows_to(0, k, k, 1)
            rows_to(0, 2 + k, 2 + k, 3)

    def rows_relay(k):
        arrived(rows_piece(3, k), x_recv.at[k])
        rows_to(3, k, 4 + k, 1)
        arrived(rows_piece(1, 2 + k), x_recv.at[2 + k])
        rows_to(1, 2 + k, 6 + k, 3)

    def rows_opposite():
        arrived(sources.at[turn(x, 2)], x_recv.at[4])

    def head_piece(sender, r, h):
        owner = turn(x, (sender + r) % RING)
        at = owner * rows + (0 if h is None else h * (rows // 2))
        count = rows if h is None else rows // 2
        return mixed.at[turn(x, sender), pl.ds(pl.multiple_of(at, 128), count), :]

    def heads_to(sender, r, h, k, step):
        src = head_piece(sender, r, h)
        send(src, src, m_send.at[0], m_recv.at[k], {"tp": turn(x, step)}, False)

    def heads_wait_all(count, k):
        arrived(mixed.at[0, pl.ds(0, count), :], m_recv.at[k])

    def heads_wait(sender, r, h, k):
        arrived(head_piece(sender, r, h), m_recv.at[k])

    barrier = pltpu.get_barrier_semaphore()
    pl.semaphore_signal(barrier, inc=1, device_id=partner, device_id_type=MESH)
    for name, here in (("sp_0", z), ("sp_1", y), ("tp", x)):
        for step in (1, 2, 3):
            pl.semaphore_signal(
                barrier, inc=1, device_id={name: turn(here, step)}, device_id_type=MESH
            )

    me = slot(0, 0, core)
    loads = []

    def load(src, dst, shared=None):
        sem = load_sem.at[2 + len(loads) if shared is None else shared]
        copy = pltpu.make_async_copy(src, dst, sem)
        copy.start()
        if shared is None:
            loads.append(copy)

    for n in range(ff // 128):
        cols = pl.ds(n * 128, 128)
        load(gate_shard.at[:, cols], weights.at[me, :, pl.ds(n * 256, 128)], 0)
        load(up_shard.at[:, cols], weights.at[me, :, pl.ds(n * 256 + 128, 128)], 0)
    load(down_shard, weights.at[me, :, pl.ds(2 * ff, ff)], 0)
    load(layer_source, sources.at[x])
    shard_loads = len(loads)
    for src, dst in (
        (wide_query_far, wide_query),
        (wide_forget_far, wide_forget),
        (wide_gap_far, wide_gap),
        (narrow_query_far, narrow_query),
        (narrow_forget_far, narrow_forget),
        (narrow_gap_far, narrow_gap),
        (values_far, values),
        (fades_far, fades),
    ):
        load(src, dst)
    first_loads = len(loads)
    load(switches_far, switches)
    load(channel_norm_scale_far, channel_norm_scale)
    mixed_loads = len(loads)
    load(mlp_scale_far, mlp_scale)
    for t in range(RING):
        for g in range(2):
            load(emission.at[g, pl.ds(t * 128, 128), :], projection.at[t, pl.ds(g * 128, 128), :], 1)

    pl.semaphore_wait(barrier, 10)

    pltpu.make_async_copy(weights.at[me], weights.at[me], load_sem.at[0]).wait()
    for copy in loads[:shard_loads]:
        copy.wait()
    start_weights(0)
    start_weights(1)
    rows_start()
    for copy in loads[shard_loads:first_loads]:
        copy.wait()
    for n in range(length // 128):
        cols = pl.ds(n * 128, 128)
        narrow_q[cols, :] = narrow_query[:, cols].astype(F32).T
        narrow_f[cols, :] = narrow_forget[:, cols].astype(F32).T
    line = lax.broadcasted_iota(jnp.int32, (BLOCK, BLOCK), 0)
    column = lax.broadcasted_iota(jnp.int32, (BLOCK, BLOCK), 1)
    mask = line >= column
    ones = jnp.where(mask, 1.0, 0.0)
    groups = (
        (wide_query, wide_forget, wide_gap, wide_out, wide_reach),
        (narrow_q, narrow_f, narrow_gap, narrow_out, narrow_reach),
    )

    def advance(pair, carried):
        for b in range(2):
            at = pl.ds(pl.multiple_of((pair * 2 + b) * BLOCK, BLOCK), BLOCK)
            left = []
            for g in range(2):
                query_ref, forget_ref, gap_ref, out_ref, reach_ref = groups[g]
                state, running = carried[g]
                key = gap_ref[...] * jax.nn.sigmoid(-forget_ref[at, :].astype(F32))
                decay = jnp.log1p(-key)
                query = jax.nn.silu(query_ref[at, :].astype(F32)) * key.shape[1] ** (-0.5)
                fade = fades[g, :, pl.ds(pl.multiple_of(pair * 2 * BLOCK, 2 * BLOCK), 2 * BLOCK)]
                faded = jnp.sum(ones * fade[:, b * BLOCK : (b + 1) * BLOCK], axis=1, keepdims=True)
                prefix = dot(ones, decay, precision=EXACT_PRECISION) + faded
                out, reach, total, state = block_step(
                    query, key, values[g, at, :], prefix, mask, state
                )
                out_ref[at, :] = out
                reach_ref[at, :] = (reach * jnp.exp(running)).astype(BF16)
                left.append((state, running + total))
            carried = tuple(left)
        return carried

    start = tuple(
        (
            jnp.zeros((values.shape[2], group[2].shape[1]), F32),
            jnp.zeros((1, group[2].shape[1]), F32),
        )
        for group in groups
    )
    (wide_state, wide_log), (narrow_state, narrow_log) = lax.fori_loop(
        0, length // (2 * BLOCK), advance, start, unroll=2
    )
    packed = jnp.concatenate([narrow_state[0:64], narrow_state[64:128]], axis=1)
    narrow_log = jnp.concatenate([narrow_log, narrow_log], axis=1)

    store_state(core_states, core, (wide_log, narrow_log, wide_state, packed))
    src = core_states.at[core]
    send(src, src, s_send.at[0], s_recv.at[0], partner)
    arrived(core_states.at[other], s_recv.at[0])
    first = load_state(core_states, 0)
    nothing = jax.tree.map(jnp.zeros_like, first)
    entering = selected(core == 1, first, nothing)
    total = combine(first, load_state(core_states, 1))
    store_state(y_states, y, total)
    src = y_states.at[y]
    for step in (1, 3, 2):
        send(src, src, s_send.at[step], s_recv.at[1 + y], {"sp_1": turn(y, step)})
    pump(0, NEAR[0:4])
    rows_relay(0)
    for step in (1, 3, 2):
        if step == 2:
            rows_relay(1)
        arrived(y_states.at[turn(y, step)], s_recv.at[1 + turn(y, step)])

    def before(ref, here):
        inside, total = (nothing, nothing)
        for k in range(RING):
            total = combine(total, load_state(ref, k))
            inside = selected(k < here, total, inside)
        return (inside, total)

    inside, total = before(y_states, y)
    entering = combine(inside, entering)
    src = z_states.at[z]
    z_copies = [
        pltpu.make_async_remote_copy(
            src_ref=src,
            dst_ref=src,
            send_sem=s_send.at[3 + step],
            recv_sem=s_recv.at[5 + z],
            device_id={"sp_0": turn(z, step)},
            device_id_type=MESH,
        )
        for step in (1, 3, 2)
    ]
    told = pltpu.make_async_remote_copy(
        src_ref=z_before.at[0],
        dst_ref=z_before.at[0],
        send_sem=s_send.at[7],
        recv_sem=s_recv.at[9],
        device_id=partner,
        device_id_type=MESH,
    )

    @pl.when(core == 1)
    def _():
        store_state(z_states, z, total)
        for copy in z_copies:
            copy.start()

    pump(0, NEAR[4:6] + ACROSS)
    pump_group(0, SIDES)

    @pl.when(core == 1)
    def _():
        for step in (1, 3, 2):
            arrived(z_states.at[turn(z, step)], s_recv.at[5 + turn(z, step)])
        store_state(z_before, 0, before(z_states, z)[0])
        told.start()

    @pl.when(core == 0)
    def _():
        told.wait_recv()

    entering = combine(load_state(z_before, 0), entering)
    _, _, wide_state, packed = entering
    narrow_state = jnp.concatenate([packed[:, 0:64], packed[:, 64:128]], axis=0).astype(BF16)
    wide_state = wide_state.astype(BF16)

    for copy in loads[first_loads:mixed_loads]:
        copy.wait()
    for n in range(RING):
        at = pl.ds(n * rows, rows)
        parts = []
        for g, (out_ref, reach_ref, state) in enumerate(
            ((wide_out, wide_reach, wide_state), (narrow_out, narrow_reach, narrow_state))
        ):
            out = out_ref[at, :] + dot(reach_ref[at, :], state, NT)
            inverse = lax.rsqrt(jnp.mean(out * out, axis=1, keepdims=True) + EPSILON)
            out = out * inverse * channel_norm_scale[...]
            parts.append((out * jax.nn.silu(switches[g, at, :].astype(F32))).astype(BF16))
        mixed[x, at, :] = jnp.concatenate(parts, axis=1)

    own_half, across_half = (((2, 1), (2, 0)), ((0, 0), (0, 1)))
    own_rows, across_rows = (((1, None), (3, None)), ((3, None), (1, None)))
    for (right, left), to_right, to_left in (
        (own_half, 3, 4),
        (own_rows, 0, 0),
        (across_half, 5, 6),
        (across_rows, 7, 8),
    ):
        heads_to(0, *right, to_right, 1)
        heads_to(0, *left, to_left, 3)

    def heads_relay(k, landing, right, left):
        heads_wait(3, *right, k)
        heads_to(3, *right, landing, 1)
        heads_wait(1, *left, k + 1)
        heads_to(1, *left, landing, 3)

    pump(0, CORNERS[0:2])
    pump(1, NEAR[0:4])
    heads_relay(3, 0, *own_half)
    pump(0, CORNERS[2:4])
    pump_group(0, EDGES)
    pump(1, NEAR[4:6])
    pump(0, CORNERS[4:6])
    pump(1, ACROSS)
    for i in (3, 1, 2):
        for h in range(2):
            spread(i, h, 1, False)
    heads_relay(5, 1, *across_half)
    pltpu.make_async_copy(projection, projection, load_sem.at[1]).wait()
    for copy in loads[mixed_loads:]:
        copy.wait()
    heads_wait_all(768, 0)

    half = rows // 2
    upper, lower = (pl.ds(0, half), pl.ds(half, half))

    def emit(pieces, chunk, raw):
        def lines(owner, h):
            return pl.ds(pl.multiple_of(owner * rows + h * half, half), half)

        left = jnp.concatenate(
            [
                jnp.concatenate([mixed[t, lines(owner, h), :] for owner, h in pieces], axis=0)
                for t in range(RING)
            ],
            axis=1,
        )

        def tile(n, squares):
            cols = pl.ds(pl.multiple_of(n * 512, 512), 512)
            found = dot(left, projection[:, :, cols].reshape(4 * 256, 512))
            source = [sources[owner, pl.ds(h * half, half), cols] for owner, h in pieces]
            found = found + jnp.concatenate(source, axis=0).astype(F32)
            raw[:, cols] = found
            found = found * found
            return squares + (
                (found[:, 0:128] + found[:, 128:256]) + (found[:, 256:384] + found[:, 384:512])
            )

        squares = lax.fori_loop(0, model // 512, tile, jnp.zeros((rows, 128), F32))
        mean = jnp.sum(squares, axis=1, keepdims=True) / model
        inverse = lax.rsqrt(mean + EPSILON)

        def scale(n, carry):
            cols = pl.ds(pl.multiple_of(n * 512, 512), 512)
            normed[chunk, :, cols] = (raw[:, cols] * inverse * mlp_scale[:, cols]).astype(BF16)
            return carry

        lax.fori_loop(0, model // 512, scale, 0)

    def widen_all(chunk, first=0, last=ff // 128):
        def widen(n, carry):
            cols = pl.ds(pl.multiple_of(n * 256, 256), 256)
            both = dot(normed[chunk], weights[:, :, cols].reshape(model, 256))
            found = (jax.nn.silu(both[:, 0:128]) * both[:, 128:256]).astype(BF16)
            hidden[:, pl.ds(pl.multiple_of(n * 128, 128), 128)] = found
            return carry

        lax.fori_loop(first, last, widen, 0, unroll=4)

    def shrink_tile(out_ref, n, passed=False):
        cols = pl.ds(pl.multiple_of(n * 256, 256), 256)
        four = weights[pl.ds(n * 4, 4), :, pl.ds(2 * ff, ff)].reshape(256, ff)
        found = dot(hidden[...], four, NT)
        if passed:
            found = found + jnp.concatenate(
                [passing[0, :, cols], passing[1, :, cols]], axis=0
            ).astype(F32)
        out_ref[:, cols] = found.astype(out_ref.dtype)

    def shrink_all(out_ref, passed=False):
        def shrink(n, carry):
            shrink_tile(out_ref, n, passed)
            return carry

        lax.fori_loop(0, model // 256, shrink, 0, unroll=4)

    def send_sum(src, dst, k, step):
        send(src, dst, r_send.at[0], r_recv.at[k], {"tp": turn(x, step)}, False)

    left_x, right_x = (turn(x, 3), turn(x, 1))

    emit(((x, 0), (x, 1)), 3, updated)
    send(normed.at[3, lower], normed.at[2, lower], n_send.at[0], n_recv.at[0], {"tp": right_x}, False)
    send(normed.at[3, upper], normed.at[2, upper], n_send.at[0], n_recv.at[0], {"tp": left_x}, False)
    heads_wait(3, 3, None, 7)
    heads_to(3, 3, 1, 2, 1)
    heads_wait(1, 1, None, 8)
    heads_to(1, 1, 0, 2, 3)
    pump_group(1, SIDES)
    pump(1, CORNERS[0:2])
    heads_wait_all(256, 1)
    rows_opposite()
    emit(((turn(x, 2), 0), (turn(x, 2), 1)), 0, own_part)
    pump(1, CORNERS[2:4])
    pump_group(0, ENDS)
    pump_group(0, FAR)
    pump(1, CORNERS[4:5])
    wait_partner(0)
    widen_all(0, 0, 4)
    pump(1, CORNERS[5:6])
    pump_group(1, EDGES)
    widen_all(0, 4, 8)
    pump_group(1, ENDS)
    widen_all(0, 8, ff // 128)
    for near, steps in ((True, (0, 3)), (False, (1, 2))):
        if not near:
            pump_group(1, FAR)
        wait_partner_half(near)
        for step in steps:
            for n in range(2):
                shrink_tile(partial.at[0], turn(z, step) * 2 + n)
        for step in steps:
            cols = pl.ds(pl.multiple_of(turn(z, step) * 512, 512), 512)
            send_sum(partial.at[0, upper, cols], passing.at[0, :, cols], 0, 1)
            send_sum(partial.at[0, lower, cols], passing.at[1, :, cols], 0, 3)
    heads_wait_all(256, 2)
    emit(((right_x, 1), (left_x, 0)), 1, own_part)
    widen_all(1)
    shrink_all(partial.at[1])
    send_sum(partial.at[1, upper], landed.at[0, lower], 1, 1)
    send_sum(partial.at[1, lower], landed.at[1, upper], 1, 3)
    arrived(normed.at[2], n_recv.at[0])
    widen_all(2)
    arrived(passing, r_recv.at[0])
    shrink_all(partial.at[2], passed=True)
    for k in range(2):
        cols = pl.ds(k * (model // 2), model // 2)
        send_sum(partial.at[2, upper, cols], landed.at[0, upper, cols], 2 + k, 1)
        send_sum(partial.at[2, lower, cols], landed.at[1, lower, cols], 2 + k, 3)
    widen_all(3)
    shrink_all(own_part)
    arrived(landed.at[0], r_recv.at[1])

    def gather_early(n, carry):
        cols = pl.ds(pl.multiple_of(n * 256, 256), 256)
        early = jnp.concatenate([landed[1, upper, cols], landed[0, lower, cols]], axis=0)
        summed = own_part[:, cols] + early.astype(F32)
        updated[:, cols] = updated[:, cols] + 0.5 * summed
        return carry

    lax.fori_loop(0, model // 256, gather_early, 0)

    def finish(n, carry):
        cols = pl.ds(pl.multiple_of(n * 256, 256), 256)
        late = jnp.concatenate([landed[0, upper, cols], landed[1, lower, cols]], axis=0)
        layer_out[:, cols] = (updated[:, cols] + 0.5 * late.astype(F32)).astype(BF16)
        return carry

    for k in range(2):
        arrived(landed.at[0, :, pl.ds(0, model // 2)], r_recv.at[2 + k])
        lax.fori_loop(k * (model // 512), (k + 1) * (model // 512), finish, 0, unroll=2)
    for copy in sent:
        copy.wait_send()
    for shards, sem in (
        (weights.at[pl.ds(0, 15)], w_send),
        (weights.at[pl.ds(0, 16)], d_send),
        (sources.at[pl.ds(0, 2)], x_send),
        (mixed.at[pl.ds(0, 3), pl.ds(0, 3 * rows), :], m_send),
        (normed.at[0], n_send),
        (partial, r_send),
    ):
        pltpu.make_async_remote_copy(
            src_ref=shards,
            dst_ref=shards,
            send_sem=sem.at[0],
            recv_sem=sem.at[0],
            device_id=partner,
            device_id_type=MESH,
        ).wait_send()

    @pl.when(core == 1)
    def _():
        for copy in z_copies:
            copy.wait_send()
        told.wait_send()


def local(
    layer_source,
    broad_probe_tensor,
    broad_retention_preact,
    broad_floor_margin,
    slim_probe_tensor,
    slim_retention_preact,
    slim_floor_margin,
    branch_content_tensor,
    emitted_switch_preact,
    extra_log_fades,
    channel_norm_scale,
    emission_projection,
    mlp_norm_scale,
    switch_projection,
    expand_projection,
    shrink_projection,
):
    rows, model = layer_source.shape
    length = broad_probe_tensor.shape[0]
    depth, ff = switch_projection.shape
    vmem = pl.BlockSpec(memory_space=pltpu.VMEM)
    far = pl.BlockSpec(memory_space=pl.ANY)
    dma = pltpu.SemaphoreType.DMA
    return pl.pallas_call(
        layer_kernel,
        out_shape=pltpu.VMEM((rows, model), BF16),
        in_specs=[far] * 16,
        out_specs=vmem,
        scratch_shapes=[
            pltpu.VMEM((32, depth, 3 * ff), BF16),
            pltpu.VMEM((RING, rows, model), BF16),
            pltpu.VMEM((RING, length, 256), BF16),
            pltpu.VMEM((RING, 256, model), BF16),
            pltpu.VMEM((rows, model), F32),
            pltpu.VMEM((RING, rows, model), BF16),
            pltpu.VMEM((rows, ff), BF16),
            pltpu.VMEM((3, rows, model), BF16),
            pltpu.VMEM((rows, model), F32),
            pltpu.VMEM((2, rows // 2, model), BF16),
            pltpu.VMEM((2, rows, model), BF16),
            pltpu.VMEM((length, 64), F32),
            pltpu.VMEM((length, 64), F32),
            pltpu.VMEM((length, 128), F32),
            pltpu.VMEM((length, 128), F32),
            pltpu.VMEM((length, 128), BF16),
            pltpu.VMEM((length, 64), BF16),
            pltpu.VMEM((2, 208, 128), BF16),
            pltpu.VMEM((RING, 208, 128), BF16),
            pltpu.VMEM((RING, 208, 128), BF16),
            pltpu.VMEM((1, 208, 128), BF16),
            pltpu.VMEM((length, 128), BF16),
            pltpu.VMEM((length, 128), BF16),
            pltpu.VMEM((1, 128), F32),
            pltpu.VMEM((64, length), BF16),
            pltpu.VMEM((64, length), BF16),
            pltpu.VMEM((1, 64), F32),
            pltpu.VMEM((2, length, 128), BF16),
            pltpu.VMEM((2, length, 128), BF16),
            pltpu.VMEM((2, 1, length), F32),
            pltpu.VMEM((1, 128), F32),
            pltpu.VMEM((1, model), F32),
            dma((14,)),
            dma((1,)),
            dma((36,)),
            dma((1,)),
            dma((3,)),
            dma((1,)),
            dma((5,)),
            dma((1,)),
            dma((9,)),
            dma((1,)),
            dma((1,)),
            dma((8,)),
            dma((10,)),
            dma((1,)),
            dma((4,)),
        ],
        compiler_params=pltpu.CompilerParams(
            collective_id=0, has_side_effects=True, vmem_limit_bytes=62 * 1024 * 1024
        ),
    )(
        layer_source,
        broad_probe_tensor,
        broad_retention_preact,
        broad_floor_margin.reshape(1, -1),
        slim_probe_tensor.T,
        slim_retention_preact.T,
        slim_floor_margin.reshape(1, -1),
        branch_content_tensor,
        emitted_switch_preact,
        jnp.swapaxes(extra_log_fades, 1, 2),
        channel_norm_scale.reshape(1, -1),
        emission_projection,
        mlp_norm_scale.reshape(1, -1),
        switch_projection,
        expand_projection,
        shrink_projection.T,
    )


def solution(mesh):
    torus = Mesh(mesh.devices.reshape(4, 4, 2, mesh.shape["tp"]), SP_TP)
    placed = (
        P(SP_TP, None),
        P(SP, "tp"),
        P(SP, "tp"),
        P("tp"),
        P(SP, "tp"),
        P(SP, "tp"),
        P("tp"),
        P(None, SP, "tp"),
        P(None, SP, "tp"),
        P(None, SP, "tp"),
        P(),
        P(),
        P(),
        P(SP, "tp"),
        P(SP, "tp"),
        P("tp", SP),
    )
    return jax.shard_map(
        local, mesh=torus, in_specs=placed, out_specs=P(SP_TP, None), check_vma=False
    )
```

```python
import jax
import jax.numpy as jnp
from jax import lax
from jax.experimental import pallas as pl
from jax.experimental.pallas import tpu as pltpu
from jax.sharding import Mesh
from jax.sharding import PartitionSpec as P

BLOCK = 64
RING = 4
SP = ("sp_0", "sp_1", "sp_2")
SP_TP = ("sp_0", "sp_1", "sp_2", "tp")

EPSILON = 1e-06
EXACT_PRECISION = lax.Precision.HIGHEST
BF16 = jnp.bfloat16
F32 = jnp.float32
NT = (((1,), (1,)), ((), ()))
TN = (((0,), (0,)), ((), ()))
MESH = pl.DeviceIdType.MESH

NEAR = ((3, 0, 0), (1, 0, 1), (0, 3, 0), (0, 1, 1), (3, 0, 1), (1, 0, 0))
ACROSS = ((2, 0, 0), (2, 0, 1))
CORNERS = ((3, 3, 0), (3, 1, 1), (1, 3, 0), (1, 1, 1), (2, 3, 0), (2, 1, 1))
SIDES = ((0, 3, 1), (0, 1, 0))
EDGES = ((3, 3, 1), (3, 1, 0), (0, 2, 0), (0, 2, 1), (1, 3, 1), (1, 1, 0))
ENDS = ((2, 3, 1), (2, 1, 0), (3, 2, 0), (3, 2, 1))
FAR = ((1, 2, 0), (1, 2, 1), (2, 2, 0), (2, 2, 1))


PASSED = NEAR + ACROSS + CORNERS
GROUPS = (SIDES, EDGES, ENDS, FAR)


def turn(value, step):
    return lax.rem(value + step, RING)


def dot(a, b, dims=(((1,), (0,)), ((), ())), precision=None):
    return lax.dot_general(a, b, dims, preferred_element_type=F32, precision=precision)


def combine(earlier, later):
    wide_early, narrow_early, wide_state_early, narrow_state_early = earlier
    wide_late, narrow_late, wide_state_late, narrow_state_late = later
    return (
        wide_early + wide_late,
        narrow_early + narrow_late,
        jnp.exp(wide_late) * wide_state_early + wide_state_late,
        jnp.exp(narrow_late) * narrow_state_early + narrow_state_late,
    )


def split_log(log):
    first = log.astype(BF16).astype(F32)
    second = (log - first).astype(BF16).astype(F32)
    return [first, second, log - first - second]


def store_state(ref, at, state):
    wide, narrow, wide_state, narrow_state = state
    ref[at, 0:128, :] = wide_state.astype(BF16)
    ref[at, 128:192, :] = narrow_state.astype(BF16)
    lines = split_log(wide) + split_log(narrow)
    lines.append(jnp.zeros((10, wide.shape[1]), F32))
    ref[at, 192:208, :] = jnp.concatenate(lines, axis=0).astype(BF16)


def load_state(ref, at):
    lines = ref[at, 192:208, :].astype(F32)
    wide = lines[0:1] + lines[1:2] + lines[2:3]
    narrow = lines[3:4] + lines[4:5] + lines[5:6]
    return (wide, narrow, ref[at, 0:128, :].astype(F32), ref[at, 128:192, :].astype(F32))


def selected(passed, new, old):
    return jax.tree.map(lambda a, b: jnp.where(passed, a, b), new, old)


def block_step(query, key, value, prefix, mask, state):
    half = BLOCK // 2
    middle, total = (prefix[half - 1 : half, :], prefix[BLOCK - 1 : BLOCK, :])
    query_in = query * jnp.exp(prefix - middle)
    key_in = key * jnp.exp(middle - prefix)
    scores = dot(query_in.astype(BF16), key_in.astype(BF16), NT)
    scores = jnp.where(mask, scores, 0.0).astype(BF16)
    inside = dot(scores, value)
    reach = query_in * jnp.exp(middle)
    earlier = dot(reach.astype(BF16), state.astype(BF16), NT)
    leaving = (key_in * jnp.exp(total - middle)).astype(BF16)
    state = state * jnp.exp(total) + dot(value, leaving, TN)
    return (inside + earlier, reach, total, state)


def layer_kernel(
    layer_source,
    wide_query_far,
    wide_forget_far,
    wide_gap_far,
    narrow_query_far,
    narrow_forget_far,
    narrow_gap_far,
    values_far,
    switches_far,
    fades_far,
    channel_norm_scale_far,
    emission,
    mlp_scale_far,
    gate_shard,
    up_shard,
    down_shard,
    layer_out,
    weights,
    sources,
    mixed,
    projection,
    updated,
    normed,
    hidden,
    partial,
    own_part,
    passing,
    landed,
    narrow_q,
    narrow_f,
    wide_out,
    narrow_out,
    wide_reach,
    narrow_reach,
    core_states,
    y_states,
    z_states,
    z_before,
    wide_query,
    wide_forget,
    wide_gap,
    narrow_query,
    narrow_forget,
    narrow_gap,
    values,
    switches,
    fades,
    channel_norm_scale,
    mlp_scale,
    load_sem,
    w_send,
    w_recv,
    d_send,
    d_recv,
    x_send,
    x_recv,
    m_send,
    m_recv,
    n_send,
    n_recv,
    s_send,
    s_recv,
    r_send,
    r_recv,
):
    z, y, core, x = (lax.axis_index(name) for name in SP_TP)
    other = 1 - core
    rows, model = layer_source.shape
    length = wide_query.shape[0]
    ff = gate_shard.shape[1]
    depth = gate_shard.shape[0]
    sent = []

    def send(src, dst, send_sem, recv_sem, to, alone=True):
        copy = pltpu.make_async_remote_copy(
            src_ref=src,
            dst_ref=dst,
            send_sem=send_sem,
            recv_sem=recv_sem,
            device_id=to,
            device_id_type=MESH,
        )
        copy.start()
        if alone:
            sent.append(copy)

    partner = {"sp_2": other}

    def arrived(ref, sem):
        pltpu.make_async_remote_copy(
            src_ref=ref,
            dst_ref=ref,
            send_sem=sem,
            recv_sem=sem,
            device_id=partner,
            device_id_type=MESH,
        ).wait_recv()

    def place(i, j, of_core):
        first = jnp.where(of_core == 0, y, z)
        second = jnp.where(of_core == 0, z, y)
        first, second = (turn(first, i), turn(second, j))
        return (
            jnp.where(of_core == 0, second, first),
            jnp.where(of_core == 0, first, second),
        )

    def slot(i, j, of_core):
        at_z, at_y = place(i, j, of_core)
        return at_z * 8 + at_y * 2 + of_core

    half_depth = depth // 2

    columns_of = (pl.ds(0, 2 * ff), pl.ds(2 * ff, ff))

    def shard(i, j, h, part, of_core):
        lines = pl.ds(h * half_depth, half_depth)
        return weights.at[slot(i, j, of_core), lines, columns_of[part]]

    def shard_part(i, j, part, of_core):
        return weights.at[slot(i, j, of_core), :, columns_of[part]]

    def toward(i, j):
        at_z, at_y = place(i, j, core)
        return {"sp_0": at_z, "sp_1": at_y}

    def mark(i, j, h, part):
        if (i, j, h) in PASSED:
            return part * 18 + PASSED.index((i, j, h))
        return part * 18 + 14 + [(i, j, h) in group for group in GROUPS].index(True)

    def forward(i, j, h, part, step, landing):
        src = shard(i, j, h, part, core)
        at = w_recv.at[mark(*landing, h, part)]
        send(src, src, w_send.at[0], at, toward(*step), False)

    def hand_over(i, j, part):
        src = shard_part(i, j, part, core)
        landing = part
        if part == 1:
            landing = jnp.where(core == 0, 1 if j in (0, 3) else 2, 1 if i in (0, 3) else 2)
        send(src, src, d_send.at[0], d_recv.at[landing], partner, False)

    def spread(i, h, part, passed_on):
        if (h == 0) == passed_on:
            forward(i, 0, h, part, (0, 1), (i, 3))
        else:
            forward(i, 0, h, part, (0, 3), (i, 1))

    handed = {}

    def pump(part, arrivals):
        for i, j, h in arrivals:
            arrived(shard(i, j, h, part, core), w_recv.at[mark(i, j, h, part)])
            if j == 0:
                if (i, h) == (3, 0):
                    forward(i, 0, h, part, (1, 0), (2, 0))
                if (i, h) == (1, 1):
                    forward(i, 0, h, part, (3, 0), (2, 0))
                spread(i, h, part, True)
                if part == 0:
                    spread(i, h, part, False)
            else:
                if (j, h) == (3, 0):
                    forward(i, j, h, part, (0, 1), (i, 2))
                if (j, h) == (1, 1):
                    forward(i, j, h, part, (0, 3), (i, 2))
            seen(i, j, part)

    def seen(i, j, part):
        handed[(i, j, part)] = handed.get((i, j, part), 0) + 1
        if handed[(i, j, part)] == 2:
            hand_over(i, j, part)

    def pump_group(part, group):
        halves = weights.at[pl.ds(0, len(group) // 2), :, columns_of[part]]
        arrived(halves, w_recv.at[mark(*group[0], part)])
        for i, j, _ in group:
            seen(i, j, part)

    def start_weights(part):
        for h in range(2):
            forward(0, 0, h, part, (1, 0), (3, 0))
            forward(0, 0, 1 - h, part, (3, 0), (1, 0))
            forward(0, 0, h, part, (0, 1), (0, 3))
            forward(0, 0, 1 - h, part, (0, 3), (0, 1))
        hand_over(0, 0, part)

    def wait_partner(part):
        arrived(weights.at[pl.ds(0, 16), :, columns_of[part]], d_recv.at[part])

    def wait_partner_half(near):
        arrived(weights.at[pl.ds(0, 8), :, columns_of[1]], d_recv.at[1 if near else 2])

    def rows_piece(step, q):
        quarter = rows // 4
        return sources.at[turn(x, step), pl.ds(q * quarter, quarter), :]

    def rows_to(step, q, landing, to):
        src = rows_piece(step, q)
        at = x_recv.at[min(landing, 4)]
        send(src, src, x_send.at[0], at, {"tp": turn(x, to)}, False)

    def rows_start():
        for k in range(2):
            rows_to(0, k, k, 1)
            rows_to(0, 2 + k, 2 + k, 3)

    def rows_relay(k):
        arrived(rows_piece(3, k), x_recv.at[k])
        rows_to(3, k, 4 + k, 1)
        arrived(rows_piece(1, 2 + k), x_recv.at[2 + k])
        rows_to(1, 2 + k, 6 + k, 3)

    def rows_opposite():
        arrived(sources.at[turn(x, 2)], x_recv.at[4])

    def head_piece(sender, r, h):
        owner = turn(x, (sender + r) % RING)
        at = owner * rows + (0 if h is None else h * (rows // 2))
        count = rows if h is None else rows // 2
        return mixed.at[turn(x, sender), pl.ds(pl.multiple_of(at, 128), count), :]

    def heads_to(sender, r, h, k, step):
        src = head_piece(sender, r, h)
        send(src, src, m_send.at[0], m_recv.at[k], {"tp": turn(x, step)}, False)

    def heads_wait_all(count, k):
        arrived(mixed.at[0, pl.ds(0, count), :], m_recv.at[k])

    def heads_wait(sender, r, h, k):
        arrived(head_piece(sender, r, h), m_recv.at[k])

    barrier = pltpu.get_barrier_semaphore()
    pl.semaphore_signal(barrier, inc=1, device_id=partner, device_id_type=MESH)
    for name, here in (("sp_0", z), ("sp_1", y), ("tp", x)):
        for step in (1, 2, 3):
            pl.semaphore_signal(
                barrier, inc=1, device_id={name: turn(here, step)}, device_id_type=MESH
            )

    me = slot(0, 0, core)
    loads = []

    def load(src, dst, shared=None):
        sem = load_sem.at[2 + len(loads) if shared is None else shared]
        copy = pltpu.make_async_copy(src, dst, sem)
        copy.start()
        if shared is None:
            loads.append(copy)

    for n in range(ff // 128):
        cols = pl.ds(n * 128, 128)
        load(gate_shard.at[:, cols], weights.at[me, :, pl.ds(n * 256, 128)], 0)
        load(up_shard.at[:, cols], weights.at[me, :, pl.ds(n * 256 + 128, 128)], 0)
    load(down_shard, weights.at[me, :, pl.ds(2 * ff, ff)], 0)
    load(layer_source, sources.at[x])
    shard_loads = len(loads)
    for src, dst in (
        (wide_query_far, wide_query),
        (wide_forget_far, wide_forget),
        (wide_gap_far, wide_gap),
        (narrow_query_far, narrow_query),
        (narrow_forget_far, narrow_forget),
        (narrow_gap_far, narrow_gap),
        (values_far, values),
        (fades_far, fades),
    ):
        load(src, dst)
    first_loads = len(loads)
    load(switches_far, switches)
    load(channel_norm_scale_far, channel_norm_scale)
    mixed_loads = len(loads)
    load(mlp_scale_far, mlp_scale)
    for t in range(RING):
        for g in range(2):
            load(emission.at[g, pl.ds(t * 128, 128), :], projection.at[t, pl.ds(g * 128, 128), :], 1)

    pl.semaphore_wait(barrier, 10)

    pltpu.make_async_copy(weights.at[me], weights.at[me], load_sem.at[0]).wait()
    for copy in loads[:shard_loads]:
        copy.wait()
    start_weights(0)
    start_weights(1)
    rows_start()
    for copy in loads[shard_loads:first_loads]:
        copy.wait()
    for n in range(length // 128):
        cols = pl.ds(n * 128, 128)
        narrow_q[cols, :] = narrow_query[:, cols].astype(F32).T
        narrow_f[cols, :] = narrow_forget[:, cols].astype(F32).T
    line = lax.broadcasted_iota(jnp.int32, (BLOCK, BLOCK), 0)
    column = lax.broadcasted_iota(jnp.int32, (BLOCK, BLOCK), 1)
    mask = line >= column
    ones = jnp.where(mask, 1.0, 0.0)
    groups = (
        (wide_query, wide_forget, wide_gap, wide_out, wide_reach),
        (narrow_q, narrow_f, narrow_gap, narrow_out, narrow_reach),
    )

    def advance(pair, carried):
        for b in range(2):
            at = pl.ds(pl.multiple_of((pair * 2 + b) * BLOCK, BLOCK), BLOCK)
            left = []
            for g in range(2):
                query_ref, forget_ref, gap_ref, out_ref, reach_ref = groups[g]
                state, running = carried[g]
                key = gap_ref[...] * jax.nn.sigmoid(-forget_ref[at, :].astype(F32))
                decay = jnp.log1p(-key)
                query = jax.nn.silu(query_ref[at, :].astype(F32)) * key.shape[1] ** (-0.5)
                fade = fades[g, :, pl.ds(pl.multiple_of(pair * 2 * BLOCK, 2 * BLOCK), 2 * BLOCK)]
                faded = jnp.sum(ones * fade[:, b * BLOCK : (b + 1) * BLOCK], axis=1, keepdims=True)
                prefix = dot(ones, decay, precision=EXACT_PRECISION) + faded
                out, reach, total, state = block_step(
                    query, key, values[g, at, :], prefix, mask, state
                )
                out_ref[at, :] = out
                reach_ref[at, :] = (reach * jnp.exp(running)).astype(BF16)
                left.append((state, running + total))
            carried = tuple(left)
        return carried

    start = tuple(
        (
            jnp.zeros((values.shape[2], group[2].shape[1]), F32),
            jnp.zeros((1, group[2].shape[1]), F32),
        )
        for group in groups
    )
    (wide_state, wide_log), (narrow_state, narrow_log) = lax.fori_loop(
        0, length // (2 * BLOCK), advance, start, unroll=2
    )
    packed = jnp.concatenate([narrow_state[0:64], narrow_state[64:128]], axis=1)
    narrow_log = jnp.concatenate([narrow_log, narrow_log], axis=1)

    store_state(core_states, core, (wide_log, narrow_log, wide_state, packed))
    src = core_states.at[core]
    send(src, src, s_send.at[0], s_recv.at[0], partner)
    arrived(core_states.at[other], s_recv.at[0])
    first = load_state(core_states, 0)
    nothing = jax.tree.map(jnp.zeros_like, first)
    entering = selected(core == 1, first, nothing)
    total = combine(first, load_state(core_states, 1))
    store_state(y_states, y, total)
    src = y_states.at[y]
    for step in (1, 3, 2):
        send(src, src, s_send.at[step], s_recv.at[1 + y], {"sp_1": turn(y, step)})
    pump(0, NEAR[0:4])
    rows_relay(0)
    for step in (1, 3, 2):
        if step == 2:
            rows_relay(1)
        arrived(y_states.at[turn(y, step)], s_recv.at[1 + turn(y, step)])

    def before(ref, here):
        inside, total = (nothing, nothing)
        for k in range(RING):
            total = combine(total, load_state(ref, k))
            inside = selected(k < here, total, inside)
        return (inside, total)

    inside, total = before(y_states, y)
    entering = combine(inside, entering)
    src = z_states.at[z]
    z_copies = [
        pltpu.make_async_remote_copy(
            src_ref=src,
            dst_ref=src,
            send_sem=s_send.at[3 + step],
            recv_sem=s_recv.at[5 + z],
            device_id={"sp_0": turn(z, step)},
            device_id_type=MESH,
        )
        for step in (1, 3, 2)
    ]
    told = pltpu.make_async_remote_copy(
        src_ref=z_before.at[0],
        dst_ref=z_before.at[0],
        send_sem=s_send.at[7],
        recv_sem=s_recv.at[9],
        device_id=partner,
        device_id_type=MESH,
    )

    @pl.when(core == 1)
    def _():
        store_state(z_states, z, total)
        for copy in z_copies:
            copy.start()

    pump(0, NEAR[4:6] + ACROSS)
    pump_group(0, SIDES)

    @pl.when(core == 1)
    def _():
        for step in (1, 3, 2):
            arrived(z_states.at[turn(z, step)], s_recv.at[5 + turn(z, step)])
        store_state(z_before, 0, before(z_states, z)[0])
        told.start()

    @pl.when(core == 0)
    def _():
        told.wait_recv()

    entering = combine(load_state(z_before, 0), entering)
    _, _, wide_state, packed = entering
    narrow_state = jnp.concatenate([packed[:, 0:64], packed[:, 64:128]], axis=0).astype(BF16)
    wide_state = wide_state.astype(BF16)

    for copy in loads[first_loads:mixed_loads]:
        copy.wait()
    for n in range(RING):
        at = pl.ds(n * rows, rows)
        parts = []
        for g, (out_ref, reach_ref, state) in enumerate(
            ((wide_out, wide_reach, wide_state), (narrow_out, narrow_reach, narrow_state))
        ):
            out = out_ref[at, :] + dot(reach_ref[at, :], state, NT)
            inverse = lax.rsqrt(jnp.mean(out * out, axis=1, keepdims=True) + EPSILON)
            out = out * inverse * channel_norm_scale[...]
            parts.append((out * jax.nn.silu(switches[g, at, :].astype(F32))).astype(BF16))
        mixed[x, at, :] = jnp.concatenate(parts, axis=1)

    own_half, across_half = (((2, 1), (2, 0)), ((0, 0), (0, 1)))
    own_rows, across_rows = (((1, None), (3, None)), ((3, None), (1, None)))
    for (right, left), to_right, to_left in (
        (own_half, 3, 4),
        (own_rows, 0, 0),
        (across_half, 5, 6),
        (across_rows, 7, 8),
    ):
        heads_to(0, *right, to_right, 1)
        heads_to(0, *left, to_left, 3)

    def heads_relay(k, landing, right, left):
        heads_wait(3, *right, k)
        heads_to(3, *right, landing, 1)
        heads_wait(1, *left, k + 1)
        heads_to(1, *left, landing, 3)

    pump(0, CORNERS[0:2])
    pump(1, NEAR[0:4])
    heads_relay(3, 0, *own_half)
    pump(0, CORNERS[2:4])
    pump_group(0, EDGES)
    pump(1, NEAR[4:6])
    pump(0, CORNERS[4:6])
    pump(1, ACROSS)
    for i in (3, 1, 2):
        for h in range(2):
            spread(i, h, 1, False)
    heads_relay(5, 1, *across_half)
    pltpu.make_async_copy(projection, projection, load_sem.at[1]).wait()
    for copy in loads[mixed_loads:]:
        copy.wait()
    heads_wait_all(768, 0)

    half = rows // 2
    upper, lower = (pl.ds(0, half), pl.ds(half, half))

    def emit(pieces, chunk, raw):
        def lines(owner, h):
            return pl.ds(pl.multiple_of(owner * rows + h * half, half), half)

        left = jnp.concatenate(
            [
                jnp.concatenate([mixed[t, lines(owner, h), :] for owner, h in pieces], axis=0)
                for t in range(RING)
            ],
            axis=1,
        )

        def tile(n, squares):
            cols = pl.ds(pl.multiple_of(n * 512, 512), 512)
            found = dot(left, projection[:, :, cols].reshape(4 * 256, 512))
            source = [sources[owner, pl.ds(h * half, half), cols] for owner, h in pieces]
            found = found + jnp.concatenate(source, axis=0).astype(F32)
            raw[:, cols] = found
            found = found * found
            return squares + (
                (found[:, 0:128] + found[:, 128:256]) + (found[:, 256:384] + found[:, 384:512])
            )

        squares = lax.fori_loop(0, model // 512, tile, jnp.zeros((rows, 128), F32))
        mean = jnp.sum(squares, axis=1, keepdims=True) / model
        inverse = lax.rsqrt(mean + EPSILON)

        def scale(n, carry):
            cols = pl.ds(pl.multiple_of(n * 512, 512), 512)
            normed[chunk, :, cols] = (raw[:, cols] * inverse * mlp_scale[:, cols]).astype(BF16)
            return carry

        lax.fori_loop(0, model // 512, scale, 0)

    def widen_all(chunk, first=0, last=ff // 128):
        def widen(n, carry):
            cols = pl.ds(pl.multiple_of(n * 256, 256), 256)
            both = dot(normed[chunk], weights[:, :, cols].reshape(model, 256))
            found = (jax.nn.silu(both[:, 0:128]) * both[:, 128:256]).astype(BF16)
            hidden[:, pl.ds(pl.multiple_of(n * 128, 128), 128)] = found
            return carry

        lax.fori_loop(first, last, widen, 0, unroll=4)

    def shrink_tile(out_ref, n, passed=False):
        cols = pl.ds(pl.multiple_of(n * 256, 256), 256)
        four = weights[pl.ds(n * 4, 4), :, pl.ds(2 * ff, ff)].reshape(256, ff)
        found = dot(hidden[...], four, NT)
        if passed:
            found = found + jnp.concatenate(
                [passing[0, :, cols], passing[1, :, cols]], axis=0
            ).astype(F32)
        out_ref[:, cols] = found.astype(out_ref.dtype)

    def shrink_all(out_ref, passed=False):
        def shrink(n, carry):
            shrink_tile(out_ref, n, passed)
            return carry

        lax.fori_loop(0, model // 256, shrink, 0, unroll=4)

    def send_sum(src, dst, k, step):
        send(src, dst, r_send.at[0], r_recv.at[k], {"tp": turn(x, step)}, False)

    left_x, right_x = (turn(x, 3), turn(x, 1))

    emit(((x, 0), (x, 1)), 3, updated)
    send(normed.at[3, lower], normed.at[2, lower], n_send.at[0], n_recv.at[0], {"tp": right_x}, False)
    send(normed.at[3, upper], normed.at[2, upper], n_send.at[0], n_recv.at[0], {"tp": left_x}, False)
    heads_wait(3, 3, None, 7)
    heads_to(3, 3, 1, 2, 1)
    heads_wait(1, 1, None, 8)
    heads_to(1, 1, 0, 2, 3)
    pump_group(1, SIDES)
    pump(1, CORNERS[0:1])
    heads_wait_all(256, 1)
    rows_opposite()
    emit(((turn(x, 2), 0), (turn(x, 2), 1)), 0, own_part)
    pump(1, CORNERS[1:4])
    pump_group(0, ENDS)
    pump_group(0, FAR)
    pump(1, CORNERS[4:5])
    wait_partner(0)
    widen_all(0, 0, 4)
    pump(1, CORNERS[5:6])
    pump_group(1, EDGES)
    widen_all(0, 4, 8)
    pump_group(1, ENDS)
    widen_all(0, 8, ff // 128)
    for near, steps in ((True, (0, 3)), (False, (1, 2))):
        if not near:
            pump_group(1, FAR)
        wait_partner_half(near)
        for step in steps:
            for n in range(2):
                shrink_tile(partial.at[0], turn(z, step) * 2 + n)
            cols = pl.ds(pl.multiple_of(turn(z, step) * 512, 512), 512)
            send_sum(partial.at[0, upper, cols], passing.at[0, :, cols], 0, 1)
            send_sum(partial.at[0, lower, cols], passing.at[1, :, cols], 0, 3)
    heads_wait_all(256, 2)
    emit(((right_x, 1), (left_x, 0)), 1, own_part)
    widen_all(1)
    shrink_all(partial.at[1])
    send_sum(partial.at[1, upper], landed.at[0, lower], 1, 1)
    send_sum(partial.at[1, lower], landed.at[1, upper], 1, 3)
    arrived(normed.at[2], n_recv.at[0])
    widen_all(2)
    arrived(passing, r_recv.at[0])
    shrink_all(partial.at[2], passed=True)
    for k in range(2):
        cols = pl.ds(k * (model // 2), model // 2)
        send_sum(partial.at[2, upper, cols], landed.at[0, upper, cols], 2 + k, 1)
        send_sum(partial.at[2, lower, cols], landed.at[1, lower, cols], 2 + k, 3)
    widen_all(3)
    shrink_all(own_part)
    arrived(landed.at[0], r_recv.at[1])

    def gather_early(n, carry):
        cols = pl.ds(pl.multiple_of(n * 256, 256), 256)
        early = jnp.concatenate([landed[1, upper, cols], landed[0, lower, cols]], axis=0)
        summed = own_part[:, cols] + early.astype(F32)
        updated[:, cols] = updated[:, cols] + 0.5 * summed
        return carry

    lax.fori_loop(0, model // 256, gather_early, 0)

    def finish(n, carry):
        cols = pl.ds(pl.multiple_of(n * 256, 256), 256)
        late = jnp.concatenate([landed[0, upper, cols], landed[1, lower, cols]], axis=0)
        layer_out[:, cols] = (updated[:, cols] + 0.5 * late.astype(F32)).astype(BF16)
        return carry

    for k in range(2):
        arrived(landed.at[0, :, pl.ds(0, model // 2)], r_recv.at[2 + k])
        lax.fori_loop(k * (model // 512), (k + 1) * (model // 512), finish, 0, unroll=2)
    for copy in sent:
        copy.wait_send()
    for shards, sem in (
        (weights.at[pl.ds(0, 15)], w_send),
        (weights.at[pl.ds(0, 16)], d_send),
        (sources.at[pl.ds(0, 2)], x_send),
        (mixed.at[pl.ds(0, 3), pl.ds(0, 3 * rows), :], m_send),
        (normed.at[0], n_send),
        (partial, r_send),
    ):
        pltpu.make_async_remote_copy(
            src_ref=shards,
            dst_ref=shards,
            send_sem=sem.at[0],
            recv_sem=sem.at[0],
            device_id=partner,
            device_id_type=MESH,
        ).wait_send()

    @pl.when(core == 1)
    def _():
        for copy in z_copies:
            copy.wait_send()
        told.wait_send()


def local(
    layer_source,
    broad_probe_tensor,
    broad_retention_preact,
    broad_floor_margin,
    slim_probe_tensor,
    slim_retention_preact,
    slim_floor_margin,
    branch_content_tensor,
    emitted_switch_preact,
    extra_log_fades,
    channel_norm_scale,
    emission_projection,
    mlp_norm_scale,
    switch_projection,
    expand_projection,
    shrink_projection,
):
    rows, model = layer_source.shape
    length = broad_probe_tensor.shape[0]
    depth, ff = switch_projection.shape
    vmem = pl.BlockSpec(memory_space=pltpu.VMEM)
    far = pl.BlockSpec(memory_space=pl.ANY)
    dma = pltpu.SemaphoreType.DMA
    return pl.pallas_call(
        layer_kernel,
        out_shape=pltpu.VMEM((rows, model), BF16),
        in_specs=[far] * 16,
        out_specs=vmem,
        scratch_shapes=[
            pltpu.VMEM((32, depth, 3 * ff), BF16),
            pltpu.VMEM((RING, rows, model), BF16),
            pltpu.VMEM((RING, length, 256), BF16),
            pltpu.VMEM((RING, 256, model), BF16),
            pltpu.VMEM((rows, model), F32),
            pltpu.VMEM((RING, rows, model), BF16),
            pltpu.VMEM((rows, ff), BF16),
            pltpu.VMEM((3, rows, model), BF16),
            pltpu.VMEM((rows, model), F32),
            pltpu.VMEM((2, rows // 2, model), BF16),
            pltpu.VMEM((2, rows, model), BF16),
            pltpu.VMEM((length, 64), F32),
            pltpu.VMEM((length, 64), F32),
            pltpu.VMEM((length, 128), F32),
            pltpu.VMEM((length, 128), F32),
            pltpu.VMEM((length, 128), BF16),
            pltpu.VMEM((length, 64), BF16),
            pltpu.VMEM((2, 208, 128), BF16),
            pltpu.VMEM((RING, 208, 128), BF16),
            pltpu.VMEM((RING, 208, 128), BF16),
            pltpu.VMEM((1, 208, 128), BF16),
            pltpu.VMEM((length, 128), BF16),
            pltpu.VMEM((length, 128), BF16),
            pltpu.VMEM((1, 128), F32),
            pltpu.VMEM((64, length), BF16),
            pltpu.VMEM((64, length), BF16),
            pltpu.VMEM((1, 64), F32),
            pltpu.VMEM((2, length, 128), BF16),
            pltpu.VMEM((2, length, 128), BF16),
            pltpu.VMEM((2, 1, length), F32),
            pltpu.VMEM((1, 128), F32),
            pltpu.VMEM((1, model), F32),
            dma((14,)),
            dma((1,)),
            dma((36,)),
            dma((1,)),
            dma((3,)),
            dma((1,)),
            dma((5,)),
            dma((1,)),
            dma((9,)),
            dma((1,)),
            dma((1,)),
            dma((8,)),
            dma((10,)),
            dma((1,)),
            dma((4,)),
        ],
        compiler_params=pltpu.CompilerParams(
            collective_id=0, has_side_effects=True, vmem_limit_bytes=62 * 1024 * 1024
        ),
    )(
        layer_source,
        broad_probe_tensor,
        broad_retention_preact,
        broad_floor_margin.reshape(1, -1),
        slim_probe_tensor.T,
        slim_retention_preact.T,
        slim_floor_margin.reshape(1, -1),
        branch_content_tensor,
        emitted_switch_preact,
        jnp.swapaxes(extra_log_fades, 1, 2),
        channel_norm_scale.reshape(1, -1),
        emission_projection,
        mlp_norm_scale.reshape(1, -1),
        switch_projection,
        expand_projection,
        shrink_projection.T,
    )


def solution(mesh):
    torus = Mesh(mesh.devices.reshape(4, 4, 2, mesh.shape["tp"]), SP_TP)
    placed = (
        P(SP_TP, None),
        P(SP, "tp"),
        P(SP, "tp"),
        P("tp"),
        P(SP, "tp"),
        P(SP, "tp"),
        P("tp"),
        P(None, SP, "tp"),
        P(None, SP, "tp"),
        P(None, SP, "tp"),
        P(),
        P(),
        P(),
        P(SP, "tp"),
        P(SP, "tp"),
        P("tp", SP),
    )
    return jax.shard_map(
        local, mesh=torus, in_specs=placed, out_specs=P(SP_TP, None), check_vma=False
    )
```
